256 devices in a mesh: fs: 16 (over y, x), tp: 16 (over z, core).
Axes of the slice: x: 4, y: 4, z: 8, core: 2. Of those that a mesh axis runs over, the one named last changes fastest.
Arguments:
- tokens: bfloat16 [65536, 1024], P(('fs', 'tp')), may hold values from -6 to 6
- norm_in: float32 [1024], replicated, may hold values from 0.1 to 1.9
- value_weight: bfloat16 [1024, 2816], P('fs', 'tp'), may hold values from -0.1875 to 0.1875
- gate_weight: bfloat16 [1024, 2816], P('fs', 'tp'), may hold values from -0.1875 to 0.1875
- value_taps: float32 [3, 2816], P(None, 'tp'), may hold values from -3 to 3
- gate_taps: float32 [3, 2816], P(None, 'tp'), may hold values from -3 to 3
- down_weight: bfloat16 [2816, 1024], P('tp', 'fs'), may hold values from -0.109375 to 0.109375
- norm_out: float32 [1024], replicated, may hold values from 0.1 to 1.9
Outputs:
- mixed: bfloat16 [65536, 1024], P(('fs', 'tp'))
The draws below stay inside these ranges and needn't reach their ends.
All inputs are finite; a program needn't handle non-finite values.
Results may differ from the reference program's by a relative error of at most 0.02.
Values may be sent and summed in bfloat16 or wider, within the bound.
No kernel may reach another device: no remote copies, remote signals or barrier semaphores. Data moves between devices by JAX's collectives and lax.ppermute only.
A program may use at most 64 MiB of HBM per device.

```python
import jax
import jax.numpy as jnp
from jax import lax

D = 1024
FF = 2816
TAPS = 3
TOKENS = 65536


def level_of(key, shape, split, least, high):
    gain = 1.0
    for axis_at, parts in split:
        draws = jax.random.uniform(jax.random.fold_in(jax.random.fold_in(key, 6), axis_at), (parts,), jnp.float32, least / len(split), high / len(split))
        gain = gain * jnp.repeat(jnp.exp(draws), shape[axis_at] // parts).reshape((-1,) + (1,) * (len(shape) - 1 - axis_at))
    return gain


def noise(own_key, dims, deviation, reach, cuts=(), held_as=jnp.bfloat16):
    values = deviation * jax.random.normal(own_key, dims, jnp.float32)
    if cuts:
        values = values * level_of(own_key, dims, cuts, -0.22, 0.18)
    return jnp.clip(values, -reach, reach).astype(held_as)


def setup_inputs(seed: int = 0) -> dict:
    splits = jax.random.split(jax.random.key(seed), 9)
    tokens = noise(splits[0], (TOKENS, D), 1.0, 6.0, ((0, 256),))
    norm_in = jnp.clip(1.0 + 0.18 * jax.random.normal(splits[1], (D,), jnp.float32), 0.1, 1.9)
    value_weight = noise(splits[2], (D, FF), D ** -0.5, 0.1875, ((0, 16), (1, 16)))
    gate_weight = noise(splits[3], (D, FF), D ** -0.5, 0.1875, ((0, 16), (1, 16)))
    value_taps = noise(splits[4], (TAPS, FF), 0.6, 3.0, ((1, 16),), jnp.float32)
    gate_taps = noise(splits[5], (TAPS, FF), 0.6, 3.0, ((1, 16),), jnp.float32)
    down_weight = noise(splits[6], (FF, D), FF ** -0.5, 0.109375, ((0, 16), (1, 16)))
    norm_out = jnp.clip(1.0 + 0.18 * jax.random.normal(splits[7], (D,), jnp.float32), 0.1, 1.9)
    return dict(tokens=tokens, norm_in=norm_in, value_weight=value_weight, gate_weight=gate_weight, value_taps=value_taps, gate_taps=gate_taps, down_weight=down_weight, norm_out=norm_out)


norm_eps = 1e-06

def normalize(values, scale):
    wide = values.astype(jnp.float32)
    power = lax.optimization_barrier(jnp.mean(wide * wide, axis=-1, keepdims=True))
    return (wide * jax.lax.rsqrt(power + norm_eps) * scale).astype(jnp.bfloat16)

def causal_conv(signal, taps):
    length = signal.shape[0]
    padded = jnp.pad(signal.astype(jnp.float32), ((2, 0), (0, 0)))
    result = padded[0:length] * taps[0]
    result = result + padded[1:length + 1] * taps[1]
    result = result + padded[2:length + 2] * taps[2]
    return result

def reference(tokens, norm_in, value_weight, gate_weight, value_taps, gate_taps, down_weight, norm_out):
    normed = normalize(tokens, norm_in)
    value = jnp.dot(normed, value_weight, preferred_element_type=jnp.float32).astype(jnp.bfloat16)
    gate = jnp.dot(normed, gate_weight, preferred_element_type=jnp.float32).astype(jnp.bfloat16)
    conv_value = causal_conv(value, value_taps)
    conv_gate = causal_conv(gate, gate_taps)
    hidden = (jax.nn.gelu(conv_gate, approximate=True) * conv_value).astype(jnp.bfloat16)
    projected = jnp.dot(hidden, down_weight, preferred_element_type=jnp.float32)
    return normalize(projected, norm_out)
```

```python
import jax
import jax.numpy as jnp
from jax import lax
from jax.experimental import pallas as pl
from jax.experimental.pallas import tpu as pltpu
from jax.sharding import Mesh
from jax.sharding import PartitionSpec as P

FS = ("y", "x")
TP = ("z", "c")
ALL = ("y", "x", "z", "c")
NY, NX, NZ, NC = 4, 4, 8, 2
EPS = 1e-06
HALO = 16
MB = 1024 * 1024


def moved(array, target):
    pairs = []
    for y in range(NY):
        for x in range(NX):
            for z in range(NZ):
                for c in range(NC):
                    to = target(y, x, z, c)
                    if to is None:
                        continue
                    source = ((y * NX + x) * NZ + z) * NC + c
                    ty, tx, tz, tc = to
                    pairs.append((source, ((ty * NX + tx) * NZ + tz) * NC + tc))
    return lax.ppermute(array, ALL, pairs)


def groups_by(k):
    return lambda y, x, z, c: (y, x, (z + 2 * k) % NZ, c)


def first_by(k):
    return lambda y, x, z, c: (y, (x + k) % NX, z, c) if c == 0 else ((y + k) % NY, x, z, c)


def second_by(k):
    return lambda y, x, z, c: ((y + k) % NY, x, z, c) if c == 0 else (y, (x + k) % NX, z, c)


def other_core(y, x, z, c):
    return (y, x, z, 1 - c)


def other_chip(y, x, z, c):
    return (y, x, z ^ 1, c)


def next_group(y, x, z, c):
    at = ((y * NX + x) * NZ + z) * NC + c + 4
    if at >= NY * NX * NZ * NC:
        return None
    return (at // (NX * NZ * NC), at // (NZ * NC) % NX, at // NC % NZ, at % NC)


def ring_of_four(block, by):
    half = block.shape[0] // 2
    before = moved(block, by(1))
    after = moved(block, by(-1))
    top = moved(before[:half], by(1))
    bottom = moved(after[half:], by(-1))
    return block, before, after, top, bottom


def vmem_call(body, out_shape, flops, *, scratch=(), scalars=0, operands=0, limit=16, nbytes=4 * MB):
    specs = [pl.BlockSpec(memory_space=pltpu.SMEM)] * scalars + [pl.BlockSpec(memory_space=pltpu.VMEM)] * operands
    many = isinstance(out_shape, (tuple, list))
    outs = [pl.BlockSpec(memory_space=pltpu.VMEM)] * len(out_shape) if many else pl.BlockSpec(memory_space=pltpu.VMEM)
    return pl.pallas_call(
        body,
        out_shape=out_shape,
        in_specs=specs,
        out_specs=outs,
        scratch_shapes=list(scratch),
        compiler_params=pltpu.CompilerParams(vmem_limit_bytes=limit * MB),
        cost_estimate=pl.CostEstimate(flops=flops, bytes_accessed=nbytes, transcendentals=0),
    )


def normed_rows(wide, scale):
    power = jnp.mean(wide * wide, axis=-1, keepdims=True)
    return (wide * lax.rsqrt(power + EPS) * scale).astype(jnp.bfloat16)


def norm_body(tokens, scale, out):
    out[...] = normed_rows(tokens[...].astype(jnp.float32), scale[...])


def final_body(own, near, far, scale, out):
    total = own[...] + near[...].astype(jnp.float32) + far[...].astype(jnp.float32)
    out[...] = normed_rows(total, scale[...])


def place(scratch, offsets, base, pieces):
    at = base
    for piece in pieces:
        for row in range(0, piece.shape[0], 64):
            where = pl.multiple_of(offsets[at], 64)
            scratch[pl.ds(where, 64), :] = piece[row : row + 64, :]
            at += 1


def gelu(v):
    inner = v * (0.7978845608028654 + 0.035677408136300125 * (v * v))
    return 0.5 * v * (1.0 + jnp.tanh(inner))


GROUPS = ((0, 512, 256), (512, 512, 256), (1024, 384, 192))


def up_body(offsets, halo, own, chip, core, w0, w1, w2, w3, w4, taps, out, x_all, w_all, acc):
    x_all[0:HALO, :] = halo[...]
    for k, ref, row in ((0, own, 0), (1, chip, 0), (2, core, 0), (3, core, 256)):
        where = pl.multiple_of(HALO + offsets[16 + k], 16)
        x_all[pl.ds(where, 256), :] = ref[row : row + 256, :]
    place(w_all, offsets, 0, (w0, w1, w2, w3, w4))
    rows = 64
    for number, (start, width, half) in enumerate(GROUPS):
        acc[:, 0:width] = jnp.dot(x_all[...], w_all[:, start : start + width], preferred_element_type=jnp.float32)
        scale = taps[:, start : start + width]

        def chunk(i, carry, start=start, width=width, number=number, scale=scale):
            r0 = pl.multiple_of(i * rows, rows)
            near = acc[pl.ds(r0, rows + HALO), 0:width]
            conv = near[14 : 14 + rows] * scale[0:1]
            conv = conv + near[15 : 15 + rows] * scale[1:2]
            conv = conv + near[16 : 16 + rows] * scale[2:3]
            if number < 2:
                hidden = gelu(conv[:, 256:512]) * conv[:, 0:256]
                out[pl.ds(r0, rows), number * 256 : number * 256 + 256] = hidden.astype(jnp.bfloat16)
            else:
                hidden = gelu(conv[:, 128:256]) * conv[:, 0:128]
                out[pl.ds(r0, rows), 512:640] = hidden.astype(jnp.bfloat16)
                tail = conv[:, 256:384]
                hidden = gelu(pltpu.roll(tail, 64, 1)) * tail
                lane = lax.broadcasted_iota(jnp.int32, hidden.shape, 1)
                hidden = jnp.where(lane < 64, hidden, 0.0)
                out[pl.ds(r0, rows), 640:768] = hidden.astype(jnp.bfloat16)
            return carry

        lax.fori_loop(0, 1024 // rows, chunk, 0)


def down_body(offsets, hidden, d0, d1, d2, d3, d4, send_far, send_near, keep_far, keep_near, d_all):
    place(d_all, offsets, 0, (d0, d1, d2, d3, d4))

    def product(k):
        where = pl.multiple_of(offsets[16 + k], 256)
        return lax.dot_general(
            hidden[pl.ds(where, 256), :], d_all[...], (((1,), (1,)), ((), ())), preferred_element_type=jnp.float32
        )

    send_far[...] = product(3).astype(jnp.bfloat16)
    send_near[...] = product(2).astype(jnp.bfloat16)
    keep_far[...] = product(1)
    keep_near[...] = product(0)


def three_parts(values):
    high = lax.reduce_precision(values, 8, 7)
    rest = values - high
    middle = lax.reduce_precision(rest, 8, 7)
    low = rest - middle
    return [p.reshape(1, -1).astype(jnp.bfloat16) for p in (high, middle, low)]


def shards(tokens, norm_in, value_weight, gate_weight, value_taps, gate_taps, down_weight, norm_out):
    f32, bf16 = jnp.float32, jnp.bfloat16
    y, x, z, c = (lax.axis_index(name) for name in ALL)
    width = value_weight.shape[1]

    top = jnp.concatenate([value_weight, gate_weight, down_weight.T], axis=1)
    taps = jnp.concatenate(three_parts(value_taps) + three_parts(gate_taps), axis=0)
    pack = jnp.concatenate([top, taps, jnp.zeros((80 - 64 - 6, 3 * width), bf16)], axis=0)
    p0, p1, p2, p3, p4 = ring_of_four(pack, groups_by)
    packs = (p0, p1, p2, jnp.concatenate([p3, p4], axis=0))

    def columns(k, rows):
        return jnp.concatenate([p[rows, k * width : (k + 1) * width] for p in packs], axis=1)

    def arranged(v, g):
        return [v[:, 0:256], g[:, 0:256], v[:, 256:512], g[:, 256:512], v[:, 512:640], g[:, 512:640], v[:, 640:704], g[:, 640:704]]

    def whole_taps(first):
        rows = []
        for tap in range(3):
            parts = [columns(tap, slice(64 + first + k, 65 + first + k)).astype(f32) for k in range(3)]
            rows.append((parts[0] + parts[1]) + parts[2])
        return jnp.concatenate(rows, axis=0)

    real = slice(0, 64)
    value = columns(0, real)
    gate = columns(1, real)
    down = columns(2, real)
    both = jnp.concatenate(arranged(value, gate) + [down, jnp.zeros((64, 64), bf16)], axis=1)
    tap_rows = jnp.concatenate(arranged(whole_taps(0), whole_taps(3)), axis=1)
    tap_rows = jnp.concatenate([tap_rows, jnp.zeros((5, tap_rows.shape[1]), f32)], axis=0)

    line = jnp.concatenate(ring_of_four(both, first_by), axis=0)
    ups = ring_of_four(line[:, :1408], second_by)
    downs = ring_of_four(line[:, 1408:], second_by)

    steps = jnp.array([0, -1, 1, 2], jnp.int32)
    mine, across = jnp.where(c == 0, x, y), jnp.where(c == 0, y, x)
    near = (mine + steps) % 4
    far = (across + steps) % 4
    place_near, place_far = jnp.where(c == 0, 1, 4), jnp.where(c == 0, 4, 1)
    blocks = (far[:, None] * place_far + near[None, :] * place_near).reshape(-1) * 64
    zb = z % 2
    rows_of = jnp.stack([zb * 2 + c, (1 - zb) * 2 + c, zb * 2 + 1 - c, (1 - zb) * 2 + 1 - c]) * 256
    offsets = jnp.concatenate([blocks, rows_of]).astype(jnp.int32)

    normed = vmem_call(norm_body, jax.ShapeDtypeStruct(tokens.shape, bf16), 2 * MB, operands=2)(tokens, norm_in.reshape(1, -1))
    chip = moved(normed, other_chip)
    core = moved(jnp.concatenate([normed, chip], axis=0), other_core)
    last = jnp.where(
        zb == 1,
        jnp.where(c == 1, normed[-HALO:], core[256 - HALO : 256]),
        jnp.where(c == 1, chip[-HALO:], core[-HALO:]),
    )
    halo = moved(last, next_group)

    hidden = vmem_call(
        up_body,
        jax.ShapeDtypeStruct((1024, 768), bf16),
        2 * 1040 * 1024 * 1408,
        scalars=1,
        operands=10,
        limit=24,
        scratch=(pltpu.VMEM((1040, 1024), bf16), pltpu.VMEM((1024, 1408), bf16), pltpu.VMEM((1040, 512), f32)),
    )(offsets, halo, normed, chip, core, *ups, tap_rows)

    block = (256, 1024)
    send_far, send_near, keep_far, keep_near = vmem_call(
        down_body,
        [jax.ShapeDtypeStruct(block, bf16)] * 2 + [jax.ShapeDtypeStruct(block, f32)] * 2,
        2 * 1024 * 768 * 1024,
        scalars=1,
        operands=6,
        limit=20,
        scratch=(pltpu.VMEM((1024, 768), bf16),),
    )(offsets, hidden, *downs)
    got_far = moved(send_far, other_core)
    got_near = moved(send_near, other_core)
    sent = (keep_far + got_far.astype(f32)).astype(bf16)
    back = moved(sent, other_chip)
    return vmem_call(final_body, jax.ShapeDtypeStruct(block, bf16), 2 * MB, operands=4)(
        keep_near, got_near, back, norm_out.reshape(1, -1)
    )


def solution(mesh):
    split = Mesh(mesh.devices.reshape(NY, NX, NZ, NC), ALL)
    return jax.shard_map(
        shards,
        mesh=split,
        in_specs=(P(ALL, None), P(), P(FS, TP), P(FS, TP), P(None, TP), P(None, TP), P(TP, FS), P()),
        out_specs=P(ALL, None),
        check_vma=False,
    )
```

```python
import jax
import jax.numpy as jnp
from jax import lax
from jax.experimental import pallas as pl
from jax.experimental.pallas import tpu as pltpu
from jax.sharding import Mesh
from jax.sharding import PartitionSpec as P

FS = ("y", "x")
TP = ("z", "c")
ALL = ("y", "x", "z", "c")
NY, NX, NZ, NC = 4, 4, 8, 2
EPS = 1e-06
HALO = 16
MB = 1024 * 1024


def moved(array, target):
    pairs = []
    for y in range(NY):
        for x in range(NX):
            for z in range(NZ):
                for c in range(NC):
                    to = target(y, x, z, c)
                    if to is None:
                        continue
                    source = ((y * NX + x) * NZ + z) * NC + c
                    ty, tx, tz, tc = to
                    pairs.append((source, ((ty * NX + tx) * NZ + tz) * NC + tc))
    return lax.ppermute(array, ALL, pairs)


def groups_by(k):
    return lambda y, x, z, c: (y, x, (z + 2 * k) % NZ, c)


def first_by(k):
    return lambda y, x, z, c: (y, (x + k) % NX, z, c) if c == 0 else ((y + k) % NY, x, z, c)


def second_by(k):
    return lambda y, x, z, c: ((y + k) % NY, x, z, c) if c == 0 else (y, (x + k) % NX, z, c)


def other_core(y, x, z, c):
    return (y, x, z, 1 - c)


def other_chip(y, x, z, c):
    return (y, x, z ^ 1, c)


def next_group(y, x, z, c):
    at = ((y * NX + x) * NZ + z) * NC + c + 4
    if at >= NY * NX * NZ * NC:
        return None
    return (at // (NX * NZ * NC), at // (NZ * NC) % NX, at // NC % NZ, at % NC)


def ring_of_four(block, by):
    half = block.shape[0] // 2
    before = moved(block, by(1))
    after = moved(block, by(-1))
    top = moved(before[:half], by(1))
    bottom = moved(after[half:], by(-1))
    return block, before, after, top, bottom


def vmem_call(body, out_shape, flops, *, scratch=(), scalars=0, operands=0, limit=16, nbytes=4 * MB):
    specs = [pl.BlockSpec(memory_space=pltpu.SMEM)] * scalars + [pl.BlockSpec(memory_space=pltpu.VMEM)] * operands
    many = isinstance(out_shape, (tuple, list))
    outs = [pl.BlockSpec(memory_space=pltpu.VMEM)] * len(out_shape) if many else pl.BlockSpec(memory_space=pltpu.VMEM)
    return pl.pallas_call(
        body,
        out_shape=out_shape,
        in_specs=specs,
        out_specs=outs,
        scratch_shapes=list(scratch),
        compiler_params=pltpu.CompilerParams(vmem_limit_bytes=limit * MB),
        cost_estimate=pl.CostEstimate(flops=flops, bytes_accessed=nbytes, transcendentals=0),
    )


def normed_rows(wide, scale):
    power = jnp.mean(wide * wide, axis=-1, keepdims=True)
    return (wide * lax.rsqrt(power + EPS) * scale).astype(jnp.bfloat16)


def norm_body(tokens, scale, gate, out):
    out[...] = normed_rows(tokens[...].astype(jnp.float32), scale[...])


def final_body(own, near, far, scale, out):
    total = own[...] + near[...].astype(jnp.float32) + far[...].astype(jnp.float32)
    out[...] = normed_rows(total, scale[...])


def place(scratch, offsets, base, pieces):
    at = base
    for piece in pieces:
        for row in range(0, piece.shape[0], 64):
            where = pl.multiple_of(offsets[at], 64)
            scratch[pl.ds(where, 64), :] = piece[row : row + 64, :]
            at += 1


def gelu(v):
    inner = v * (0.7978845608028654 + 0.035677408136300125 * (v * v))
    return 0.5 * v * (1.0 + jnp.tanh(inner))


GROUPS = ((0, 512, 256), (512, 512, 256), (1024, 384, 192))


def up_body(offsets, halo, own, chip, core, w0, w1, w2, w3, w4, taps, out, x_all, w_all, acc):
    x_all[0:HALO, :] = halo[...]
    for k, ref, row in ((0, own, 0), (1, chip, 0), (2, core, 0), (3, core, 256)):
        where = pl.multiple_of(HALO + offsets[16 + k], 16)
        x_all[pl.ds(where, 256), :] = ref[row : row + 256, :]
    place(w_all, offsets, 0, (w0, w1, w2, w3, w4))
    rows = 64
    for number, (start, width, half) in enumerate(GROUPS):
        acc[:, 0:width] = jnp.dot(x_all[...], w_all[:, start : start + width], preferred_element_type=jnp.float32)
        scale = taps[:, start : start + width]

        def chunk(i, carry, start=start, width=width, number=number, scale=scale):
            r0 = pl.multiple_of(i * rows, rows)
            near = acc[pl.ds(r0, rows + HALO), 0:width]
            conv = near[14 : 14 + rows] * scale[0:1]
            conv = conv + near[15 : 15 + rows] * scale[1:2]
            conv = conv + near[16 : 16 + rows] * scale[2:3]
            if number < 2:
                hidden = gelu(conv[:, 256:512]) * conv[:, 0:256]
                out[pl.ds(r0, rows), number * 256 : number * 256 + 256] = hidden.astype(jnp.bfloat16)
            else:
                hidden = gelu(conv[:, 128:256]) * conv[:, 0:128]
                out[pl.ds(r0, rows), 512:640] = hidden.astype(jnp.bfloat16)
                tail = conv[:, 256:384]
                hidden = gelu(pltpu.roll(tail, 64, 1)) * tail
                lane = lax.broadcasted_iota(jnp.int32, hidden.shape, 1)
                hidden = jnp.where(lane < 64, hidden, 0.0)
                out[pl.ds(r0, rows), 640:768] = hidden.astype(jnp.bfloat16)
            return carry

        lax.fori_loop(0, 1024 // rows, chunk, 0)


def down_body(offsets, hidden, d0, d1, d2, d3, d4, send_far, send_near, keep_far, keep_near, d_all):
    place(d_all, offsets, 0, (d0, d1, d2, d3, d4))

    def product(k):
        where = pl.multiple_of(offsets[16 + k], 256)
        return lax.dot_general(
            hidden[pl.ds(where, 256), :], d_all[...], (((1,), (1,)), ((), ())), preferred_element_type=jnp.float32
        )

    send_far[...] = product(3).astype(jnp.bfloat16)
    send_near[...] = product(2).astype(jnp.bfloat16)
    keep_far[...] = product(1)
    keep_near[...] = product(0)


PACK = 216


def three_parts(values):
    high = values.astype(jnp.bfloat16).astype(jnp.float32)
    rest = values - high
    middle = rest.astype(jnp.bfloat16).astype(jnp.float32)
    return [high, middle, rest - middle]


def pack_body(value, gate, down, value_taps, gate_taps, out):
    out[0:64, :] = value[...]
    out[64:128, :] = gate[...]
    out[128:192, :] = down[...]
    parts = three_parts(value_taps[...]) + three_parts(gate_taps[...])
    rows = jnp.concatenate(parts + [jnp.zeros((6, value.shape[1]), jnp.float32)], axis=0)
    out[192:PACK, :] = rows.astype(jnp.bfloat16)


def arranged(v, g):
    return jnp.concatenate(
        [v[:, 0:256], g[:, 0:256], v[:, 256:512], g[:, 256:512], v[:, 512:640], g[:, 512:640], v[:, 640:704], g[:, 640:704]],
        axis=1,
    )


def assemble_body(p0, p1, p2, p3, both, taps):
    packs = (p0, p1, p2, p3)

    def wide(row, count):
        return jnp.concatenate([p[row : row + count, :].astype(jnp.float32) for p in packs], axis=1)

    both[:, 0:1408] = arranged(wide(0, 64), wide(64, 64)).astype(jnp.bfloat16)
    down = jnp.concatenate([wide(128, 64), jnp.zeros((64, 64), jnp.float32)], axis=1)
    both[:, 1408:2176] = down.astype(jnp.bfloat16)
    parts = wide(192, 24)
    whole = [(parts[k : k + 3] + parts[k + 3 : k + 6]) + parts[k + 6 : k + 9] for k in (0, 9)]
    taps[...] = jnp.concatenate([arranged(*whole), jnp.zeros((5, 1408), jnp.float32)], axis=0)


def line_body(own, before, after, top, bottom, up, down):
    row = 0
    for piece in (own, before, after, top, bottom):
        count = piece.shape[0]
        up[row : row + count, :] = piece[:, 0:1408]
        down[row : row + count, :] = piece[:, 1408:2176]
        row += count


def shards(tokens, norm_in, value_weight, gate_weight, value_taps, gate_taps, down_weight, norm_out):
    f32, bf16 = jnp.float32, jnp.bfloat16
    y, x, z, c = (lax.axis_index(name) for name in ALL)
    width = value_weight.shape[1]

    pack = vmem_call(pack_body, jax.ShapeDtypeStruct((PACK, width), bf16), MB // 4, operands=5)(
        value_weight, gate_weight, down_weight.T, value_taps, gate_taps
    )
    before = moved(pack, groups_by(1))
    after = moved(pack, groups_by(-1))
    opposite = moved(
        jnp.where(c == 0, before, after), lambda y, x, z, c: groups_by(1 if c == 0 else -1)(y, x, z, c)
    )
    both, tap_rows = vmem_call(
        assemble_body, [jax.ShapeDtypeStruct((64, 2176), bf16), jax.ShapeDtypeStruct((8, 1408), f32)], MB, operands=4
    )(pack, before, after, opposite)

    up_line, down_line = vmem_call(
        line_body,
        [jax.ShapeDtypeStruct((256, 1408), bf16), jax.ShapeDtypeStruct((256, 768), bf16)],
        MB,
        operands=5,
    )(*ring_of_four(both, first_by))
    ups = ring_of_four(up_line, second_by)
    downs = ring_of_four(down_line, second_by)

    steps = jnp.array([0, -1, 1, 2], jnp.int32)
    mine, across = jnp.where(c == 0, x, y), jnp.where(c == 0, y, x)
    near = (mine + steps) % 4
    far = (across + steps) % 4
    place_near, place_far = jnp.where(c == 0, 1, 4), jnp.where(c == 0, 4, 1)
    blocks = (far[:, None] * place_far + near[None, :] * place_near).reshape(-1) * 64
    zb = z % 2
    rows_of = jnp.stack([zb * 2 + c, (1 - zb) * 2 + c, zb * 2 + 1 - c, (1 - zb) * 2 + 1 - c]) * 256
    offsets = jnp.concatenate([blocks, rows_of]).astype(jnp.int32)

    normed = vmem_call(norm_body, jax.ShapeDtypeStruct(tokens.shape, bf16), 2 * MB, operands=3)(
        tokens, norm_in.reshape(1, -1), opposite[:16]
    )
    chip = moved(normed, other_chip)
    core = moved(jnp.concatenate([normed, chip], axis=0), other_core)
    last = jnp.where(
        zb == 1,
        jnp.where(c == 1, normed[-HALO:], core[256 - HALO : 256]),
        jnp.where(c == 1, chip[-HALO:], core[-HALO:]),
    )
    halo = moved(last, next_group)

    hidden = vmem_call(
        up_body,
        jax.ShapeDtypeStruct((1024, 768), bf16),
        2 * 1040 * 1024 * 1408,
        scalars=1,
        operands=10,
        limit=24,
        scratch=(pltpu.VMEM((1040, 1024), bf16), pltpu.VMEM((1024, 1408), bf16), pltpu.VMEM((1040, 512), f32)),
    )(offsets, halo, normed, chip, core, *ups, tap_rows)

    block = (256, 1024)
    send_far, send_near, keep_far, keep_near = vmem_call(
        down_body,
        [jax.ShapeDtypeStruct(block, bf16)] * 2 + [jax.ShapeDtypeStruct(block, f32)] * 2,
        2 * 1024 * 768 * 1024,
        scalars=1,
        operands=6,
        limit=20,
        scratch=(pltpu.VMEM((1024, 768), bf16),),
    )(offsets, hidden, *downs)
    got_far = moved(send_far, other_core)
    got_near = moved(send_near, other_core)
    sent = (keep_far + got_far.astype(f32)).astype(bf16)
    back = moved(sent, other_chip)
    return vmem_call(final_body, jax.ShapeDtypeStruct(block, bf16), 2 * MB, operands=4)(
        keep_near, got_near, back, norm_out.reshape(1, -1)
    )


def solution(mesh):
    split = Mesh(mesh.devices.reshape(NY, NX, NZ, NC), ALL)
    return jax.shard_map(
        shards,
        mesh=split,
        in_specs=(P(ALL, None), P(), P(FS, TP), P(FS, TP), P(None, TP), P(None, TP), P(TP, FS), P()),
        out_specs=P(ALL, None),
        check_vma=False,
    )
```

```python
import jax
import jax.numpy as jnp
from jax import lax
from jax.experimental import pallas as pl
from jax.experimental.pallas import tpu as pltpu
from jax.sharding import Mesh
from jax.sharding import PartitionSpec as P


FS = ("y", "x")
TP = ("z", "c")
ALL = ("y", "x", "z", "c")
NY, NX, NZ, NC = 4, 4, 8, 2
EPS = 1e-06
HALO = 16
MB = 1024 * 1024


def moved(array, target):
    pairs = []
    for y in range(NY):
        for x in range(NX):
            for z in range(NZ):
                for c in range(NC):
                    to = target(y, x, z, c)
                    if to is None:
                        continue
                    source = ((y * NX + x) * NZ + z) * NC + c
                    ty, tx, tz, tc = to
                    pairs.append((source, ((ty * NX + tx) * NZ + tz) * NC + tc))
    return lax.ppermute(array, ALL, pairs)


def groups_by(k):
    return lambda y, x, z, c: (y, x, (z + 2 * k) % NZ, c)


def first_by(k):
    return lambda y, x, z, c: (y, (x + k) % NX, z, c) if c == 0 else ((y + k) % NY, x, z, c)


def second_by(k):
    return lambda y, x, z, c: ((y + k) % NY, x, z, c) if c == 0 else (y, (x + k) % NX, z, c)


def other_core(y, x, z, c):
    return (y, x, z, 1 - c)


def other_chip(y, x, z, c):
    return (y, x, z ^ 1, c)


def next_group(y, x, z, c):
    at = ((y * NX + x) * NZ + z) * NC + c + 4
    if at >= NY * NX * NZ * NC:
        return None
    return (at // (NX * NZ * NC), at // (NZ * NC) % NX, at // NC % NZ, at % NC)


def all_of_four(block, by):
    return block, moved(block, by(1)), moved(block, by(-1)), moved(block, by(2))


def ring_of_four(block, by):
    half = block.shape[0] // 2
    before = moved(block, by(1))
    after = moved(block, by(-1))
    top = moved(before[:half], by(1))
    bottom = moved(after[half:], by(-1))
    return block, before, after, top, bottom


VM = pl.BlockSpec(memory_space=pltpu.VMEM)
SM = pl.BlockSpec(memory_space=pltpu.SMEM)
ANY = pl.BlockSpec(memory_space=pl.ANY)


def call(body, ins, outs, specs, *, flops=MB, nbytes=MB, scratch=(), limit=16):
    return pl.pallas_call(
        body,
        out_shape=outs,
        in_specs=specs,
        out_specs=[VM] * len(outs),
        scratch_shapes=list(scratch),
        compiler_params=pltpu.CompilerParams(vmem_limit_bytes=limit * MB),
        cost_estimate=pl.CostEstimate(flops=flops, bytes_accessed=nbytes, transcendentals=0),
    )(*ins)


def sds(shape, dtype=jnp.bfloat16):
    return jax.ShapeDtypeStruct(shape, dtype)


def normed_rows(wide, scale):
    power = jnp.mean(wide * wide, axis=-1, keepdims=True)
    return wide * lax.rsqrt(power + EPS) * scale


def turned(wide):
    blocks = [wide[:, (y * NX + x) * 64 : (y * NX + x + 1) * 64] for x in range(NX) for y in range(NY)]
    return jnp.concatenate(blocks, axis=1)


def norm_body(spots, tokens, scale, out):
    rows = normed_rows(tokens[...].astype(jnp.float32), scale[...])

    @pl.when(spots[24] == 0)
    def _():
        out[...] = rows.astype(jnp.bfloat16)

    @pl.when(spots[24] == 1)
    def _():
        out[...] = turned(rows).astype(jnp.bfloat16)


def stack_body(own, chip, out):
    out[0:256, :] = turned(own[...].astype(jnp.float32)).astype(jnp.bfloat16)
    out[256:512, :] = turned(chip[...].astype(jnp.float32)).astype(jnp.bfloat16)


def last_body(spots, own, chip, core, out):
    for k, ref, row in ((0, own, 240), (1, chip, 240), (2, core, 240), (3, core, 496)):

        @pl.when(spots[16 + k] == 768)
        def _(ref=ref, row=row):
            out[...] = ref[row : row + HALO, :]


def rows_body(spots, halo, own, chip, core, out):
    out[0:HALO, :] = halo[...]
    for k, ref, row in ((0, own, 0), (1, chip, 0), (2, core, 0), (3, core, 256)):
        where = pl.multiple_of(HALO + spots[16 + k], 16)
        out[pl.ds(where, 256), :] = ref[row : row + 256, :]


def final_body(own, near, far, scale, out):
    total = own[...] + near[...].astype(jnp.float32) + far[...].astype(jnp.float32)
    out[...] = normed_rows(total, scale[...]).astype(jnp.bfloat16)


PACK = 216


def three_parts(values):
    high = values.astype(jnp.bfloat16).astype(jnp.float32)
    rest = values - high
    middle = rest.astype(jnp.bfloat16).astype(jnp.float32)
    return [high, middle, rest - middle]


def pack_body(weights, taps, out):
    out[0:192, :] = weights[...]
    parts = three_parts(taps[0:3, :]) + three_parts(taps[3:6, :])
    rows = jnp.concatenate(parts + [jnp.zeros((6, out.shape[1]), jnp.float32)], axis=0)
    out[192:PACK, :] = rows.astype(jnp.bfloat16)


def arranged(v, g):
    return jnp.concatenate(
        [v[:, 0:256], g[:, 0:256], v[:, 256:512], g[:, 256:512], v[:, 512:640], g[:, 512:640], v[:, 640:704], g[:, 640:704]],
        axis=1,
    )


def assemble_body(p0, p1, p2, p3, both, taps):
    packs = (p0, p1, p2, p3)

    def wide(row, count):
        return jnp.concatenate([p[row : row + count, :].astype(jnp.float32) for p in packs], axis=1)

    both[:, 0:1408] = arranged(wide(0, 64), wide(64, 64)).astype(jnp.bfloat16)
    down = jnp.concatenate([wide(128, 64), jnp.zeros((64, 64), jnp.float32)], axis=1)
    both[:, 1408:2176] = down.astype(jnp.bfloat16)
    parts = wide(192, 24)
    whole = [(parts[k : k + 3] + parts[k + 3 : k + 6]) + parts[k + 6 : k + 9] for k in (0, 9)]
    taps[...] = jnp.concatenate([arranged(*whole), jnp.zeros((5, 1408), jnp.float32)], axis=0)


def line_body(spots, b0, b1, b2, b3, up, down):
    for k, piece in enumerate((b0, b1, b2, b3)):
        where = pl.multiple_of(spots[20 + k], 64)
        up[pl.ds(where, 64), :] = piece[:, 0:1408]
        down[pl.ds(where, 64), :] = piece[:, 1408:2176]


def gelu(v):
    inner = v * (0.7978845608028654 + 0.035677408136300125 * (v * v))
    return 0.5 * v * (1.0 + jnp.tanh(inner))


GROUPS = ((0, 512), (512, 512), (1024, 384))


def begin_body(spots, x_rows, w0, w1, w2, acc, x_some, w_some):
    for k, piece in enumerate((w0, w1, w2)):
        where = pl.multiple_of(spots[25 + k], 256)
        x_some[:, k * 256 : k * 256 + 256] = x_rows[:, pl.ds(where, 256)]
        w_some[k * 256 : k * 256 + 256, :] = piece[...]
    for start, width in GROUPS:
        columns = slice(start, start + width)
        acc[:, columns] = jnp.dot(x_some[...], w_some[:, columns], preferred_element_type=jnp.float32)


def down_body(spots, d0, d1, d2, d3, d4, gate, out):
    at = 0
    for piece in (d0, d1, d2, d3, d4):
        for row in range(0, piece.shape[0], 64):
            where = pl.multiple_of(spots[at], 64)
            out[pl.ds(where, 64), :] = piece[row : row + 64, :]
            at += 1


def end_body(block, spots, x_rows, acc, w3, w4, taps, d_all, gate, out, w_some, full, hidden):
    w_some[0:128, :] = w3[...]
    w_some[128:256, :] = w4[...]
    r0 = pl.multiple_of(spots[16 + block], 256)
    where = pl.multiple_of(spots[28], 256)
    x_some = x_rows[pl.ds(r0, 256 + HALO), pl.ds(where, 256)]
    for number, (start, width) in enumerate(GROUPS):
        columns = slice(start, start + width)
        full[:, columns] = acc[pl.ds(r0, 256 + HALO), columns] + jnp.dot(
            x_some, w_some[:, columns], preferred_element_type=jnp.float32
        )
        scale = taps[:, columns]
        for row in range(0, 256, 64):
            near = full[row : row + 64 + HALO, columns]
            conv = near[14 : 14 + 64] * scale[0:1]
            conv = conv + near[15 : 15 + 64] * scale[1:2]
            conv = conv + near[16 : 16 + 64] * scale[2:3]
            some = slice(row, row + 64)
            if number < 2:
                made = gelu(conv[:, 256:512]) * conv[:, 0:256]
                hidden[some, number * 256 : number * 256 + 256] = made.astype(jnp.bfloat16)
            else:
                made = gelu(conv[:, 128:256]) * conv[:, 0:128]
                hidden[some, 512:640] = made.astype(jnp.bfloat16)
                tail = conv[:, 256:384]
                made = gelu(pltpu.roll(tail, 64, 1)) * tail
                lane = lax.broadcasted_iota(jnp.int32, made.shape, 1)
                hidden[some, 640:768] = jnp.where(lane < 64, made, 0.0).astype(jnp.bfloat16)
    product = lax.dot_general(
        hidden[...], d_all[...], (((1,), (1,)), ((), ())), preferred_element_type=jnp.float32
    )
    out[...] = product.astype(out.dtype)


def shards(tokens, norm_in, value_weight, gate_weight, value_taps, gate_taps, down_weight, norm_out):
    f32 = jnp.float32
    y, x, z, c = (lax.axis_index(name) for name in ALL)
    width = value_weight.shape[1]

    mine, across = jnp.where(c == 0, x, y), jnp.where(c == 0, y, x)
    near = [(mine + k) % 4 for k in (0, 3, 1, 2)]
    far = [(across + k) % 4 for k in (0, 3, 1, 2)]
    place_near, place_far = jnp.where(c == 0, 64, 256), jnp.where(c == 0, 256, 64)
    zb = z % 2
    blocks = [f * place_far + n * place_near for f in far for n in range(4)]
    members = [zb * 2 + c, (1 - zb) * 2 + c, zb * 2 + 1 - c, (1 - zb) * 2 + 1 - c]
    spots = jnp.stack(
        [b.astype(jnp.int32) for b in blocks + [m * 256 for m in members] + [n * 64 for n in near] + [c] + [f * 256 for f in far]]
    )

    (pack,) = call(
        pack_body,
        (
            jnp.concatenate([value_weight, gate_weight, down_weight.T], axis=0),
            jnp.concatenate([value_taps, gate_taps], axis=0),
        ),
        [sds((PACK, width))],
        [VM] * 2,
    )
    packs = all_of_four(pack, groups_by)
    both, tap_rows = call(assemble_body, packs, [sds((64, 2176)), sds((8, 1408), f32)], [VM] * 4)
    up_line, down_line = call(
        line_body, (spots, *all_of_four(both, first_by)), [sds((256, 1408)), sds((256, 768))], [SM] + [VM] * 4
    )
    ups = ring_of_four(up_line, second_by)
    downs = ring_of_four(down_line, second_by)

    (normed,) = call(
        norm_body, (spots, tokens, norm_in.reshape(1, -1)), [sds(tokens.shape)], [SM, VM, VM]
    )
    chip = moved(normed, other_chip)
    (stacked,) = call(stack_body, (normed, chip), [sds((512, 1024))], [VM, VM])
    core = moved(stacked, other_core)
    (last,) = call(last_body, (spots, normed, chip, core), [sds((HALO, 1024))], [SM, VM, VM, VM])
    halo = moved(last, next_group)
    (x_rows,) = call(rows_body, (spots, halo, normed, chip, core), [sds((1024 + HALO, 1024))], [SM] + [VM] * 4)

    (acc,) = call(
        begin_body,
        (spots, x_rows, *ups[:3]),
        [sds((1024 + HALO, 1408), f32)],
        [SM] + [VM] * 4,
        flops=2 * 1040 * 768 * 1408,
        nbytes=8 * MB,
        limit=16,
        scratch=(pltpu.VMEM((1024 + HALO, 768), jnp.bfloat16), pltpu.VMEM((768, 1408), jnp.bfloat16)),
    )
    (d_all,) = call(down_body, (spots, *downs, acc), [sds((1024, 768))], [SM] + [VM] * 5 + [ANY])

    def end(block, dtype, gate):
        def body(*refs):
            end_body(block, *refs)

        (out,) = call(
            body,
            (spots, x_rows, acc, ups[3], ups[4], tap_rows, d_all, gate),
            [sds((256, 1024), dtype)],
            [SM] + [VM] * 6 + [ANY],
            flops=2 * 272 * 256 * 1408 + 2 * 256 * 768 * 1024,
            nbytes=4 * MB,
            limit=16,
            scratch=(
                pltpu.VMEM((256, 1408), jnp.bfloat16),
                pltpu.VMEM((256 + HALO, 1408), f32),
                pltpu.VMEM((256, 768), jnp.bfloat16),
            ),
        )
        return out

    first = end(3, jnp.bfloat16, d_all)
    got_far = moved(first, other_core)
    second = end(1, f32, first)
    sent = (second + got_far.astype(f32)).astype(jnp.bfloat16)
    back = moved(sent, other_chip)
    third = end(2, jnp.bfloat16, sent)
    got_near = moved(third, other_core)
    fourth = end(0, f32, third)
    (out,) = call(final_body, (fourth, got_near, back, norm_out.reshape(1, -1)), [sds((256, 1024))], [VM] * 4)
    return out


def solution(mesh):
    split = Mesh(mesh.devices.reshape(NY, NX, NZ, NC), ALL)
    return jax.shard_map(
        shards,
        mesh=split,
        in_specs=(P(ALL, None), P(), P(FS, TP), P(FS, TP), P(None, TP), P(None, TP), P(TP, FS), P()),
        out_specs=P(ALL, None),
        check_vma=False,
    )
```

```python
import jax
import jax.numpy as jnp
from jax import lax
from jax.experimental import pallas as pl
from jax.experimental.pallas import tpu as pltpu
from jax.sharding import Mesh
from jax.sharding import PartitionSpec as P


FS = ("y", "x")
TP = ("z", "c")
ALL = ("y", "x", "z", "c")
NY, NX, NZ, NC = 4, 4, 8, 2
EPS = 1e-06
HALO = 16
MB = 1024 * 1024


def moved(array, target):
    pairs = []
    for y in range(NY):
        for x in range(NX):
            for z in range(NZ):
                for c in range(NC):
                    to = target(y, x, z, c)
                    if to is None:
                        continue
                    source = ((y * NX + x) * NZ + z) * NC + c
                    ty, tx, tz, tc = to
                    pairs.append((source, ((ty * NX + tx) * NZ + tz) * NC + tc))
    return lax.ppermute(array, ALL, pairs)


def quarter_to(k):
    def target(y, x, z, c):
        up = (z + k) % 2 == 0
        return (y, x, (z + k if up else z - k) % NZ, c)

    return target


def first_by(k):
    return lambda y, x, z, c: (y, (x + k) % NX, z, c) if c == 0 else ((y + k) % NY, x, z, c)


def second_by(k):
    return lambda y, x, z, c: ((y + k) % NY, x, z, c) if c == 0 else (y, (x + k) % NX, z, c)


def other_core(y, x, z, c):
    return (y, x, z, 1 - c)


def other_chip(y, x, z, c):
    return (y, x, z ^ 1, c)


def next_group(y, x, z, c):
    at = ((y * NX + x) * NZ + z) * NC + c + 4
    if at >= NY * NX * NZ * NC:
        return None
    return (at // (NX * NZ * NC), at // (NZ * NC) % NX, at // NC % NZ, at % NC)


def all_of_four(block, by):
    return block, moved(block, by(1)), moved(block, by(-1)), moved(block, by(2))


def ring_of_four(block, by):
    half = block.shape[0] // 2
    before = moved(block, by(1))
    after = moved(block, by(-1))
    top = moved(before[:half], by(1))
    bottom = moved(after[half:], by(-1))
    return block, before, after, top, bottom


VM = pl.BlockSpec(memory_space=pltpu.VMEM)
SM = pl.BlockSpec(memory_space=pltpu.SMEM)
ANY = pl.BlockSpec(memory_space=pl.ANY)


def call(body, ins, outs, specs, *, flops=MB, nbytes=MB, scratch=(), limit=16):
    return pl.pallas_call(
        body,
        out_shape=outs,
        in_specs=specs,
        out_specs=[VM] * len(outs),
        scratch_shapes=list(scratch),
        compiler_params=pltpu.CompilerParams(vmem_limit_bytes=limit * MB),
        cost_estimate=pl.CostEstimate(flops=flops, bytes_accessed=nbytes, transcendentals=0),
    )(*ins)


def sds(shape, dtype=jnp.bfloat16):
    return jax.ShapeDtypeStruct(shape, dtype)


def normed_rows(wide, scale):
    power = jnp.mean(wide * wide, axis=-1, keepdims=True)
    return wide * lax.rsqrt(power + EPS) * scale


def turned(wide):
    blocks = [wide[:, (y * NX + x) * 64 : (y * NX + x + 1) * 64] for x in range(NX) for y in range(NY)]
    return jnp.concatenate(blocks, axis=1)


def norm_body(spots, tokens, scale, out):
    rows = normed_rows(tokens[...].astype(jnp.float32), scale[...])

    @pl.when(spots[24] == 0)
    def _():
        out[...] = rows.astype(jnp.bfloat16)

    @pl.when(spots[24] == 1)
    def _():
        out[...] = turned(rows).astype(jnp.bfloat16)


def stack_body(own, chip, out):
    out[0:256, :] = turned(own[...].astype(jnp.float32)).astype(jnp.bfloat16)
    out[256:512, :] = turned(chip[...].astype(jnp.float32)).astype(jnp.bfloat16)


def last_body(spots, own, chip, core, out):
    for k, ref, row in ((0, own, 240), (1, chip, 240), (2, core, 240), (3, core, 496)):

        @pl.when(spots[16 + k] == 768)
        def _(ref=ref, row=row):
            out[...] = ref[row : row + HALO, :]


def rows_body(spots, halo, own, chip, core, out):
    out[0:HALO, :] = halo[...]
    for k, ref, row in ((0, own, 0), (1, chip, 0), (2, core, 0), (3, core, 256)):
        where = pl.multiple_of(HALO + spots[16 + k], 16)
        out[pl.ds(where, 256), :] = ref[row : row + 256, :]


def final_body(own, near, far, scale, out):
    total = own[...] + near[...].astype(jnp.float32) + far[...].astype(jnp.float32)
    out[...] = normed_rows(total, scale[...]).astype(jnp.bfloat16)


PACK = 344


def three_parts(values):
    high = values.astype(jnp.bfloat16).astype(jnp.float32)
    rest = values - high
    middle = rest.astype(jnp.bfloat16).astype(jnp.float32)
    return [high, middle, rest - middle]


def pack_body(weights, taps, out):
    f32, bf16 = jnp.float32, jnp.bfloat16
    parts = three_parts(taps[0:3, :]) + three_parts(taps[3:6, :])
    rows = jnp.concatenate(parts + [jnp.zeros((6, 176), f32)], axis=0)
    rest = weights[:, 128:176].astype(f32)
    out[0:192, :] = weights[:, 0:128]
    out[320:344, :] = rows[:, 0:128].astype(bf16)
    pair = jnp.concatenate([rest[0:64], rest[64:128], jnp.zeros((64, 32), f32)], axis=1)
    out[192:256, :] = pair.astype(bf16)
    more = jnp.concatenate([rows[:, 128:176], jnp.zeros((40, 48), f32)], axis=0)
    gap = jnp.zeros((64, 16), f32)
    out[256:320, :] = jnp.concatenate([rest[128:192], gap, more, gap], axis=1).astype(bf16)


def arranged(v, g):
    return jnp.concatenate(
        [v[:, 0:256], g[:, 0:256], v[:, 256:512], g[:, 256:512], v[:, 512:640], g[:, 512:640], v[:, 640:704], g[:, 640:704]],
        axis=1,
    )


def assemble_body(p0, p1, p2, p3, both, taps):
    f32 = jnp.float32

    def wide(row, other, lane, count=64):
        pieces = []
        for p in (p0, p1, p2, p3):
            pieces.append(p[row : row + count, :].astype(f32))
            pieces.append(p[other : other + count, :].astype(f32)[:, lane : lane + 48])
        return jnp.concatenate(pieces, axis=1)

    both[:, 0:1408] = arranged(wide(0, 192, 0), wide(64, 192, 48)).astype(jnp.bfloat16)
    down = jnp.concatenate([wide(128, 256, 0), jnp.zeros((64, 64), f32)], axis=1)
    both[:, 1408:2176] = down.astype(jnp.bfloat16)
    parts = wide(320, 256, 64, 24)
    whole = [(parts[k : k + 3] + parts[k + 3 : k + 6]) + parts[k + 6 : k + 9] for k in (0, 9)]
    taps[...] = jnp.concatenate([arranged(*whole), jnp.zeros((5, 1408), f32)], axis=0)


def line_body(spots, b0, b1, b2, b3, up, down):
    for k, piece in enumerate((b0, b1, b2, b3)):
        where = pl.multiple_of(spots[20 + k], 64)
        up[pl.ds(where, 64), :] = piece[:, 0:1408]
        down[pl.ds(where, 64), :] = piece[:, 1408:2176]


def gelu(v):
    inner = v * (0.7978845608028654 + 0.035677408136300125 * (v * v))
    return 0.5 * v * (1.0 + jnp.tanh(inner))


GROUPS = ((0, 512), (512, 512), (1024, 384))


def begin_body(spots, x_rows, w0, w1, w2, acc, x_some, w_some):
    for k, piece in enumerate((w0, w1, w2)):
        where = pl.multiple_of(spots[25 + k], 256)
        x_some[:, k * 256 : k * 256 + 256] = x_rows[:, pl.ds(where, 256)]
        w_some[k * 256 : k * 256 + 256, :] = piece[...]
    for start, width in GROUPS:
        columns = slice(start, start + width)
        acc[:, columns] = jnp.dot(x_some[...], w_some[:, columns], preferred_element_type=jnp.float32)


def down_body(spots, d0, d1, d2, d3, d4, gate, out):
    at = 0
    for piece in (d0, d1, d2, d3, d4):
        for row in range(0, piece.shape[0], 64):
            where = pl.multiple_of(spots[at], 64)
            out[pl.ds(where, 64), :] = piece[row : row + 64, :]
            at += 1


def hidden_body(half, spots, x_rows, acc, w3, w4, taps, gate, hidden, w_some, full):
    w_some[0:128, :] = w3[...]
    w_some[128:256, :] = w4[...]
    r0 = pl.multiple_of(spots[half], 512)
    where = pl.multiple_of(spots[28], 256)
    x_some = x_rows[pl.ds(r0, 512 + HALO), pl.ds(where, 256)]
    for number, (start, width) in enumerate(GROUPS):
        columns = slice(start, start + width)
        full[:, columns] = acc[pl.ds(r0, 512 + HALO), columns] + jnp.dot(
            x_some, w_some[:, columns], preferred_element_type=jnp.float32
        )
        scale = taps[:, columns]
        for row in range(0, 512, 64):
            near = full[row : row + 64 + HALO, columns]
            conv = near[14 : 14 + 64] * scale[0:1]
            conv = conv + near[15 : 15 + 64] * scale[1:2]
            conv = conv + near[16 : 16 + 64] * scale[2:3]
            some = slice(row, row + 64)
            if number < 2:
                made = gelu(conv[:, 256:512]) * conv[:, 0:256]
                hidden[some, number * 256 : number * 256 + 256] = made.astype(jnp.bfloat16)
            else:
                made = gelu(conv[:, 128:256]) * conv[:, 0:128]
                hidden[some, 512:640] = made.astype(jnp.bfloat16)
                tail = conv[:, 256:384]
                made = gelu(pltpu.roll(tail, 64, 1)) * tail
                lane = lax.broadcasted_iota(jnp.int32, made.shape, 1)
                hidden[some, 640:768] = jnp.where(lane < 64, made, 0.0).astype(jnp.bfloat16)


def product_body(spot, spots, hidden, d_all, gate, out):
    r0 = pl.multiple_of(spots[spot], 256)
    product = lax.dot_general(
        hidden[pl.ds(r0, 256), :], d_all[...], (((1,), (1,)), ((), ())), preferred_element_type=jnp.float32
    )
    out[...] = product.astype(out.dtype)


def shards(tokens, norm_in, value_weight, gate_weight, value_taps, gate_taps, down_weight, norm_out):
    f32 = jnp.float32
    y, x, z, c = (lax.axis_index(name) for name in ALL)

    mine, across = jnp.where(c == 0, x, y), jnp.where(c == 0, y, x)
    near = [(mine + k) % 4 for k in (0, 3, 1, 2)]
    far = [(across + k) % 4 for k in (0, 3, 1, 2)]
    place_near, place_far = jnp.where(c == 0, 64, 256), jnp.where(c == 0, 256, 64)
    zb = z % 2
    blocks = [f * place_far + n * place_near for f in far for n in range(4)]
    members = [zb * 2 + c, (1 - zb) * 2 + c, zb * 2 + 1 - c, (1 - zb) * 2 + 1 - c]
    spots = jnp.stack(
        [b.astype(jnp.int32) for b in blocks + [m * 256 for m in members] + [n * 64 for n in near] + [c] + [f * 256 for f in far]
            + [(1 - zb) * 512, zb * 512, c * 256, (1 - c) * 256]]
    )

    (pack,) = call(
        pack_body,
        (
            jnp.concatenate([value_weight, gate_weight, down_weight.T], axis=0),
            jnp.concatenate([value_taps, gate_taps], axis=0),
        ),
        [sds((PACK, 128))],
        [VM] * 2,
    )
    packs = [pack] + [moved(pack, quarter_to(k)) for k in (1, 2, 3)]
    both, tap_rows = call(assemble_body, packs, [sds((64, 2176)), sds((8, 1408), f32)], [VM] * 4)
    up_line, down_line = call(
        line_body, (spots, *all_of_four(both, first_by)), [sds((256, 1408)), sds((256, 768))], [SM] + [VM] * 4
    )
    ups = ring_of_four(up_line, second_by)
    downs = ring_of_four(down_line, second_by)

    (normed,) = call(
        norm_body, (spots, tokens, norm_in.reshape(1, -1)), [sds(tokens.shape)], [SM, VM, VM]
    )
    chip = moved(normed, other_chip)
    (stacked,) = call(stack_body, (normed, chip), [sds((512, 1024))], [VM, VM])
    core = moved(stacked, other_core)
    (last,) = call(last_body, (spots, normed, chip, core), [sds((HALO, 1024))], [SM, VM, VM, VM])
    halo = moved(last, next_group)
    (x_rows,) = call(rows_body, (spots, halo, normed, chip, core), [sds((1024 + HALO, 1024))], [SM] + [VM] * 4)

    (acc,) = call(
        begin_body,
        (spots, x_rows, *ups[:3]),
        [sds((1024 + HALO, 1408), f32)],
        [SM] + [VM] * 4,
        flops=2 * 1040 * 768 * 1408,
        nbytes=8 * MB,
        limit=16,
        scratch=(pltpu.VMEM((1024 + HALO, 768), jnp.bfloat16), pltpu.VMEM((768, 1408), jnp.bfloat16)),
    )

    def hidden_of(half, gate):
        def body(*refs):
            hidden_body(half, *refs)

        (out,) = call(
            body,
            (spots, x_rows, acc, ups[3], ups[4], tap_rows, gate),
            [sds((512, 768))],
            [SM] + [VM] * 5 + [ANY],
            flops=2 * 528 * 256 * 1408 * 3,
            nbytes=4 * MB,
            limit=16,
            scratch=(pltpu.VMEM((256, 1408), jnp.bfloat16), pltpu.VMEM((512 + HALO, 1408), f32)),
        )
        return out

    def product_of(spot, hidden, dtype, gate):
        def body(*refs):
            product_body(spot, *refs)

        (out,) = call(
            body,
            (spots, hidden, d_all, gate),
            [sds((256, 1024), dtype)],
            [SM] + [VM] * 2 + [ANY],
            flops=2 * 256 * 768 * 1024,
            nbytes=2 * MB,
        )
        return out

    hidden_far = hidden_of(29, acc)
    (d_all,) = call(down_body, (spots, *downs, hidden_far), [sds((1024, 768))], [SM] + [VM] * 5 + [ANY])
    first = product_of(32, hidden_far, jnp.bfloat16, d_all)
    got_far = moved(first, other_core)
    second = product_of(31, hidden_far, f32, first)
    sent = (second + got_far.astype(f32)).astype(jnp.bfloat16)
    back = moved(sent, other_chip)
    hidden_near = hidden_of(30, sent)
    third = product_of(32, hidden_near, jnp.bfloat16, sent)
    got_near = moved(third, other_core)
    fourth = product_of(31, hidden_near, f32, third)
    (out,) = call(final_body, (fourth, got_near, back, norm_out.reshape(1, -1)), [sds((256, 1024))], [VM] * 4)
    return out


def solution(mesh):
    split = Mesh(mesh.devices.reshape(NY, NX, NZ, NC), ALL)
    return jax.shard_map(
        shards,
        mesh=split,
        in_specs=(P(ALL, None), P(), P(FS, TP), P(FS, TP), P(None, TP), P(None, TP), P(TP, FS), P()),
        out_specs=P(ALL, None),
        check_vma=False,
    )
```

```python
import jax
import jax.numpy as jnp
from jax import lax
from jax.experimental import pallas as pl
from jax.experimental.pallas import tpu as pltpu
from jax.sharding import Mesh
from jax.sharding import PartitionSpec as P


FS = ("y", "x")
TP = ("z", "c")
ALL = ("y", "x", "z", "c")
NY, NX, NZ, NC = 4, 4, 8, 2
EPS = 1e-06
HALO = 16
MB = 1024 * 1024


def moved(array, target):
    pairs = []
    for y in range(NY):
        for x in range(NX):
            for z in range(NZ):
                for c in range(NC):
                    to = target(y, x, z, c)
                    if to is None:
                        continue
                    source = ((y * NX + x) * NZ + z) * NC + c
                    ty, tx, tz, tc = to
                    pairs.append((source, ((ty * NX + tx) * NZ + tz) * NC + tc))
    return lax.ppermute(array, ALL, pairs)


def quarter_to(k):
    def target(y, x, z, c):
        up = (z + k) % 2 == 0
        return (y, x, (z + k if up else z - k) % NZ, c)

    return target


def first_by(k):
    return lambda y, x, z, c: (y, (x + k) % NX, z, c) if c == 0 else ((y + k) % NY, x, z, c)


def second_by(k):
    return lambda y, x, z, c: ((y + k) % NY, x, z, c) if c == 0 else (y, (x + k) % NX, z, c)


def other_core(y, x, z, c):
    return (y, x, z, 1 - c)


def other_chip(y, x, z, c):
    return (y, x, z ^ 1, c)


def next_device(y, x, z, c):
    at = ((y * NX + x) * NZ + z) * NC + c + 1
    if at >= NY * NX * NZ * NC:
        return None
    return (at // (NX * NZ * NC), at // (NZ * NC) % NX, at // NC % NZ, at % NC)


def all_of_four(block, by):
    return block, moved(block, by(1)), moved(block, by(-1)), moved(block, by(2))


def ring_of_four(block, by):
    half = block.shape[0] // 2
    before = moved(block, by(1))
    after = moved(block, by(-1))
    top = moved(before[:half], by(1))
    bottom = moved(after[half:], by(-1))
    return block, before, after, top, bottom


VM = pl.BlockSpec(memory_space=pltpu.VMEM)
SM = pl.BlockSpec(memory_space=pltpu.SMEM)
ANY = pl.BlockSpec(memory_space=pl.ANY)


def call(body, ins, outs, specs, *, flops=MB, nbytes=MB, scratch=(), limit=16):
    return pl.pallas_call(
        body,
        out_shape=outs,
        in_specs=specs,
        out_specs=[VM] * len(outs),
        scratch_shapes=list(scratch),
        compiler_params=pltpu.CompilerParams(vmem_limit_bytes=limit * MB),
        cost_estimate=pl.CostEstimate(flops=flops, bytes_accessed=nbytes, transcendentals=0),
    )(*ins)


def sds(shape, dtype=jnp.bfloat16):
    return jax.ShapeDtypeStruct(shape, dtype)


def normed_rows(wide, scale):
    power = jnp.mean(wide * wide, axis=-1, keepdims=True)
    return wide * lax.rsqrt(power + EPS) * scale


def turned(wide):
    blocks = [wide[:, (y * NX + x) * 64 : (y * NX + x + 1) * 64] for x in range(NX) for y in range(NY)]
    return jnp.concatenate(blocks, axis=1)


def norm_body(spots, tokens, scale, out, last):
    rows = normed_rows(tokens[...].astype(jnp.float32), scale[...])
    last[...] = rows[256 - HALO :].astype(jnp.bfloat16)

    @pl.when(spots[24] == 0)
    def _():
        out[...] = rows.astype(jnp.bfloat16)

    @pl.when(spots[24] == 1)
    def _():
        out[...] = turned(rows).astype(jnp.bfloat16)


def join_body(own, halo, out):
    out[0:256, :] = own[...]
    out[256 : 256 + HALO, :] = halo[...]


def stack_body(spots, own, chip, out):
    out[0:256, :] = turned(own[0:256, :].astype(jnp.float32)).astype(jnp.bfloat16)
    out[256:512, :] = turned(chip[0:256, :].astype(jnp.float32)).astype(jnp.bfloat16)
    even = spots[29] == 512
    halo = jnp.where(even, own[256 : 256 + HALO, :].astype(jnp.float32), chip[256 : 256 + HALO, :].astype(jnp.float32))
    out[512 : 512 + HALO, :] = turned(halo).astype(jnp.bfloat16)


def rows_body(spots, own, chip, core, out):
    for k, ref, row in ((0, own, 0), (1, chip, 0), (2, core, 0), (3, core, 256)):
        where = pl.multiple_of(HALO + spots[16 + k], 16)
        out[pl.ds(where, 256), :] = ref[row : row + 256, :]
    even = spots[29] == 512

    @pl.when(spots[24] == 1)
    def _():
        out[0:HALO, :] = core[512 : 512 + HALO, :]

    @pl.when(jnp.logical_and(spots[24] == 0, even))
    def _():
        out[0:HALO, :] = own[256 : 256 + HALO, :]

    @pl.when(jnp.logical_and(spots[24] == 0, jnp.logical_not(even)))
    def _():
        out[0:HALO, :] = chip[256 : 256 + HALO, :]


def final_body(own, near, far, scale, out):
    total = own[...] + near[...].astype(jnp.float32) + far[...].astype(jnp.float32)
    out[...] = normed_rows(total, scale[...]).astype(jnp.bfloat16)


PACK = 344


def three_parts(values):
    high = values.astype(jnp.bfloat16).astype(jnp.float32)
    rest = values - high
    middle = rest.astype(jnp.bfloat16).astype(jnp.float32)
    return [high, middle, rest - middle]


def pack_body(weights, taps, out):
    f32, bf16 = jnp.float32, jnp.bfloat16
    parts = three_parts(taps[0:3, :]) + three_parts(taps[3:6, :])
    rows = jnp.concatenate(parts + [jnp.zeros((6, 176), f32)], axis=0)
    rest = weights[:, 128:176].astype(f32)
    out[0:192, :] = weights[:, 0:128]
    out[320:344, :] = rows[:, 0:128].astype(bf16)
    pair = jnp.concatenate([rest[0:64], rest[64:128], jnp.zeros((64, 32), f32)], axis=1)
    out[192:256, :] = pair.astype(bf16)
    more = jnp.concatenate([rows[:, 128:176], jnp.zeros((40, 48), f32)], axis=0)
    gap = jnp.zeros((64, 16), f32)
    out[256:320, :] = jnp.concatenate([rest[128:192], gap, more, gap], axis=1).astype(bf16)


def arranged(v, g):
    return jnp.concatenate(
        [v[:, 0:256], g[:, 0:256], v[:, 256:512], g[:, 256:512], v[:, 512:640], g[:, 512:640], v[:, 640:704], g[:, 640:704]],
        axis=1,
    )


def assemble_body(p0, p1, p2, p3, both, taps):
    f32 = jnp.float32

    def wide(row, other, lane, count=64):
        pieces = []
        for p in (p0, p1, p2, p3):
            pieces.append(p[row : row + count, :].astype(f32))
            pieces.append(p[other : other + count, :].astype(f32)[:, lane : lane + 48])
        return jnp.concatenate(pieces, axis=1)

    both[:, 0:1408] = arranged(wide(0, 192, 0), wide(64, 192, 48)).astype(jnp.bfloat16)
    down = jnp.concatenate([wide(128, 256, 0), jnp.zeros((64, 64), f32)], axis=1)
    both[:, 1408:2176] = down.astype(jnp.bfloat16)
    parts = wide(320, 256, 64, 24)
    whole = [(parts[k : k + 3] + parts[k + 3 : k + 6]) + parts[k + 6 : k + 9] for k in (0, 9)]
    taps[...] = jnp.concatenate([arranged(*whole), jnp.zeros((5, 1408), f32)], axis=0)


def line_body(spots, b0, b1, b2, b3, up, down):
    for k, piece in enumerate((b0, b1, b2, b3)):
        where = pl.multiple_of(spots[20 + k], 64)
        up[pl.ds(where, 64), :] = piece[:, 0:1408]
        down[pl.ds(where, 64), :] = piece[:, 1408:2176]


def gelu(v):
    inner = v * (0.7978845608028654 + 0.035677408136300125 * (v * v))
    return 0.5 * v * (1.0 + jnp.tanh(inner))


GROUPS = ((0, 512), (512, 512), (1024, 384))


def own_body(spots, x_rows, w0, acc):
    x_some = x_rows[:, pl.ds(pl.multiple_of(spots[25], 256), 256)]
    for start, width in GROUPS:
        columns = slice(start, start + width)
        acc[:, columns] = jnp.dot(x_some, w0[:, columns], preferred_element_type=jnp.float32)


def more_body(spots, x_rows, before, w1, w2, acc, x_some, w_some):
    for k, piece in enumerate((w1, w2)):
        where = pl.multiple_of(spots[26 + k], 256)
        x_some[:, k * 256 : k * 256 + 256] = x_rows[:, pl.ds(where, 256)]
        w_some[k * 256 : k * 256 + 256, :] = piece[...]
    for start, width in GROUPS:
        columns = slice(start, start + width)
        acc[:, columns] = before[:, columns] + jnp.dot(
            x_some[...], w_some[:, columns], preferred_element_type=jnp.float32
        )


def down_body(spots, d0, d1, d2, d3, d4, gate, out, d_rows):
    at = 0
    for piece in (d0, d1, d2, d3, d4):
        for row in range(0, piece.shape[0], 64):
            where = pl.multiple_of(spots[at], 64)
            d_rows[pl.ds(where, 64), :] = piece[row : row + 64, :]
            at += 1
    for row in range(0, 1024, 128):
        out[:, row : row + 128] = d_rows[row : row + 128, :].T


def hidden_body(half, spots, x_rows, acc, w3, w4, taps, gate, hidden, w_some, full):
    w_some[0:128, :] = w3[...]
    w_some[128:256, :] = w4[...]
    r0 = pl.multiple_of(spots[half], 512)
    where = pl.multiple_of(spots[28], 256)
    x_some = x_rows[pl.ds(r0, 512 + HALO), pl.ds(where, 256)]
    for number, (start, width) in enumerate(GROUPS):
        columns = slice(start, start + width)
        full[:, columns] = acc[pl.ds(r0, 512 + HALO), columns] + jnp.dot(
            x_some, w_some[:, columns], preferred_element_type=jnp.float32
        )
        scale = taps[:, columns]
        for row in range(0, 512, 64):
            near = full[row : row + 64 + HALO, columns]
            conv = near[14 : 14 + 64] * scale[0:1]
            conv = conv + near[15 : 15 + 64] * scale[1:2]
            conv = conv + near[16 : 16 + 64] * scale[2:3]
            some = slice(row, row + 64)
            if number < 2:
                made = gelu(conv[:, 256:512]) * conv[:, 0:256]
                hidden[some, number * 256 : number * 256 + 256] = made.astype(jnp.bfloat16)
            else:
                made = gelu(conv[:, 128:256]) * conv[:, 0:128]
                hidden[some, 512:640] = made.astype(jnp.bfloat16)
                tail = conv[:, 256:384]
                made = gelu(pltpu.roll(tail, 64, 1)) * tail
                lane = lax.broadcasted_iota(jnp.int32, made.shape, 1)
                hidden[some, 640:768] = jnp.where(lane < 64, made, 0.0).astype(jnp.bfloat16)


def product_body(spot, spots, hidden, d_all, gate, out):
    r0 = pl.multiple_of(spots[spot], 256)
    product = jnp.dot(hidden[pl.ds(r0, 256), :], d_all[...], preferred_element_type=jnp.float32)
    out[...] = product.astype(out.dtype)


def shards(tokens, norm_in, value_weight, gate_weight, value_taps, gate_taps, down_weight, norm_out):
    f32 = jnp.float32
    y, x, z, c = (lax.axis_index(name) for name in ALL)

    mine, across = jnp.where(c == 0, x, y), jnp.where(c == 0, y, x)
    near = [(mine + k) % 4 for k in (0, 3, 1, 2)]
    far = [(across + k) % 4 for k in (0, 3, 1, 2)]
    place_near, place_far = jnp.where(c == 0, 64, 256), jnp.where(c == 0, 256, 64)
    zb = z % 2
    blocks = [f * place_far + n * place_near for f in far for n in range(4)]
    members = [zb * 2 + c, (1 - zb) * 2 + c, zb * 2 + 1 - c, (1 - zb) * 2 + 1 - c]
    spots = jnp.stack(
        [b.astype(jnp.int32) for b in blocks + [m * 256 for m in members] + [n * 64 for n in near] + [c] + [f * 256 for f in far]
            + [(1 - zb) * 512, zb * 512, c * 256, (1 - c) * 256]]
    )

    (pack,) = call(
        pack_body,
        (
            jnp.concatenate([value_weight, gate_weight, down_weight.T], axis=0),
            jnp.concatenate([value_taps, gate_taps], axis=0),
        ),
        [sds((PACK, 128))],
        [VM] * 2,
    )
    packs = [pack] + [moved(pack, quarter_to(k)) for k in (1, 2, 3)]
    both, tap_rows = call(assemble_body, packs, [sds((64, 2176)), sds((8, 1408), f32)], [VM] * 4)
    up_line, down_line = call(
        line_body, (spots, *all_of_four(both, first_by)), [sds((256, 1408)), sds((256, 768))], [SM] + [VM] * 4
    )
    ups = ring_of_four(up_line, second_by)
    downs = ring_of_four(down_line, second_by)

    normed, last = call(
        norm_body,
        (spots, tokens, norm_in.reshape(1, -1)),
        [sds(tokens.shape), sds((HALO, 1024))],
        [SM, VM, VM],
    )
    halo = moved(last, next_device)
    (joined,) = call(join_body, (normed, halo), [sds((256 + HALO, 1024))], [VM] * 2)
    chip = moved(joined, other_chip)
    (stacked,) = call(stack_body, (spots, joined, chip), [sds((512 + HALO, 1024))], [SM, VM, VM])
    core = moved(stacked, other_core)
    (x_rows,) = call(rows_body, (spots, joined, chip, core), [sds((1024 + HALO, 1024))], [SM] + [VM] * 3)

    sums = [sds((1024 + HALO, 1408), f32)]
    (acc_own,) = call(
        own_body, (spots, x_rows, ups[0]), sums, [SM] + [VM] * 2, flops=2 * 1040 * 256 * 1408, nbytes=8 * MB
    )
    (acc,) = call(
        more_body,
        (spots, x_rows, acc_own, *ups[1:3]),
        sums,
        [SM] + [VM] * 4,
        flops=2 * 1040 * 512 * 1408,
        nbytes=8 * MB,
        limit=16,
        scratch=(pltpu.VMEM((1024 + HALO, 512), jnp.bfloat16), pltpu.VMEM((512, 1408), jnp.bfloat16)),
    )

    def hidden_of(half, gate):
        def body(*refs):
            hidden_body(half, *refs)

        (out,) = call(
            body,
            (spots, x_rows, acc, ups[3], ups[4], tap_rows, gate),
            [sds((512, 768))],
            [SM] + [VM] * 5 + [ANY],
            flops=2 * 528 * 256 * 1408 * 3,
            nbytes=4 * MB,
            limit=16,
            scratch=(pltpu.VMEM((256, 1408), jnp.bfloat16), pltpu.VMEM((512 + HALO, 1408), f32)),
        )
        return out

    def product_of(spot, hidden, dtype, gate):
        def body(*refs):
            product_body(spot, *refs)

        (out,) = call(
            body,
            (spots, hidden, d_all, gate),
            [sds((256, 1024), dtype)],
            [SM] + [VM] * 2 + [ANY],
            flops=2 * 256 * 768 * 1024,
            nbytes=2 * MB,
        )
        return out

    hidden_far = hidden_of(29, acc)
    (d_all,) = call(
        down_body,
        (spots, *downs, hidden_far),
        [sds((768, 1024))],
        [SM] + [VM] * 5 + [ANY],
        scratch=(pltpu.VMEM((1024, 768), jnp.bfloat16),),
    )
    first = product_of(32, hidden_far, jnp.bfloat16, d_all)
    got_far = moved(first, other_core)
    second = product_of(31, hidden_far, f32, first)
    sent = (second + got_far.astype(f32)).astype(jnp.bfloat16)
    back = moved(sent, other_chip)
    hidden_near = hidden_of(30, sent)
    third = product_of(32, hidden_near, jnp.bfloat16, sent)
    got_near = moved(third, other_core)
    fourth = product_of(31, hidden_near, f32, third)
    (out,) = call(final_body, (fourth, got_near, back, norm_out.reshape(1, -1)), [sds((256, 1024))], [VM] * 4)
    return out


def solution(mesh):
    split = Mesh(mesh.devices.reshape(NY, NX, NZ, NC), ALL)
    return jax.shard_map(
        shards,
        mesh=split,
        in_specs=(P(ALL, None), P(), P(FS, TP), P(FS, TP), P(None, TP), P(None, TP), P(TP, FS), P()),
        out_specs=P(ALL, None),
        check_vma=False,
    )
```

```python
import jax
import jax.numpy as jnp
from jax import lax
from jax.experimental import pallas as pl
from jax.experimental.pallas import tpu as pltpu
from jax.sharding import Mesh
from jax.sharding import PartitionSpec as P


FS = ("y", "x")
TP = ("z", "c")
ALL = ("y", "x", "z", "c")
NY, NX, NZ, NC = 4, 4, 8, 2
EPS = 1e-06
HALO = 16
MB = 1024 * 1024


def moved(array, target):
    pairs = []
    for y in range(NY):
        for x in range(NX):
            for z in range(NZ):
                for c in range(NC):
                    to = target(y, x, z, c)
                    if to is None:
                        continue
                    source = ((y * NX + x) * NZ + z) * NC + c
                    ty, tx, tz, tc = to
                    pairs.append((source, ((ty * NX + tx) * NZ + tz) * NC + tc))
    return lax.ppermute(array, ALL, pairs)


def quarter_to(k):
    def target(y, x, z, c):
        up = (z + k) % 2 == 0
        return (y, x, (z + k if up else z - k) % NZ, c)

    return target


def first_by(k):
    return lambda y, x, z, c: (y, (x + k) % NX, z, c) if c == 0 else ((y + k) % NY, x, z, c)


def second_by(k):
    return lambda y, x, z, c: ((y + k) % NY, x, z, c) if c == 0 else (y, (x + k) % NX, z, c)


def other_core(y, x, z, c):
    return (y, x, z, 1 - c)


def other_chip(y, x, z, c):
    return (y, x, z ^ 1, c)


def next_device(y, x, z, c):
    at = ((y * NX + x) * NZ + z) * NC + c + 1
    if at >= NY * NX * NZ * NC:
        return None
    return (at // (NX * NZ * NC), at // (NZ * NC) % NX, at // NC % NZ, at % NC)


def all_of_four(block, by):
    return block, moved(block, by(1)), moved(block, by(-1)), moved(block, by(2))


def ring_of_four(block, by):
    half = block.shape[0] // 2
    before = moved(block, by(1))
    after = moved(block, by(-1))
    top = moved(before[:half], by(1))
    bottom = moved(after[half:], by(-1))
    return block, before, after, top, bottom


VM = pl.BlockSpec(memory_space=pltpu.VMEM)
SM = pl.BlockSpec(memory_space=pltpu.SMEM)
ANY = pl.BlockSpec(memory_space=pl.ANY)


def call(body, ins, outs, specs, *, flops=MB, nbytes=MB, scratch=(), limit=16):
    return pl.pallas_call(
        body,
        out_shape=outs,
        in_specs=specs,
        out_specs=[VM] * len(outs),
        scratch_shapes=list(scratch),
        compiler_params=pltpu.CompilerParams(vmem_limit_bytes=limit * MB),
        cost_estimate=pl.CostEstimate(flops=flops, bytes_accessed=nbytes, transcendentals=0),
    )(*ins)


def sds(shape, dtype=jnp.bfloat16):
    return jax.ShapeDtypeStruct(shape, dtype)


def normed_rows(wide, scale):
    power = jnp.mean(wide * wide, axis=-1, keepdims=True)
    return wide * lax.rsqrt(power + EPS) * scale


def turned(wide):
    blocks = [wide[:, (y * NX + x) * 64 : (y * NX + x + 1) * 64] for x in range(NX) for y in range(NY)]
    return jnp.concatenate(blocks, axis=1)


def join_body(own, halo, out):
    out[0:256, :] = own[...]
    out[256 : 256 + HALO, :] = halo[...]


def stack_body(spots, own, chip, out):
    out[0:256, :] = own[0:256, :]
    out[256:512, :] = chip[0:256, :]
    even = spots[29] == 512

    @pl.when(even)
    def _():
        out[512 : 512 + HALO, :] = own[256 : 256 + HALO, :]

    @pl.when(jnp.logical_not(even))
    def _():
        out[512 : 512 + HALO, :] = chip[256 : 256 + HALO, :]


def rows_body(spots, stacked, core, scale, out):
    pieces = (
        (HALO + spots[16], stacked, 0, 256),
        (HALO + spots[17], stacked, 256, 256),
        (HALO + spots[18], core, 0, 256),
        (HALO + spots[19], core, 256, 256),
    )

    def write(order):
        for at, ref, row, count in pieces:
            for part in range(0, count, 64):
                wide = ref[row + part : row + part + 64, :].astype(jnp.float32)
                where = pl.multiple_of(at + part, 16)
                out[pl.ds(where, 64), :] = order(normed_rows(wide, scale[...])).astype(jnp.bfloat16)

    @pl.when(spots[24] == 0)
    def _():
        write(lambda rows: rows)
        halo = normed_rows(stacked[512 : 512 + HALO, :].astype(jnp.float32), scale[...])
        out[0:HALO, :] = halo.astype(jnp.bfloat16)

    @pl.when(spots[24] == 1)
    def _():
        write(turned)
        halo = normed_rows(core[512 : 512 + HALO, :].astype(jnp.float32), scale[...])
        out[0:HALO, :] = turned(halo).astype(jnp.bfloat16)


def final_body(own, near, far, scale, out):
    total = own[...] + near[...].astype(jnp.float32) + far[...].astype(jnp.float32)
    out[...] = normed_rows(total, scale[...]).astype(jnp.bfloat16)


PACK = 344


def three_parts(values):
    high = values.astype(jnp.bfloat16).astype(jnp.float32)
    rest = values - high
    middle = rest.astype(jnp.bfloat16).astype(jnp.float32)
    return [high, middle, rest - middle]


def pack_body(weights, taps, out):
    f32, bf16 = jnp.float32, jnp.bfloat16
    parts = three_parts(taps[0:3, :]) + three_parts(taps[3:6, :])
    rows = jnp.concatenate(parts + [jnp.zeros((6, 176), f32)], axis=0)
    rest = weights[:, 128:176].astype(f32)
    out[0:192, :] = weights[:, 0:128]
    out[320:344, :] = rows[:, 0:128].astype(bf16)
    pair = jnp.concatenate([rest[0:64], rest[64:128], jnp.zeros((64, 32), f32)], axis=1)
    out[192:256, :] = pair.astype(bf16)
    more = jnp.concatenate([rows[:, 128:176], jnp.zeros((40, 48), f32)], axis=0)
    gap = jnp.zeros((64, 16), f32)
    out[256:320, :] = jnp.concatenate([rest[128:192], gap, more, gap], axis=1).astype(bf16)


def arranged(v, g):
    return jnp.concatenate(
        [v[:, 0:256], g[:, 0:256], v[:, 256:512], g[:, 256:512], v[:, 512:640], g[:, 512:640], v[:, 640:704], g[:, 640:704]],
        axis=1,
    )


def assemble_body(p0, p1, p2, p3, both, taps):
    f32 = jnp.float32

    def wide(row, other, lane, count=64):
        pieces = []
        for p in (p0, p1, p2, p3):
            pieces.append(p[row : row + count, :].astype(f32))
            pieces.append(p[other : other + count, :].astype(f32)[:, lane : lane + 48])
        return jnp.concatenate(pieces, axis=1)

    both[:, 0:1408] = arranged(wide(0, 192, 0), wide(64, 192, 48)).astype(jnp.bfloat16)
    down = jnp.concatenate([wide(128, 256, 0), jnp.zeros((64, 64), f32)], axis=1)
    both[:, 1408:2176] = down.astype(jnp.bfloat16)
    parts = wide(320, 256, 64, 24)
    whole = [(parts[k : k + 3] + parts[k + 3 : k + 6]) + parts[k + 6 : k + 9] for k in (0, 9)]
    taps[...] = jnp.concatenate([arranged(*whole), jnp.zeros((5, 1408), f32)], axis=0)


def line_body(spots, b0, b1, b2, b3, up, down):
    for k, piece in enumerate((b0, b1, b2, b3)):
        where = pl.multiple_of(spots[20 + k], 64)
        up[pl.ds(where, 64), :] = piece[:, 0:1408]
        down[pl.ds(where, 64), :] = piece[:, 1408:2176]


def gelu(v):
    inner = v * (0.7978845608028654 + 0.035677408136300125 * (v * v))
    return 0.5 * v * (1.0 + jnp.tanh(inner))


GROUPS = ((0, 512), (512, 512), (1024, 384))


def own_body(spots, x_rows, w0, acc):
    x_some = x_rows[:, pl.ds(pl.multiple_of(spots[25], 256), 256)]
    for start, width in GROUPS:
        columns = slice(start, start + width)
        acc[:, columns] = jnp.dot(x_some, w0[:, columns], preferred_element_type=jnp.float32)


def more_body(spots, x_rows, before, w1, w2, acc, x_some, w_some):
    for k, piece in enumerate((w1, w2)):
        where = pl.multiple_of(spots[26 + k], 256)
        x_some[:, k * 256 : k * 256 + 256] = x_rows[:, pl.ds(where, 256)]
        w_some[k * 256 : k * 256 + 256, :] = piece[...]
    for start, width in GROUPS:
        columns = slice(start, start + width)
        acc[:, columns] = before[:, columns] + jnp.dot(
            x_some[...], w_some[:, columns], preferred_element_type=jnp.float32
        )


def down_body(spots, d0, d1, d2, d3, d4, gate, out):
    at = 0
    for piece in (d0, d1, d2, d3, d4):
        for row in range(0, piece.shape[0], 64):
            where = pl.multiple_of(spots[at], 64)
            out[pl.ds(where, 64), :] = piece[row : row + 64, :]
            at += 1


def hidden_body(half, spots, x_rows, acc, w3, w4, taps, gate, hidden, w_some, full):
    w_some[0:128, :] = w3[...]
    w_some[128:256, :] = w4[...]
    r0 = pl.multiple_of(spots[half], 512)
    where = pl.multiple_of(spots[28], 256)
    x_some = x_rows[pl.ds(r0, 512 + HALO), pl.ds(where, 256)]
    for number, (start, width) in enumerate(GROUPS):
        columns = slice(start, start + width)
        full[:, columns] = acc[pl.ds(r0, 512 + HALO), columns] + jnp.dot(
            x_some, w_some[:, columns], preferred_element_type=jnp.float32
        )
        scale = taps[:, columns]
        for row in range(0, 512, 64):
            near = full[row : row + 64 + HALO, columns]
            conv = near[14 : 14 + 64] * scale[0:1]
            conv = conv + near[15 : 15 + 64] * scale[1:2]
            conv = conv + near[16 : 16 + 64] * scale[2:3]
            some = slice(row, row + 64)
            if number < 2:
                made = gelu(conv[:, 256:512]) * conv[:, 0:256]
                hidden[some, number * 256 : number * 256 + 256] = made.astype(jnp.bfloat16)
            else:
                made = gelu(conv[:, 128:256]) * conv[:, 0:128]
                hidden[some, 512:640] = made.astype(jnp.bfloat16)
                tail = conv[:, 256:384]
                made = gelu(pltpu.roll(tail, 64, 1)) * tail
                lane = lax.broadcasted_iota(jnp.int32, made.shape, 1)
                hidden[some, 640:768] = jnp.where(lane < 64, made, 0.0).astype(jnp.bfloat16)


def product_body(spot, spots, hidden, d_all, gate, out):
    r0 = pl.multiple_of(spots[spot], 256)
    product = lax.dot_general(
        hidden[pl.ds(r0, 256), :], d_all[...], (((1,), (1,)), ((), ())), preferred_element_type=jnp.float32
    )
    out[...] = product.astype(out.dtype)


def shards(tokens, norm_in, value_weight, gate_weight, value_taps, gate_taps, down_weight, norm_out):
    f32 = jnp.float32
    y, x, z, c = (lax.axis_index(name) for name in ALL)

    mine, across = jnp.where(c == 0, x, y), jnp.where(c == 0, y, x)
    near = [(mine + k) % 4 for k in (0, 3, 1, 2)]
    far = [(across + k) % 4 for k in (0, 3, 1, 2)]
    place_near, place_far = jnp.where(c == 0, 64, 256), jnp.where(c == 0, 256, 64)
    zb = z % 2
    blocks = [f * place_far + n * place_near for f in far for n in range(4)]
    members = [zb * 2 + c, (1 - zb) * 2 + c, zb * 2 + 1 - c, (1 - zb) * 2 + 1 - c]
    spots = jnp.stack(
        [b.astype(jnp.int32) for b in blocks + [m * 256 for m in members] + [n * 64 for n in near] + [c] + [f * 256 for f in far]
            + [(1 - zb) * 512, zb * 512, c * 256, (1 - c) * 256]]
    )

    (pack,) = call(
        pack_body,
        (
            jnp.concatenate([value_weight, gate_weight, down_weight.T], axis=0),
            jnp.concatenate([value_taps, gate_taps], axis=0),
        ),
        [sds((PACK, 128))],
        [VM] * 2,
    )
    packs = [pack] + [moved(pack, quarter_to(k)) for k in (1, 2, 3)]
    both, tap_rows = call(assemble_body, packs, [sds((64, 2176)), sds((8, 1408), f32)], [VM] * 4)
    up_line, down_line = call(
        line_body, (spots, *all_of_four(both, first_by)), [sds((256, 1408)), sds((256, 768))], [SM] + [VM] * 4
    )
    ups = ring_of_four(up_line, second_by)
    downs = ring_of_four(down_line, second_by)

    halo = moved(tokens[-HALO:], next_device)
    (joined,) = call(join_body, (tokens, halo), [sds((256 + HALO, 1024))], [VM] * 2)
    chip = moved(joined, other_chip)
    (stacked,) = call(stack_body, (spots, joined, chip), [sds((512 + HALO, 1024))], [SM, VM, VM])
    core = moved(stacked, other_core)
    (x_rows,) = call(
        rows_body,
        (spots, stacked, core, norm_in.reshape(1, -1)),
        [sds((1024 + HALO, 1024))],
        [SM] + [VM] * 3,
    )

    sums = [sds((1024 + HALO, 1408), f32)]
    (acc_own,) = call(
        own_body, (spots, x_rows, ups[0]), sums, [SM] + [VM] * 2, flops=2 * 1040 * 256 * 1408, nbytes=8 * MB
    )
    (acc,) = call(
        more_body,
        (spots, x_rows, acc_own, *ups[1:3]),
        sums,
        [SM] + [VM] * 4,
        flops=2 * 1040 * 512 * 1408,
        nbytes=8 * MB,
        limit=16,
        scratch=(pltpu.VMEM((1024 + HALO, 512), jnp.bfloat16), pltpu.VMEM((512, 1408), jnp.bfloat16)),
    )

    def hidden_of(half, gate):
        def body(*refs):
            hidden_body(half, *refs)

        (out,) = call(
            body,
            (spots, x_rows, acc, ups[3], ups[4], tap_rows, gate),
            [sds((512, 768))],
            [SM] + [VM] * 5 + [ANY],
            flops=2 * 528 * 256 * 1408 * 3,
            nbytes=4 * MB,
            limit=16,
            scratch=(pltpu.VMEM((256, 1408), jnp.bfloat16), pltpu.VMEM((512 + HALO, 1408), f32)),
        )
        return out

    def product_of(spot, hidden, dtype, gate):
        def body(*refs):
            product_body(spot, *refs)

        (out,) = call(
            body,
            (spots, hidden, d_all, gate),
            [sds((256, 1024), dtype)],
            [SM] + [VM] * 2 + [ANY],
            flops=2 * 256 * 768 * 1024,
            nbytes=2 * MB,
        )
        return out

    hidden_far = hidden_of(29, acc)
    (d_all,) = call(
        down_body,
        (spots, *downs, hidden_far),
        [sds((1024, 768))],
        [SM] + [VM] * 5 + [ANY],
    )
    first = product_of(32, hidden_far, jnp.bfloat16, d_all)
    got_far = moved(first, other_core)
    second = product_of(31, hidden_far, f32, first)
    sent = (second + got_far.astype(f32)).astype(jnp.bfloat16)
    back = moved(sent, other_chip)
    hidden_near = hidden_of(30, sent)
    third = product_of(32, hidden_near, jnp.bfloat16, sent)
    got_near = moved(third, other_core)
    fourth = product_of(31, hidden_near, f32, third)
    (out,) = call(final_body, (fourth, got_near, back, norm_out.reshape(1, -1)), [sds((256, 1024))], [VM] * 4)
    return out


def solution(mesh):
    split = Mesh(mesh.devices.reshape(NY, NX, NZ, NC), ALL)
    return jax.shard_map(
        shards,
        mesh=split,
        in_specs=(P(ALL, None), P(), P(FS, TP), P(FS, TP), P(None, TP), P(None, TP), P(TP, FS), P()),
        out_specs=P(ALL, None),
        check_vma=False,
    )
```

```python
import jax
import jax.numpy as jnp
from jax import lax
from jax.experimental import pallas as pl
from jax.experimental.pallas import tpu as pltpu
from jax.sharding import Mesh
from jax.sharding import PartitionSpec as P


FS = ("y", "x")
TP = ("z", "c")
ALL = ("y", "x", "z", "c")
NY, NX, NZ, NC = 4, 4, 8, 2
EPS = 1e-06
HALO = 16
MB = 1024 * 1024


def moved(array, target):
    pairs = []
    for y in range(NY):
        for x in range(NX):
            for z in range(NZ):
                for c in range(NC):
                    to = target(y, x, z, c)
                    if to is None:
                        continue
                    source = ((y * NX + x) * NZ + z) * NC + c
                    ty, tx, tz, tc = to
                    pairs.append((source, ((ty * NX + tx) * NZ + tz) * NC + tc))
    return lax.ppermute(array, ALL, pairs)


def quarter_to(k):
    def target(y, x, z, c):
        up = (z + k) % 2 == 0
        return (y, x, (z + k if up else z - k) % NZ, c)

    return target


def first_by(k):
    return lambda y, x, z, c: (y, (x + k) % NX, z, c) if c == 0 else ((y + k) % NY, x, z, c)


def second_by(k):
    return lambda y, x, z, c: ((y + k) % NY, x, z, c) if c == 0 else (y, (x + k) % NX, z, c)


def other_core(y, x, z, c):
    return (y, x, z, 1 - c)


def other_chip(y, x, z, c):
    return (y, x, z ^ 1, c)


def after_by(k):
    def target(y, x, z, c):
        at = ((y * NX + x) * NZ + z) * NC + c + k
        if at >= NY * NX * NZ * NC:
            return None
        return (at // (NX * NZ * NC), at // (NZ * NC) % NX, at // NC % NZ, at % NC)

    return target


def all_of_four(block, by):
    return block, moved(block, by(1)), moved(block, by(-1)), moved(block, by(2))


def ring_of_four(block, by):
    half = block.shape[0] // 2
    before = moved(block, by(1))
    after = moved(block, by(-1))
    top = moved(before[:half], by(1))
    bottom = moved(after[half:], by(-1))
    return block, before, after, top, bottom


VM = pl.BlockSpec(memory_space=pltpu.VMEM)
SM = pl.BlockSpec(memory_space=pltpu.SMEM)
ANY = pl.BlockSpec(memory_space=pl.ANY)


def call(body, ins, outs, specs, *, flops=MB, nbytes=MB, scratch=(), limit=16):
    return pl.pallas_call(
        body,
        out_shape=outs,
        in_specs=specs,
        out_specs=[VM] * len(outs),
        scratch_shapes=list(scratch),
        compiler_params=pltpu.CompilerParams(vmem_limit_bytes=limit * MB),
        cost_estimate=pl.CostEstimate(flops=flops, bytes_accessed=nbytes, transcendentals=0),
    )(*ins)


def sds(shape, dtype=jnp.bfloat16):
    return jax.ShapeDtypeStruct(shape, dtype)


def normed_rows(wide, scale):
    power = jnp.mean(wide * wide, axis=-1, keepdims=True)
    return wide * lax.rsqrt(power + EPS) * scale


def turned(wide):
    blocks = [wide[:, (y * NX + x) * 64 : (y * NX + x + 1) * 64] for x in range(NX) for y in range(NY)]
    return jnp.concatenate(blocks, axis=1)


def stack_body(spots, own, chip, even_halo, odd_halo, out):
    out[0:256, :] = own[...]
    out[256:512, :] = chip[...]
    even = spots[29] == 512

    @pl.when(even)
    def _():
        out[512 : 512 + HALO, :] = even_halo[...]

    @pl.when(jnp.logical_not(even))
    def _():
        out[512 : 512 + HALO, :] = odd_halo[...]


def rows_body(spots, stacked, core, scale, out):
    pieces = (
        (HALO + spots[16], stacked, 0, 256),
        (HALO + spots[17], stacked, 256, 256),
        (HALO + spots[18], core, 0, 256),
        (HALO + spots[19], core, 256, 256),
    )

    def write(order):
        for at, ref, row, count in pieces:
            for part in range(0, count, 64):
                wide = ref[row + part : row + part + 64, :].astype(jnp.float32)
                where = pl.multiple_of(at + part, 16)
                out[pl.ds(where, 64), :] = order(normed_rows(wide, scale[...])).astype(jnp.bfloat16)

    @pl.when(spots[24] == 0)
    def _():
        write(lambda rows: rows)
        halo = normed_rows(stacked[512 : 512 + HALO, :].astype(jnp.float32), scale[...])
        out[0:HALO, :] = halo.astype(jnp.bfloat16)

    @pl.when(spots[24] == 1)
    def _():
        write(turned)
        halo = normed_rows(core[512 : 512 + HALO, :].astype(jnp.float32), scale[...])
        out[0:HALO, :] = turned(halo).astype(jnp.bfloat16)


def final_body(own, near, far, scale, out):
    total = own[...] + near[...].astype(jnp.float32) + far[...].astype(jnp.float32)
    out[...] = normed_rows(total, scale[...]).astype(jnp.bfloat16)


PACK = 344


def three_parts(values):
    high = values.astype(jnp.bfloat16).astype(jnp.float32)
    rest = values - high
    middle = rest.astype(jnp.bfloat16).astype(jnp.float32)
    return [high, middle, rest - middle]


def pack_body(weights, taps, out):
    f32, bf16 = jnp.float32, jnp.bfloat16
    parts = three_parts(taps[0:3, :]) + three_parts(taps[3:6, :])
    rows = jnp.concatenate(parts + [jnp.zeros((6, 176), f32)], axis=0)
    rest = weights[:, 128:176].astype(f32)
    out[0:192, :] = weights[:, 0:128]
    out[320:344, :] = rows[:, 0:128].astype(bf16)
    pair = jnp.concatenate([rest[0:64], rest[64:128], jnp.zeros((64, 32), f32)], axis=1)
    out[192:256, :] = pair.astype(bf16)
    more = jnp.concatenate([rows[:, 128:176], jnp.zeros((40, 48), f32)], axis=0)
    gap = jnp.zeros((64, 16), f32)
    out[256:320, :] = jnp.concatenate([rest[128:192], gap, more, gap], axis=1).astype(bf16)


def arranged(v, g):
    return jnp.concatenate(
        [v[:, 0:256], g[:, 0:256], v[:, 256:512], g[:, 256:512], v[:, 512:640], g[:, 512:640], v[:, 640:704], g[:, 640:704]],
        axis=1,
    )


def assemble_body(p0, p1, p2, p3, both, taps):
    f32 = jnp.float32

    def wide(row, other, lane, count=64):
        pieces = []
        for p in (p0, p1, p2, p3):
            pieces.append(p[row : row + count, :].astype(f32))
            pieces.append(p[other : other + count, :].astype(f32)[:, lane : lane + 48])
        return jnp.concatenate(pieces, axis=1)

    both[:, 0:1408] = arranged(wide(0, 192, 0), wide(64, 192, 48)).astype(jnp.bfloat16)
    down = jnp.concatenate([wide(128, 256, 0), jnp.zeros((64, 64), f32)], axis=1)
    both[:, 1408:2176] = down.astype(jnp.bfloat16)
    parts = wide(320, 256, 64, 24)
    whole = [(parts[k : k + 3] + parts[k + 3 : k + 6]) + parts[k + 6 : k + 9] for k in (0, 9)]
    taps[...] = jnp.concatenate([arranged(*whole), jnp.zeros((5, 1408), f32)], axis=0)


def line_body(spots, b0, b1, b2, b3, up, down):
    for k, piece in enumerate((b0, b1, b2, b3)):
        where = pl.multiple_of(spots[20 + k], 64)
        up[pl.ds(where, 64), :] = piece[:, 0:1408]
        down[pl.ds(where, 64), :] = piece[:, 1408:2176]


def gelu(v):
    inner = v * (0.7978845608028654 + 0.035677408136300125 * (v * v))
    return 0.5 * v * (1.0 + jnp.tanh(inner))


GROUPS = ((0, 512), (512, 512), (1024, 384))


def own_body(spots, x_rows, w0, acc):
    x_some = x_rows[:, pl.ds(pl.multiple_of(spots[25], 256), 256)]
    for start, width in GROUPS:
        columns = slice(start, start + width)
        acc[:, columns] = jnp.dot(x_some, w0[:, columns], preferred_element_type=jnp.float32)


def more_body(spots, x_rows, before, w1, w2, acc, x_some, w_some):
    for k, piece in enumerate((w1, w2)):
        where = pl.multiple_of(spots[26 + k], 256)
        x_some[:, k * 256 : k * 256 + 256] = x_rows[:, pl.ds(where, 256)]
        w_some[k * 256 : k * 256 + 256, :] = piece[...]
    for start, width in GROUPS:
        columns = slice(start, start + width)
        acc[:, columns] = before[:, columns] + jnp.dot(
            x_some[...], w_some[:, columns], preferred_element_type=jnp.float32
        )


def down_body(spots, d0, d1, d2, d3, d4, gate, out):
    at = 0
    for piece in (d0, d1, d2, d3, d4):
        for row in range(0, piece.shape[0], 64):
            where = pl.multiple_of(spots[at], 64)
            out[pl.ds(where, 64), :] = piece[row : row + 64, :]
            at += 1


def hidden_body(half, spots, x_rows, acc, w3, w4, taps, gate, hidden, w_some, full):
    w_some[0:128, :] = w3[...]
    w_some[128:256, :] = w4[...]
    r0 = pl.multiple_of(spots[half], 512)
    where = pl.multiple_of(spots[28], 256)
    x_some = x_rows[pl.ds(r0, 512 + HALO), pl.ds(where, 256)]
    for number, (start, width) in enumerate(GROUPS):
        columns = slice(start, start + width)
        full[:, columns] = acc[pl.ds(r0, 512 + HALO), columns] + jnp.dot(
            x_some, w_some[:, columns], preferred_element_type=jnp.float32
        )
        scale = taps[:, columns]
        for row in range(0, 512, 64):
            near = full[row : row + 64 + HALO, columns]
            conv = near[14 : 14 + 64] * scale[0:1]
            conv = conv + near[15 : 15 + 64] * scale[1:2]
            conv = conv + near[16 : 16 + 64] * scale[2:3]
            some = slice(row, row + 64)
            if number < 2:
                made = gelu(conv[:, 256:512]) * conv[:, 0:256]
                hidden[some, number * 256 : number * 256 + 256] = made.astype(jnp.bfloat16)
            else:
                made = gelu(conv[:, 128:256]) * conv[:, 0:128]
                hidden[some, 512:640] = made.astype(jnp.bfloat16)
                tail = conv[:, 256:384]
                made = gelu(pltpu.roll(tail, 64, 1)) * tail
                lane = lax.broadcasted_iota(jnp.int32, made.shape, 1)
                hidden[some, 640:768] = jnp.where(lane < 64, made, 0.0).astype(jnp.bfloat16)


def product_body(spot, spots, hidden, d_all, gate, out):
    r0 = pl.multiple_of(spots[spot], 256)
    product = lax.dot_general(
        hidden[pl.ds(r0, 256), :], d_all[...], (((1,), (1,)), ((), ())), preferred_element_type=jnp.float32
    )
    out[...] = product.astype(out.dtype)


def shards(tokens, norm_in, value_weight, gate_weight, value_taps, gate_taps, down_weight, norm_out):
    f32 = jnp.float32
    y, x, z, c = (lax.axis_index(name) for name in ALL)

    mine, across = jnp.where(c == 0, x, y), jnp.where(c == 0, y, x)
    near = [(mine + k) % 4 for k in (0, 3, 1, 2)]
    far = [(across + k) % 4 for k in (0, 3, 1, 2)]
    place_near, place_far = jnp.where(c == 0, 64, 256), jnp.where(c == 0, 256, 64)
    zb = z % 2
    blocks = [f * place_far + n * place_near for f in far for n in range(4)]
    members = [zb * 2 + c, (1 - zb) * 2 + c, zb * 2 + 1 - c, (1 - zb) * 2 + 1 - c]
    spots = jnp.stack(
        [b.astype(jnp.int32) for b in blocks + [m * 256 for m in members] + [n * 64 for n in near] + [c] + [f * 256 for f in far]
            + [(1 - zb) * 512, zb * 512, c * 256, (1 - c) * 256]]
    )

    (pack,) = call(
        pack_body,
        (
            jnp.concatenate([value_weight, gate_weight, down_weight.T], axis=0),
            jnp.concatenate([value_taps, gate_taps], axis=0),
        ),
        [sds((PACK, 128))],
        [VM] * 2,
    )
    packs = [pack] + [moved(pack, quarter_to(k)) for k in (1, 2, 3)]
    both, tap_rows = call(assemble_body, packs, [sds((64, 2176)), sds((8, 1408), f32)], [VM] * 4)
    up_line, down_line = call(
        line_body, (spots, *all_of_four(both, first_by)), [sds((256, 1408)), sds((256, 768))], [SM] + [VM] * 4
    )
    ups = ring_of_four(up_line, second_by)
    downs = ring_of_four(down_line, second_by)

    chip = moved(tokens, other_chip)
    last = tokens[-HALO:]
    halos = (moved(last, after_by(1)), moved(last, after_by(3)))
    (stacked,) = call(stack_body, (spots, tokens, chip, *halos), [sds((512 + HALO, 1024))], [SM] + [VM] * 4)
    core = moved(stacked, other_core)
    (x_rows,) = call(
        rows_body,
        (spots, stacked, core, norm_in.reshape(1, -1)),
        [sds((1024 + HALO, 1024))],
        [SM] + [VM] * 3,
    )

    sums = [sds((1024 + HALO, 1408), f32)]
    (acc_own,) = call(
        own_body, (spots, x_rows, ups[0]), sums, [SM] + [VM] * 2, flops=2 * 1040 * 256 * 1408, nbytes=8 * MB
    )
    (acc,) = call(
        more_body,
        (spots, x_rows, acc_own, *ups[1:3]),
        sums,
        [SM] + [VM] * 4,
        flops=2 * 1040 * 512 * 1408,
        nbytes=8 * MB,
        limit=16,
        scratch=(pltpu.VMEM((1024 + HALO, 512), jnp.bfloat16), pltpu.VMEM((512, 1408), jnp.bfloat16)),
    )

    def hidden_of(half, gate):
        def body(*refs):
            hidden_body(half, *refs)

        (out,) = call(
            body,
            (spots, x_rows, acc, ups[3], ups[4], tap_rows, gate),
            [sds((512, 768))],
            [SM] + [VM] * 5 + [ANY],
            flops=2 * 528 * 256 * 1408 * 3,
            nbytes=4 * MB,
            limit=16,
            scratch=(pltpu.VMEM((256, 1408), jnp.bfloat16), pltpu.VMEM((512 + HALO, 1408), f32)),
        )
        return out

    def product_of(spot, hidden, dtype, gate):
        def body(*refs):
            product_body(spot, *refs)

        (out,) = call(
            body,
            (spots, hidden, d_all, gate),
            [sds((256, 1024), dtype)],
            [SM] + [VM] * 2 + [ANY],
            flops=2 * 256 * 768 * 1024,
            nbytes=2 * MB,
        )
        return out

    hidden_far = hidden_of(29, acc)
    (d_all,) = call(
        down_body,
        (spots, *downs, hidden_far),
        [sds((1024, 768))],
        [SM] + [VM] * 5 + [ANY],
    )
    first = product_of(32, hidden_far, jnp.bfloat16, d_all)
    got_far = moved(first, other_core)
    second = product_of(31, hidden_far, f32, first)
    sent = (second + got_far.astype(f32)).astype(jnp.bfloat16)
    back = moved(sent, other_chip)
    hidden_near = hidden_of(30, sent)
    third = product_of(32, hidden_near, jnp.bfloat16, sent)
    got_near = moved(third, other_core)
    fourth = product_of(31, hidden_near, f32, third)
    (out,) = call(final_body, (fourth, got_near, back, norm_out.reshape(1, -1)), [sds((256, 1024))], [VM] * 4)
    return out


def solution(mesh):
    split = Mesh(mesh.devices.reshape(NY, NX, NZ, NC), ALL)
    return jax.shard_map(
        shards,
        mesh=split,
        in_specs=(P(ALL, None), P(), P(FS, TP), P(FS, TP), P(None, TP), P(None, TP), P(TP, FS), P()),
        out_specs=P(ALL, None),
        check_vma=False,
    )
```

```python
import jax
import jax.numpy as jnp
from jax import lax
from jax.experimental import pallas as pl
from jax.experimental.pallas import tpu as pltpu
from jax.sharding import Mesh
from jax.sharding import PartitionSpec as P


FS = ("y", "x")
TP = ("z", "c")
ALL = ("y", "x", "z", "c")
NY, NX, NZ, NC = 4, 4, 8, 2
EPS = 1e-06
HALO = 16
MB = 1024 * 1024


def moved(array, target):
    pairs = []
    for y in range(NY):
        for x in range(NX):
            for z in range(NZ):
                for c in range(NC):
                    to = target(y, x, z, c)
                    if to is None:
                        continue
                    source = ((y * NX + x) * NZ + z) * NC + c
                    ty, tx, tz, tc = to
                    pairs.append((source, ((ty * NX + tx) * NZ + tz) * NC + tc))
    return lax.ppermute(array, ALL, pairs)


def quarter_to(k):
    def target(y, x, z, c):
        up = (z + k) % 2 == 0
        return (y, x, (z + k if up else z - k) % NZ, c)

    return target


def first_by(k):
    return lambda y, x, z, c: (y, (x + k) % NX, z, c) if c == 0 else ((y + k) % NY, x, z, c)


def second_by(k):
    return lambda y, x, z, c: ((y + k) % NY, x, z, c) if c == 0 else (y, (x + k) % NX, z, c)


def other_core(y, x, z, c):
    return (y, x, z, 1 - c)


def other_chip(y, x, z, c):
    return (y, x, z ^ 1, c)


def next_device(y, x, z, c):
    at = ((y * NX + x) * NZ + z) * NC + c + 1
    if at >= NY * NX * NZ * NC:
        return None
    return (at // (NX * NZ * NC), at // (NZ * NC) % NX, at // NC % NZ, at % NC)


def all_of_four(block, by):
    return block, moved(block, by(1)), moved(block, by(-1)), moved(block, by(2))


def ring_of_four(block, by):
    half = block.shape[0] // 2
    before = moved(block, by(1))
    after = moved(block, by(-1))
    top = moved(before[:half], by(1))
    bottom = moved(after[half:], by(-1))
    return block, before, after, top, bottom


VM = pl.BlockSpec(memory_space=pltpu.VMEM)
SM = pl.BlockSpec(memory_space=pltpu.SMEM)
ANY = pl.BlockSpec(memory_space=pl.ANY)


def call(body, ins, outs, specs, *, flops=MB, nbytes=MB, scratch=(), limit=16):
    return pl.pallas_call(
        body,
        out_shape=outs,
        in_specs=specs,
        out_specs=[VM] * len(outs),
        scratch_shapes=list(scratch),
        compiler_params=pltpu.CompilerParams(vmem_limit_bytes=limit * MB),
        cost_estimate=pl.CostEstimate(flops=flops, bytes_accessed=nbytes, transcendentals=0),
    )(*ins)


def sds(shape, dtype=jnp.bfloat16):
    return jax.ShapeDtypeStruct(shape, dtype)


def normed_rows(wide, scale):
    power = jnp.mean(wide * wide, axis=-1, keepdims=True)
    return wide * lax.rsqrt(power + EPS) * scale


def turned(wide):
    blocks = [wide[:, (y * NX + x) * 64 : (y * NX + x + 1) * 64] for x in range(NX) for y in range(NY)]
    return jnp.concatenate(blocks, axis=1)


def norm_body(spots, tokens, scale, out, last):
    rows = normed_rows(tokens[...].astype(jnp.float32), scale[...])
    last[...] = rows[256 - HALO :].astype(jnp.bfloat16)

    @pl.when(spots[24] == 0)
    def _():
        out[...] = rows.astype(jnp.bfloat16)

    @pl.when(spots[24] == 1)
    def _():
        out[...] = turned(rows).astype(jnp.bfloat16)


def join_body(own, halo, out):
    out[0:256, :] = own[...]
    out[256 : 256 + HALO, :] = halo[...]


def stack_body(spots, own, chip, out):
    out[0:256, :] = turned(own[0:256, :].astype(jnp.float32)).astype(jnp.bfloat16)
    out[256:512, :] = turned(chip[0:256, :].astype(jnp.float32)).astype(jnp.bfloat16)
    even = spots[29] == 512
    halo = jnp.where(even, own[256 : 256 + HALO, :].astype(jnp.float32), chip[256 : 256 + HALO, :].astype(jnp.float32))
    out[512 : 512 + HALO, :] = turned(halo).astype(jnp.bfloat16)


def rows_body(spots, own, chip, core, out):
    for k, ref, row in ((0, own, 0), (1, chip, 0), (2, core, 0), (3, core, 256)):
        where = pl.multiple_of(HALO + spots[16 + k], 16)
        out[pl.ds(where, 256), :] = ref[row : row + 256, :]
    even = spots[29] == 512

    @pl.when(spots[24] == 1)
    def _():
        out[0:HALO, :] = core[512 : 512 + HALO, :]

    @pl.when(jnp.logical_and(spots[24] == 0, even))
    def _():
        out[0:HALO, :] = own[256 : 256 + HALO, :]

    @pl.when(jnp.logical_and(spots[24] == 0, jnp.logical_not(even)))
    def _():
        out[0:HALO, :] = chip[256 : 256 + HALO, :]


def final_body(own, near, far_low, far_high, scale, out):
    for row, far in ((0, far_low), (128, far_high)):
        some = slice(row, row + 128)
        total = own[some, :] + near[some, :].astype(jnp.float32) + far[...].astype(jnp.float32)
        out[some, :] = normed_rows(total, scale[...]).astype(jnp.bfloat16)


PACK = 344


def three_parts(values):
    high = values.astype(jnp.bfloat16).astype(jnp.float32)
    rest = values - high
    middle = rest.astype(jnp.bfloat16).astype(jnp.float32)
    return [high, middle, rest - middle]


def pack_body(weights, taps, out):
    f32, bf16 = jnp.float32, jnp.bfloat16
    parts = three_parts(taps[0:3, :]) + three_parts(taps[3:6, :])
    rows = jnp.concatenate(parts + [jnp.zeros((6, 176), f32)], axis=0)
    rest = weights[:, 128:176].astype(f32)
    out[0:192, :] = weights[:, 0:128]
    out[320:344, :] = rows[:, 0:128].astype(bf16)
    pair = jnp.concatenate([rest[0:64], rest[64:128], jnp.zeros((64, 32), f32)], axis=1)
    out[192:256, :] = pair.astype(bf16)
    more = jnp.concatenate([rows[:, 128:176], jnp.zeros((40, 48), f32)], axis=0)
    gap = jnp.zeros((64, 16), f32)
    out[256:320, :] = jnp.concatenate([rest[128:192], gap, more, gap], axis=1).astype(bf16)


def arranged(v, g):
    return jnp.concatenate(
        [v[:, 0:256], g[:, 0:256], v[:, 256:512], g[:, 256:512], v[:, 512:640], g[:, 512:640], v[:, 640:704], g[:, 640:704]],
        axis=1,
    )


def assemble_body(p0, p1, p2, p3, both, taps):
    f32 = jnp.float32

    def wide(row, other, lane, count=64):
        pieces = []
        for p in (p0, p1, p2, p3):
            pieces.append(p[row : row + count, :].astype(f32))
            pieces.append(p[other : other + count, :].astype(f32)[:, lane : lane + 48])
        return jnp.concatenate(pieces, axis=1)

    both[:, 0:1408] = arranged(wide(0, 192, 0), wide(64, 192, 48)).astype(jnp.bfloat16)
    down = jnp.concatenate([wide(128, 256, 0), jnp.zeros((64, 64), f32)], axis=1)
    both[:, 1408:2176] = down.astype(jnp.bfloat16)
    parts = wide(320, 256, 64, 24)
    whole = [(parts[k : k + 3] + parts[k + 3 : k + 6]) + parts[k + 6 : k + 9] for k in (0, 9)]
    taps[...] = jnp.concatenate([arranged(*whole), jnp.zeros((5, 1408), f32)], axis=0)


def line_body(spots, b0, b1, b2, b3, up, down):
    for k, piece in enumerate((b0, b1, b2, b3)):
        where = pl.multiple_of(spots[20 + k], 64)
        up[pl.ds(where, 64), :] = piece[:, 0:1408]
        down[pl.ds(where, 64), :] = piece[:, 1408:2176]


def gelu(v):
    inner = v * (0.7978845608028654 + 0.035677408136300125 * (v * v))
    return 0.5 * v * (1.0 + jnp.tanh(inner))


GROUPS = ((0, 512), (512, 512), (1024, 384))


def own_body(spots, x_rows, w0, acc):
    x_some = x_rows[:, pl.ds(pl.multiple_of(spots[25], 256), 256)]
    for start, width in GROUPS:
        columns = slice(start, start + width)
        acc[:, columns] = jnp.dot(x_some, w0[:, columns], preferred_element_type=jnp.float32)


def more_body(spots, x_rows, before, w1, w2, acc, x_some, w_some):
    for k, piece in enumerate((w1, w2)):
        where = pl.multiple_of(spots[26 + k], 256)
        x_some[:, k * 256 : k * 256 + 256] = x_rows[:, pl.ds(where, 256)]
        w_some[k * 256 : k * 256 + 256, :] = piece[...]
    for start, width in GROUPS:
        columns = slice(start, start + width)
        acc[:, columns] = before[:, columns] + jnp.dot(
            x_some[...], w_some[:, columns], preferred_element_type=jnp.float32
        )


def down_body(spots, d0, d1, d2, d3, d4, gate, out):
    at = 0
    for piece in (d0, d1, d2, d3, d4):
        for row in range(0, piece.shape[0], 64):
            where = pl.multiple_of(spots[at], 64)
            out[pl.ds(where, 64), :] = piece[row : row + 64, :]
            at += 1


def hidden_body(half, spots, x_rows, acc, w3, w4, taps, gate, hidden, w_some, full):
    w_some[0:128, :] = w3[...]
    w_some[128:256, :] = w4[...]
    r0 = pl.multiple_of(spots[half], 512)
    where = pl.multiple_of(spots[28], 256)
    x_some = x_rows[pl.ds(r0, 512 + HALO), pl.ds(where, 256)]
    for number, (start, width) in enumerate(GROUPS):
        columns = slice(start, start + width)
        full[:, columns] = acc[pl.ds(r0, 512 + HALO), columns] + jnp.dot(
            x_some, w_some[:, columns], preferred_element_type=jnp.float32
        )
        scale = taps[:, columns]
        for row in range(0, 512, 64):
            near = full[row : row + 64 + HALO, columns]
            conv = near[14 : 14 + 64] * scale[0:1]
            conv = conv + near[15 : 15 + 64] * scale[1:2]
            conv = conv + near[16 : 16 + 64] * scale[2:3]
            some = slice(row, row + 64)
            if number < 2:
                made = gelu(conv[:, 256:512]) * conv[:, 0:256]
                hidden[some, number * 256 : number * 256 + 256] = made.astype(jnp.bfloat16)
            else:
                made = gelu(conv[:, 128:256]) * conv[:, 0:128]
                hidden[some, 512:640] = made.astype(jnp.bfloat16)
                tail = conv[:, 256:384]
                made = gelu(pltpu.roll(tail, 64, 1)) * tail
                lane = lax.broadcasted_iota(jnp.int32, made.shape, 1)
                hidden[some, 640:768] = jnp.where(lane < 64, made, 0.0).astype(jnp.bfloat16)


def product_body(spot, ahead, spots, hidden, d_all, gate, out):
    r0 = pl.multiple_of(spots[spot], 256)
    rows = out.shape[0]
    product = lax.dot_general(
        hidden[pl.ds(r0 + ahead, rows), :], d_all[...], (((1,), (1,)), ((), ())), preferred_element_type=jnp.float32
    )
    out[...] = product.astype(out.dtype)


def shards(tokens, norm_in, value_weight, gate_weight, value_taps, gate_taps, down_weight, norm_out):
    f32 = jnp.float32
    y, x, z, c = (lax.axis_index(name) for name in ALL)

    mine, across = jnp.where(c == 0, x, y), jnp.where(c == 0, y, x)
    near = [(mine + k) % 4 for k in (0, 3, 1, 2)]
    far = [(across + k) % 4 for k in (0, 3, 1, 2)]
    place_near, place_far = jnp.where(c == 0, 64, 256), jnp.where(c == 0, 256, 64)
    zb = z % 2
    blocks = [f * place_far + n * place_near for f in far for n in range(4)]
    members = [zb * 2 + c, (1 - zb) * 2 + c, zb * 2 + 1 - c, (1 - zb) * 2 + 1 - c]
    spots = jnp.stack(
        [b.astype(jnp.int32) for b in blocks + [m * 256 for m in members] + [n * 64 for n in near] + [c] + [f * 256 for f in far]
            + [(1 - zb) * 512, zb * 512, c * 256, (1 - c) * 256]]
    )

    (pack,) = call(
        pack_body,
        (
            jnp.concatenate([value_weight, gate_weight, down_weight.T], axis=0),
            jnp.concatenate([value_taps, gate_taps], axis=0),
        ),
        [sds((PACK, 128))],
        [VM] * 2,
    )
    packs = [pack] + [moved(pack, quarter_to(k)) for k in (1, 2, 3)]
    both, tap_rows = call(assemble_body, packs, [sds((64, 2176)), sds((8, 1408), f32)], [VM] * 4)
    up_line, down_line = call(
        line_body, (spots, *all_of_four(both, first_by)), [sds((256, 1408)), sds((256, 768))], [SM] + [VM] * 4
    )
    ups = ring_of_four(up_line, second_by)
    downs = ring_of_four(down_line, second_by)

    normed, last = call(
        norm_body,
        (spots, tokens, norm_in.reshape(1, -1)),
        [sds(tokens.shape), sds((HALO, 1024))],
        [SM, VM, VM],
    )
    halo = moved(last, next_device)
    (joined,) = call(join_body, (normed, halo), [sds((256 + HALO, 1024))], [VM] * 2)
    chip = moved(joined, other_chip)
    (stacked,) = call(stack_body, (spots, joined, chip), [sds((512 + HALO, 1024))], [SM, VM, VM])
    core = moved(stacked, other_core)
    (x_rows,) = call(rows_body, (spots, joined, chip, core), [sds((1024 + HALO, 1024))], [SM] + [VM] * 3)

    sums = [sds((1024 + HALO, 1408), f32)]
    (acc_own,) = call(
        own_body, (spots, x_rows, ups[0]), sums, [SM] + [VM] * 2, flops=2 * 1040 * 256 * 1408, nbytes=8 * MB
    )
    (acc,) = call(
        more_body,
        (spots, x_rows, acc_own, *ups[1:3]),
        sums,
        [SM] + [VM] * 4,
        flops=2 * 1040 * 512 * 1408,
        nbytes=8 * MB,
        limit=16,
        scratch=(pltpu.VMEM((1024 + HALO, 512), jnp.bfloat16), pltpu.VMEM((512, 1408), jnp.bfloat16)),
    )

    def hidden_of(half, gate):
        def body(*refs):
            hidden_body(half, *refs)

        (out,) = call(
            body,
            (spots, x_rows, acc, ups[3], ups[4], tap_rows, gate),
            [sds((512, 768))],
            [SM] + [VM] * 5 + [ANY],
            flops=2 * 528 * 256 * 1408 * 3,
            nbytes=4 * MB,
            limit=16,
            scratch=(pltpu.VMEM((256, 1408), jnp.bfloat16), pltpu.VMEM((512 + HALO, 1408), f32)),
        )
        return out

    def product_of(spot, hidden, dtype, gate, ahead=0, rows=256):
        def body(*refs):
            product_body(spot, ahead, *refs)

        (out,) = call(
            body,
            (spots, hidden, d_all, gate),
            [sds((rows, 1024), dtype)],
            [SM] + [VM] * 2 + [ANY],
            flops=2 * rows * 768 * 1024,
            nbytes=2 * MB,
        )
        return out

    hidden_far = hidden_of(29, acc)
    (d_all,) = call(
        down_body,
        (spots, *downs, hidden_far),
        [sds((1024, 768))],
        [SM] + [VM] * 5 + [ANY],
    )
    gate, back = d_all, []
    for ahead in (0, 128):
        away = product_of(32, hidden_far, jnp.bfloat16, gate, ahead, 128)
        got = moved(away, other_core)
        kept = product_of(31, hidden_far, f32, away, ahead, 128)
        gate = (kept + got.astype(f32)).astype(jnp.bfloat16)
        back.append(moved(gate, other_chip))
    hidden_near = hidden_of(30, gate)
    third = product_of(32, hidden_near, jnp.bfloat16, gate)
    got_near = moved(third, other_core)
    fourth = product_of(31, hidden_near, f32, third)
    (out,) = call(final_body, (fourth, got_near, *back, norm_out.reshape(1, -1)), [sds((256, 1024))], [VM] * 5)
    return out


def solution(mesh):
    split = Mesh(mesh.devices.reshape(NY, NX, NZ, NC), ALL)
    return jax.shard_map(
        shards,
        mesh=split,
        in_specs=(P(ALL, None), P(), P(FS, TP), P(FS, TP), P(None, TP), P(None, TP), P(TP, FS), P()),
        out_specs=P(ALL, None),
        check_vma=False,
    )
```

```python
import jax
import jax.numpy as jnp
from jax import lax
from jax.experimental import pallas as pl
from jax.experimental.pallas import tpu as pltpu
from jax.sharding import Mesh
from jax.sharding import PartitionSpec as P


FS = ("y", "x")
TP = ("z", "c")
ALL = ("y", "x", "z", "c")
NY, NX, NZ, NC = 4, 4, 8, 2
EPS = 1e-06
HALO = 16
MB = 1024 * 1024


def moved(array, target):
    pairs = []
    for y in range(NY):
        for x in range(NX):
            for z in range(NZ):
                for c in range(NC):
                    to = target(y, x, z, c)
                    if to is None:
                        continue
                    source = ((y * NX + x) * NZ + z) * NC + c
                    ty, tx, tz, tc = to
                    pairs.append((source, ((ty * NX + tx) * NZ + tz) * NC + tc))
    return lax.ppermute(array, ALL, pairs)


def quarter_to(k):
    def target(y, x, z, c):
        up = (z + k) % 2 == 0
        return (y, x, (z + k if up else z - k) % NZ, c)

    return target


def first_by(k):
    return lambda y, x, z, c: (y, (x + k) % NX, z, c) if c == 0 else ((y + k) % NY, x, z, c)


def second_by(k):
    return lambda y, x, z, c: ((y + k) % NY, x, z, c) if c == 0 else (y, (x + k) % NX, z, c)


def other_core(y, x, z, c):
    return (y, x, z, 1 - c)


def other_chip(y, x, z, c):
    return (y, x, z ^ 1, c)


def after_by(k):
    def target(y, x, z, c):
        at = ((y * NX + x) * NZ + z) * NC + c + k
        if at >= NY * NX * NZ * NC:
            return None
        return (at // (NX * NZ * NC), at // (NZ * NC) % NX, at // NC % NZ, at % NC)

    return target


def all_of_four(block, by):
    return block, moved(block, by(1)), moved(block, by(-1)), moved(block, by(2))


def ring_of_four(block, by):
    half = block.shape[0] // 2
    before = moved(block, by(1))
    after = moved(block, by(-1))
    top = moved(before[:half], by(1))
    bottom = moved(after[half:], by(-1))
    return block, before, after, top, bottom


VM = pl.BlockSpec(memory_space=pltpu.VMEM)
SM = pl.BlockSpec(memory_space=pltpu.SMEM)
ANY = pl.BlockSpec(memory_space=pl.ANY)


def call(body, ins, outs, specs, *, flops=MB, nbytes=MB, scratch=(), limit=16):
    return pl.pallas_call(
        body,
        out_shape=outs,
        in_specs=specs,
        out_specs=[VM] * len(outs),
        scratch_shapes=list(scratch),
        compiler_params=pltpu.CompilerParams(vmem_limit_bytes=limit * MB),
        cost_estimate=pl.CostEstimate(flops=flops, bytes_accessed=nbytes, transcendentals=0),
    )(*ins)


def sds(shape, dtype=jnp.bfloat16):
    return jax.ShapeDtypeStruct(shape, dtype)


def normed_rows(wide, scale):
    power = jnp.mean(wide * wide, axis=-1, keepdims=True)
    return wide * lax.rsqrt(power + EPS) * scale


def turned(wide):
    blocks = [wide[:, (y * NX + x) * 64 : (y * NX + x + 1) * 64] for x in range(NX) for y in range(NY)]
    return jnp.concatenate(blocks, axis=1)


def join_body(spots, tokens, halo, scale, out):
    rows = normed_rows(tokens[...].astype(jnp.float32), scale[...])
    ahead = normed_rows(halo[...].astype(jnp.float32), scale[...])
    out[256 : 256 + HALO, :] = ahead.astype(jnp.bfloat16)

    @pl.when(spots[24] == 0)
    def _():
        out[0:256, :] = rows.astype(jnp.bfloat16)

    @pl.when(spots[24] == 1)
    def _():
        out[0:256, :] = turned(rows).astype(jnp.bfloat16)


def stack_body(spots, own, chip, out):
    out[0:256, :] = turned(own[0:256, :].astype(jnp.float32)).astype(jnp.bfloat16)
    out[256:512, :] = turned(chip[0:256, :].astype(jnp.float32)).astype(jnp.bfloat16)
    even = spots[29] == 512
    halo = jnp.where(even, own[256 : 256 + HALO, :].astype(jnp.float32), chip[256 : 256 + HALO, :].astype(jnp.float32))
    out[512 : 512 + HALO, :] = turned(halo).astype(jnp.bfloat16)


def rows_body(spots, own, chip, core, out):
    for k, ref, row in ((0, own, 0), (1, chip, 0), (2, core, 0), (3, core, 256)):
        where = pl.multiple_of(HALO + spots[16 + k], 16)
        out[pl.ds(where, 256), :] = ref[row : row + 256, :]
    even = spots[29] == 512

    @pl.when(spots[24] == 1)
    def _():
        out[0:HALO, :] = core[512 : 512 + HALO, :]

    @pl.when(jnp.logical_and(spots[24] == 0, even))
    def _():
        out[0:HALO, :] = own[256 : 256 + HALO, :]

    @pl.when(jnp.logical_and(spots[24] == 0, jnp.logical_not(even)))
    def _():
        out[0:HALO, :] = chip[256 : 256 + HALO, :]


def final_body(own, near, far, scale, out):
    total = own[...] + near[...].astype(jnp.float32) + far[...].astype(jnp.float32)
    out[...] = normed_rows(total, scale[...]).astype(jnp.bfloat16)


PACK = 344


def three_parts(values):
    high = values.astype(jnp.bfloat16).astype(jnp.float32)
    rest = values - high
    middle = rest.astype(jnp.bfloat16).astype(jnp.float32)
    return [high, middle, rest - middle]


def pack_body(weights, taps, tokens, out, last):
    f32, bf16 = jnp.float32, jnp.bfloat16
    parts = three_parts(taps[0:3, :]) + three_parts(taps[3:6, :])
    rows = jnp.concatenate(parts + [jnp.zeros((6, 176), f32)], axis=0)
    last[...] = tokens[256 - HALO :, :]
    rest = weights[:, 128:176].astype(f32)
    out[0:192, :] = weights[:, 0:128]
    out[320:344, :] = rows[:, 0:128].astype(bf16)
    pair = jnp.concatenate([rest[0:64], rest[64:128], jnp.zeros((64, 32), f32)], axis=1)
    out[192:256, :] = pair.astype(bf16)
    more = jnp.concatenate([rows[:, 128:176], jnp.zeros((40, 48), f32)], axis=0)
    gap = jnp.zeros((64, 16), f32)
    out[256:320, :] = jnp.concatenate([rest[128:192], gap, more, gap], axis=1).astype(bf16)


def arranged(v, g):
    return jnp.concatenate(
        [v[:, 0:256], g[:, 0:256], v[:, 256:512], g[:, 256:512], v[:, 512:640], g[:, 512:640], v[:, 640:704], g[:, 640:704]],
        axis=1,
    )


def assemble_body(p0, p1, p2, p3, both, taps):
    f32 = jnp.float32

    def wide(row, other, lane, count=64):
        pieces = []
        for p in (p0, p1, p2, p3):
            pieces.append(p[row : row + count, :].astype(f32))
            pieces.append(p[other : other + count, :].astype(f32)[:, lane : lane + 48])
        return jnp.concatenate(pieces, axis=1)

    both[:, 0:1408] = arranged(wide(0, 192, 0), wide(64, 192, 48)).astype(jnp.bfloat16)
    down = jnp.concatenate([wide(128, 256, 0), jnp.zeros((64, 64), f32)], axis=1)
    both[:, 1408:2176] = down.astype(jnp.bfloat16)
    parts = wide(320, 256, 64, 24)
    whole = [(parts[k : k + 3] + parts[k + 3 : k + 6]) + parts[k + 6 : k + 9] for k in (0, 9)]
    taps[...] = jnp.concatenate([arranged(*whole), jnp.zeros((5, 1408), f32)], axis=0)


def line_body(spots, b0, b1, b2, b3, up, down):
    for k, piece in enumerate((b0, b1, b2, b3)):
        where = pl.multiple_of(spots[20 + k], 64)
        up[pl.ds(where, 64), :] = piece[:, 0:1408]
        down[pl.ds(where, 64), :] = piece[:, 1408:2176]


def gelu(v):
    inner = v * (0.7978845608028654 + 0.035677408136300125 * (v * v))
    return 0.5 * v * (1.0 + jnp.tanh(inner))


GROUPS = ((0, 512), (512, 512), (1024, 384))


def own_body(spots, x_rows, w0, acc):
    x_some = x_rows[:, pl.ds(pl.multiple_of(spots[25], 256), 256)]
    for start, width in GROUPS:
        columns = slice(start, start + width)
        acc[:, columns] = jnp.dot(x_some, w0[:, columns], preferred_element_type=jnp.float32)


def more_body(spots, x_rows, before, w1, w2, acc, x_some, w_some):
    for k, piece in enumerate((w1, w2)):
        where = pl.multiple_of(spots[26 + k], 256)
        x_some[:, k * 256 : k * 256 + 256] = x_rows[:, pl.ds(where, 256)]
        w_some[k * 256 : k * 256 + 256, :] = piece[...]
    for start, width in GROUPS:
        columns = slice(start, start + width)
        acc[:, columns] = before[:, columns] + jnp.dot(
            x_some[...], w_some[:, columns], preferred_element_type=jnp.float32
        )


def down_body(spots, d0, d1, d2, d3, d4, gate, out):
    at = 0
    for piece in (d0, d1, d2, d3, d4):
        for row in range(0, piece.shape[0], 64):
            where = pl.multiple_of(spots[at], 64)
            out[pl.ds(where, 64), :] = piece[row : row + 64, :]
            at += 1


def hidden_body(half, spots, x_rows, acc, w3, w4, taps, gate, hidden, w_some, full):
    w_some[0:128, :] = w3[...]
    w_some[128:256, :] = w4[...]
    r0 = pl.multiple_of(spots[half], 512)
    where = pl.multiple_of(spots[28], 256)
    x_some = x_rows[pl.ds(r0, 512 + HALO), pl.ds(where, 256)]
    for number, (start, width) in enumerate(GROUPS):
        columns = slice(start, start + width)
        full[:, columns] = acc[pl.ds(r0, 512 + HALO), columns] + jnp.dot(
            x_some, w_some[:, columns], preferred_element_type=jnp.float32
        )
        scale = taps[:, columns]
        for row in range(0, 512, 64):
            near = full[row : row + 64 + HALO, columns]
            conv = near[14 : 14 + 64] * scale[0:1]
            conv = conv + near[15 : 15 + 64] * scale[1:2]
            conv = conv + near[16 : 16 + 64] * scale[2:3]
            some = slice(row, row + 64)
            if number < 2:
                made = gelu(conv[:, 256:512]) * conv[:, 0:256]
                hidden[some, number * 256 : number * 256 + 256] = made.astype(jnp.bfloat16)
            else:
                made = gelu(conv[:, 128:256]) * conv[:, 0:128]
                hidden[some, 512:640] = made.astype(jnp.bfloat16)
                tail = conv[:, 256:384]
                made = gelu(pltpu.roll(tail, 64, 1)) * tail
                lane = lax.broadcasted_iota(jnp.int32, made.shape, 1)
                hidden[some, 640:768] = jnp.where(lane < 64, made, 0.0).astype(jnp.bfloat16)


def product_body(spot, spots, hidden, d_all, gate, out):
    r0 = pl.multiple_of(spots[spot], 256)
    product = lax.dot_general(
        hidden[pl.ds(r0, 256), :], d_all[...], (((1,), (1,)), ((), ())), preferred_element_type=jnp.float32
    )
    out[...] = product.astype(out.dtype)


def shards(tokens, norm_in, value_weight, gate_weight, value_taps, gate_taps, down_weight, norm_out):
    f32 = jnp.float32
    y, x, z, c = (lax.axis_index(name) for name in ALL)

    mine, across = jnp.where(c == 0, x, y), jnp.where(c == 0, y, x)
    near = [(mine + k) % 4 for k in (0, 3, 1, 2)]
    far = [(across + k) % 4 for k in (0, 3, 1, 2)]
    place_near, place_far = jnp.where(c == 0, 64, 256), jnp.where(c == 0, 256, 64)
    zb = z % 2
    blocks = [f * place_far + n * place_near for f in far for n in range(4)]
    members = [zb * 2 + c, (1 - zb) * 2 + c, zb * 2 + 1 - c, (1 - zb) * 2 + 1 - c]
    spots = jnp.stack(
        [b.astype(jnp.int32) for b in blocks + [m * 256 for m in members] + [n * 64 for n in near] + [c] + [f * 256 for f in far]
            + [(1 - zb) * 512, zb * 512, c * 256, (1 - c) * 256]]
    )

    pack, last = call(
        pack_body,
        (
            jnp.concatenate([value_weight, gate_weight, down_weight.T], axis=0),
            jnp.concatenate([value_taps, gate_taps], axis=0),
            tokens,
        ),
        [sds((PACK, 128)), sds((HALO, 1024))],
        [VM] * 3,
    )
    halo = moved(last, after_by(1))
    packs = [pack] + [moved(pack, quarter_to(k)) for k in (1, 2, 3)]
    both, tap_rows = call(assemble_body, packs, [sds((64, 2176)), sds((8, 1408), f32)], [VM] * 4)
    up_line, down_line = call(
        line_body, (spots, *all_of_four(both, first_by)), [sds((256, 1408)), sds((256, 768))], [SM] + [VM] * 4
    )
    ups = ring_of_four(up_line, second_by)
    downs = ring_of_four(down_line, second_by)

    (joined,) = call(
        join_body,
        (spots, tokens, halo, norm_in.reshape(1, -1)),
        [sds((256 + HALO, 1024))],
        [SM] + [VM] * 3,
    )
    chip = moved(joined, other_chip)
    (stacked,) = call(stack_body, (spots, joined, chip), [sds((512 + HALO, 1024))], [SM, VM, VM])
    core = moved(stacked, other_core)
    (x_rows,) = call(rows_body, (spots, joined, chip, core), [sds((1024 + HALO, 1024))], [SM] + [VM] * 3)

    sums = [sds((1024 + HALO, 1408), f32)]
    (acc_own,) = call(
        own_body, (spots, x_rows, ups[0]), sums, [SM] + [VM] * 2, flops=2 * 1040 * 256 * 1408, nbytes=8 * MB
    )
    (acc,) = call(
        more_body,
        (spots, x_rows, acc_own, *ups[1:3]),
        sums,
        [SM] + [VM] * 4,
        flops=2 * 1040 * 512 * 1408,
        nbytes=8 * MB,
        limit=16,
        scratch=(pltpu.VMEM((1024 + HALO, 512), jnp.bfloat16), pltpu.VMEM((512, 1408), jnp.bfloat16)),
    )

    def hidden_of(half, gate):
        def body(*refs):
            hidden_body(half, *refs)

        (out,) = call(
            body,
            (spots, x_rows, acc, ups[3], ups[4], tap_rows, gate),
            [sds((512, 768))],
            [SM] + [VM] * 5 + [ANY],
            flops=2 * 528 * 256 * 1408 * 3,
            nbytes=4 * MB,
            limit=16,
            scratch=(pltpu.VMEM((256, 1408), jnp.bfloat16), pltpu.VMEM((512 + HALO, 1408), f32)),
        )
        return out

    def product_of(spot, hidden, dtype, gate):
        def body(*refs):
            product_body(spot, *refs)

        (out,) = call(
            body,
            (spots, hidden, d_all, gate),
            [sds((256, 1024), dtype)],
            [SM] + [VM] * 2 + [ANY],
            flops=2 * 256 * 768 * 1024,
            nbytes=2 * MB,
        )
        return out

    hidden_far = hidden_of(29, acc)
    (d_all,) = call(
        down_body,
        (spots, *downs, hidden_far),
        [sds((1024, 768))],
        [SM] + [VM] * 5 + [ANY],
    )
    first = product_of(32, hidden_far, jnp.bfloat16, d_all)
    got_far = moved(first, other_core)
    second = product_of(31, hidden_far, f32, first)
    sent = (second + got_far.astype(f32)).astype(jnp.bfloat16)
    back = moved(sent, other_chip)
    hidden_near = hidden_of(30, sent)
    third = product_of(32, hidden_near, jnp.bfloat16, sent)
    got_near = moved(third, other_core)
    fourth = product_of(31, hidden_near, f32, third)
    (out,) = call(final_body, (fourth, got_near, back, norm_out.reshape(1, -1)), [sds((256, 1024))], [VM] * 4)
    return out


def solution(mesh):
    split = Mesh(mesh.devices.reshape(NY, NX, NZ, NC), ALL)
    return jax.shard_map(
        shards,
        mesh=split,
        in_specs=(P(ALL, None), P(), P(FS, TP), P(FS, TP), P(None, TP), P(None, TP), P(TP, FS), P()),
        out_specs=P(ALL, None),
        check_vma=False,
    )
```

```python
import jax
import jax.numpy as jnp
from jax import lax
from jax.experimental import pallas as pl
from jax.experimental.pallas import tpu as pltpu
from jax.sharding import Mesh
from jax.sharding import PartitionSpec as P


FS = ("y", "x")
TP = ("z", "c")
ALL = ("y", "x", "z", "c")
NY, NX, NZ, NC = 4, 4, 8, 2
EPS = 1e-06
HALO = 16
BLOCK = 256 + HALO
MB = 1024 * 1024


def moved(array, target):
    pairs = []
    for y in range(NY):
        for x in range(NX):
            for z in range(NZ):
                for c in range(NC):
                    to = target(y, x, z, c)
                    if to is None:
                        continue
                    source = ((y * NX + x) * NZ + z) * NC + c
                    ty, tx, tz, tc = to
                    pairs.append((source, ((ty * NX + tx) * NZ + tz) * NC + tc))
    return lax.ppermute(array, ALL, pairs)


def same_parity(k):
    return lambda y, x, z, c: (y, x, (z + k) % NZ, c)


def first_by(k):
    return lambda y, x, z, c: (y, (x + k) % NX, z, c) if c == 0 else ((y + k) % NY, x, z, c)


def second_by(k):
    return lambda y, x, z, c: ((y + k) % NY, x, z, c) if c == 0 else (y, (x + k) % NX, z, c)


def other_core(y, x, z, c):
    return (y, x, z, 1 - c)


def to_helper(y, x, z, c):
    return (y, x, (z - 1 if c == 0 else z + 1) % NZ, c)


def from_helper(y, x, z, c):
    return (y, x, (z + 1 if c == 0 else z - 1) % NZ, c)


def next_device(y, x, z, c):
    at = ((y * NX + x) * NZ + z) * NC + c + 1
    if at >= NY * NX * NZ * NC:
        return None
    return (at // (NX * NZ * NC), at // (NZ * NC) % NX, at // NC % NZ, at % NC)


def all_of_four(block, by):
    return block, moved(block, by(1)), moved(block, by(-1)), moved(block, by(2))


def ring_of_four(block, by):
    half = block.shape[0] // 2
    before = moved(block, by(1))
    after = moved(block, by(-1))
    top = moved(before[:half], by(1))
    bottom = moved(after[half:], by(-1))
    return block, before, after, top, bottom


VM = pl.BlockSpec(memory_space=pltpu.VMEM)
SM = pl.BlockSpec(memory_space=pltpu.SMEM)
ANY = pl.BlockSpec(memory_space=pl.ANY)


def call(body, ins, outs, specs, *, flops=MB, nbytes=MB, scratch=(), limit=16):
    return pl.pallas_call(
        body,
        out_shape=outs,
        in_specs=specs,
        out_specs=[VM] * len(outs),
        scratch_shapes=list(scratch),
        compiler_params=pltpu.CompilerParams(vmem_limit_bytes=limit * MB),
        cost_estimate=pl.CostEstimate(flops=flops, bytes_accessed=nbytes, transcendentals=0),
    )(*ins)


def sds(shape, dtype=jnp.bfloat16):
    return jax.ShapeDtypeStruct(shape, dtype)


def normed_rows(wide, scale):
    power = jnp.mean(wide * wide, axis=-1, keepdims=True)
    return wide * lax.rsqrt(power + EPS) * scale


def turned(wide):
    blocks = [wide[:, (y * NX + x) * 64 : (y * NX + x + 1) * 64] for x in range(NX) for y in range(NY)]
    return jnp.concatenate(blocks, axis=1)


def norm_body(spots, tokens, scale, out, last):
    rows = normed_rows(tokens[...].astype(jnp.float32), scale[...])
    last[...] = rows[256 - HALO :].astype(jnp.bfloat16)

    @pl.when(spots[24] == 0)
    def _():
        out[...] = rows.astype(jnp.bfloat16)

    @pl.when(spots[24] == 1)
    def _():
        out[...] = turned(rows).astype(jnp.bfloat16)


def join_body(spots, own, halo, out):
    out[HALO:BLOCK, :] = own[...]

    @pl.when(spots[24] == 0)
    def _():
        out[0:HALO, :] = halo[...]

    @pl.when(spots[24] == 1)
    def _():
        out[0:HALO, :] = turned(halo[...].astype(jnp.float32)).astype(jnp.bfloat16)


def stack_body(own, chip, out):
    out[0:BLOCK, :] = turned(own[...].astype(jnp.float32)).astype(jnp.bfloat16)
    out[BLOCK : 2 * BLOCK, :] = turned(chip[...].astype(jnp.float32)).astype(jnp.bfloat16)


def rows_body(spots, own, chip, core, out):
    for k, ref, row in ((0, own, 0), (1, chip, 0), (2, core, 0), (3, core, BLOCK)):
        where = pl.multiple_of(spots[16 + k], 16)
        out[pl.ds(where, BLOCK), :] = ref[row : row + BLOCK, :]


def final_body(own, near, far, scale, out):
    total = own[...] + near[...].astype(jnp.float32) + far[...].astype(jnp.float32)
    out[...] = normed_rows(total, scale[...]).astype(jnp.bfloat16)


PACK = 344


def three_parts(values):
    high = values.astype(jnp.bfloat16).astype(jnp.float32)
    rest = values - high
    middle = rest.astype(jnp.bfloat16).astype(jnp.float32)
    return [high, middle, rest - middle]


def pack_body(weights, taps, out):
    f32, bf16 = jnp.float32, jnp.bfloat16
    parts = three_parts(taps[0:3, :]) + three_parts(taps[3:6, :])
    rows = jnp.concatenate(parts + [jnp.zeros((6, 176), f32)], axis=0)
    rest = weights[:, 128:176].astype(f32)
    out[0:192, :] = weights[:, 0:128]
    out[320:344, :] = rows[:, 0:128].astype(bf16)
    pair = jnp.concatenate([rest[0:64], rest[64:128], jnp.zeros((64, 32), f32)], axis=1)
    out[192:256, :] = pair.astype(bf16)
    more = jnp.concatenate([rows[:, 128:176], jnp.zeros((40, 48), f32)], axis=0)
    gap = jnp.zeros((64, 16), f32)
    out[256:320, :] = jnp.concatenate([rest[128:192], gap, more, gap], axis=1).astype(bf16)


def arranged(v, g):
    return jnp.concatenate(
        [v[:, 0:256], g[:, 0:256], v[:, 256:512], g[:, 256:512], v[:, 512:640], g[:, 512:640], v[:, 640:704], g[:, 640:704]],
        axis=1,
    )


def assemble_body(p0, p1, p2, p3, both, taps):
    f32 = jnp.float32

    def wide(row, other, lane, count=64):
        pieces = []
        for p in (p0, p1, p2, p3):
            pieces.append(p[row : row + count, :].astype(f32))
            pieces.append(p[other : other + count, :].astype(f32)[:, lane : lane + 48])
        return jnp.concatenate(pieces, axis=1)

    both[:, 0:1408] = arranged(wide(0, 192, 0), wide(64, 192, 48)).astype(jnp.bfloat16)
    down = jnp.concatenate([wide(128, 256, 0), jnp.zeros((64, 64), f32)], axis=1)
    both[:, 1408:2176] = down.astype(jnp.bfloat16)
    parts = wide(320, 256, 64, 24)
    whole = [(parts[k : k + 3] + parts[k + 3 : k + 6]) + parts[k + 6 : k + 9] for k in (0, 9)]
    taps[...] = jnp.concatenate([arranged(*whole), jnp.zeros((5, 1408), f32)], axis=0)


def line_body(spots, b0, b1, b2, b3, up, down):
    for k, piece in enumerate((b0, b1, b2, b3)):
        where = pl.multiple_of(spots[20 + k], 64)
        up[pl.ds(where, 64), :] = piece[:, 0:1408]
        down[pl.ds(where, 64), :] = piece[:, 1408:2176]


def gelu(v):
    inner = v * (0.7978845608028654 + 0.035677408136300125 * (v * v))
    return 0.5 * v * (1.0 + jnp.tanh(inner))


GROUPS = ((0, 512), (512, 512), (1024, 384))


def own_body(spots, x_rows, w0, acc):
    x_some = x_rows[:, pl.ds(pl.multiple_of(spots[25], 256), 256)]
    for start, width in GROUPS:
        columns = slice(start, start + width)
        acc[:, columns] = jnp.dot(x_some, w0[:, columns], preferred_element_type=jnp.float32)


def more_body(spots, x_rows, before, w1, w2, acc, x_some, w_some):
    for k, piece in enumerate((w1, w2)):
        where = pl.multiple_of(spots[26 + k], 256)
        x_some[:, k * 256 : k * 256 + 256] = x_rows[:, pl.ds(where, 256)]
        w_some[k * 256 : k * 256 + 256, :] = piece[...]
    for start, width in GROUPS:
        columns = slice(start, start + width)
        acc[:, columns] = before[:, columns] + jnp.dot(
            x_some[...], w_some[:, columns], preferred_element_type=jnp.float32
        )


def down_body(spots, d0, d1, d2, d3, d4, gate, out):
    at = 0
    for piece in (d0, d1, d2, d3, d4):
        for row in range(0, piece.shape[0], 64):
            where = pl.multiple_of(spots[at], 64)
            out[pl.ds(where, 64), :] = piece[row : row + 64, :]
            at += 1


def hidden_body(half, spots, x_rows, acc, w3, w4, taps, gate, hidden, w_some, full):
    w_some[0:128, :] = w3[...]
    w_some[128:256, :] = w4[...]
    r0 = half * 2 * BLOCK
    where = pl.multiple_of(spots[28], 256)
    x_some = x_rows[r0 : r0 + 2 * BLOCK, pl.ds(where, 256)]
    for number, (start, width) in enumerate(GROUPS):
        columns = slice(start, start + width)
        full[:, columns] = acc[r0 : r0 + 2 * BLOCK, columns] + jnp.dot(
            x_some, w_some[:, columns], preferred_element_type=jnp.float32
        )
        scale = taps[:, columns]
        for row in range(0, 512, 64):
            at = row + HALO * (row // 256)
            near = full[at : at + 64 + HALO, columns]
            conv = near[14 : 14 + 64] * scale[0:1]
            conv = conv + near[15 : 15 + 64] * scale[1:2]
            conv = conv + near[16 : 16 + 64] * scale[2:3]
            some = slice(row, row + 64)
            if number < 2:
                made = gelu(conv[:, 256:512]) * conv[:, 0:256]
                hidden[some, number * 256 : number * 256 + 256] = made.astype(jnp.bfloat16)
            else:
                made = gelu(conv[:, 128:256]) * conv[:, 0:128]
                hidden[some, 512:640] = made.astype(jnp.bfloat16)
                tail = conv[:, 256:384]
                made = gelu(pltpu.roll(tail, 64, 1)) * tail
                lane = lax.broadcasted_iota(jnp.int32, made.shape, 1)
                hidden[some, 640:768] = jnp.where(lane < 64, made, 0.0).astype(jnp.bfloat16)


def product_body(spot, spots, hidden, d_all, gate, out):
    r0 = pl.multiple_of(spots[spot], 256)
    product = lax.dot_general(
        hidden[pl.ds(r0, 256), :], d_all[...], (((1,), (1,)), ((), ())), preferred_element_type=jnp.float32
    )
    out[...] = product.astype(out.dtype)


def shards(tokens, norm_in, value_weight, gate_weight, value_taps, gate_taps, down_weight, norm_out):
    f32 = jnp.float32
    y, x, _, c = (lax.axis_index(name) for name in ALL)

    mine, across = jnp.where(c == 0, x, y), jnp.where(c == 0, y, x)
    near = [(mine + k) % 4 for k in (0, 3, 1, 2)]
    far = [(across + k) % 4 for k in (0, 3, 1, 2)]
    place_near, place_far = jnp.where(c == 0, 64, 256), jnp.where(c == 0, 256, 64)
    blocks = [f * place_far + n * place_near for f in far for n in range(4)]
    members = [2 + c, c, 3 - c, 1 - c]
    spots = jnp.stack(
        [b.astype(jnp.int32) for b in blocks + [m * BLOCK for m in members] + [n * 64 for n in near] + [c] + [f * 256 for f in far]
            + [c * 256, (1 - c) * 256]]
    )

    (pack,) = call(
        pack_body,
        (
            jnp.concatenate([value_weight, gate_weight, down_weight.T], axis=0),
            jnp.concatenate([value_taps, gate_taps], axis=0),
        ),
        [sds((PACK, 128))],
        [VM] * 2,
    )
    packs = [pack] + [moved(pack, same_parity(k)) for k in (4, 2, -2)]
    both, tap_rows = call(assemble_body, packs, [sds((64, 2176)), sds((8, 1408), f32)], [VM] * 4)
    up_line, down_line = call(
        line_body, (spots, *all_of_four(both, first_by)), [sds((256, 1408)), sds((256, 768))], [SM] + [VM] * 4
    )
    ups = ring_of_four(up_line, second_by)
    downs = ring_of_four(down_line, second_by)

    normed, last = call(
        norm_body,
        (spots, tokens, norm_in.reshape(1, -1)),
        [sds(tokens.shape), sds((HALO, 1024))],
        [SM, VM, VM],
    )
    halo = moved(last, next_device)
    (joined,) = call(join_body, (spots, normed, halo), [sds((BLOCK, 1024))], [SM] + [VM] * 2)
    chip = moved(joined, to_helper)
    (stacked,) = call(stack_body, (joined, chip), [sds((2 * BLOCK, 1024))], [VM, VM])
    core = moved(stacked, other_core)
    (x_rows,) = call(rows_body, (spots, joined, chip, core), [sds((4 * BLOCK, 1024))], [SM] + [VM] * 3)

    sums = [sds((4 * BLOCK, 1408), f32)]
    (acc_own,) = call(
        own_body, (spots, x_rows, ups[0]), sums, [SM] + [VM] * 2, flops=2 * 1040 * 256 * 1408, nbytes=8 * MB
    )
    (acc,) = call(
        more_body,
        (spots, x_rows, acc_own, *ups[1:3]),
        sums,
        [SM] + [VM] * 4,
        flops=2 * 1088 * 512 * 1408,
        nbytes=8 * MB,
        limit=16,
        scratch=(pltpu.VMEM((4 * BLOCK, 512), jnp.bfloat16), pltpu.VMEM((512, 1408), jnp.bfloat16)),
    )

    def hidden_of(half, gate):
        def body(*refs):
            hidden_body(half, *refs)

        (out,) = call(
            body,
            (spots, x_rows, acc, ups[3], ups[4], tap_rows, gate),
            [sds((512, 768))],
            [SM] + [VM] * 5 + [ANY],
            flops=2 * 544 * 256 * 1408 * 3,
            nbytes=4 * MB,
            limit=16,
            scratch=(pltpu.VMEM((256, 1408), jnp.bfloat16), pltpu.VMEM((2 * BLOCK, 1408), f32)),
        )
        return out

    def product_of(spot, hidden, dtype, gate):
        def body(*refs):
            product_body(spot, *refs)

        (out,) = call(
            body,
            (spots, hidden, d_all, gate),
            [sds((256, 1024), dtype)],
            [SM] + [VM] * 2 + [ANY],
            flops=2 * 256 * 768 * 1024,
            nbytes=2 * MB,
        )
        return out

    hidden_far = hidden_of(0, acc)
    (d_all,) = call(
        down_body,
        (spots, *downs, hidden_far),
        [sds((1024, 768))],
        [SM] + [VM] * 5 + [ANY],
    )
    first = product_of(30, hidden_far, jnp.bfloat16, d_all)
    got_far = moved(first, other_core)
    second = product_of(29, hidden_far, f32, first)
    sent = (second + got_far.astype(f32)).astype(jnp.bfloat16)
    back = moved(sent, from_helper)
    hidden_near = hidden_of(1, sent)
    third = product_of(30, hidden_near, jnp.bfloat16, sent)
    got_near = moved(third, other_core)
    fourth = product_of(29, hidden_near, f32, third)
    (out,) = call(final_body, (fourth, got_near, back, norm_out.reshape(1, -1)), [sds((256, 1024))], [VM] * 4)
    return out


def solution(mesh):
    split = Mesh(mesh.devices.reshape(NY, NX, NZ, NC), ALL)
    return jax.shard_map(
        shards,
        mesh=split,
        in_specs=(P(ALL, None), P(), P(FS, TP), P(FS, TP), P(None, TP), P(None, TP), P(TP, FS), P()),
        out_specs=P(ALL, None),
        check_vma=False,
    )
```

```python
import jax
import jax.numpy as jnp
from jax import lax
from jax.experimental import pallas as pl
from jax.experimental.pallas import tpu as pltpu
from jax.sharding import Mesh
from jax.sharding import PartitionSpec as P


FS = ("y", "x")
TP = ("z", "c")
ALL = ("y", "x", "z", "c")
NY, NX, NZ, NC = 4, 4, 8, 2
EPS = 1e-06
HALO = 16
BLOCK = 256 + HALO
MB = 1024 * 1024


def moved(array, target):
    pairs = []
    for y in range(NY):
        for x in range(NX):
            for z in range(NZ):
                for c in range(NC):
                    to = target(y, x, z, c)
                    if to is None:
                        continue
                    source = ((y * NX + x) * NZ + z) * NC + c
                    ty, tx, tz, tc = to
                    pairs.append((source, ((ty * NX + tx) * NZ + tz) * NC + tc))
    return lax.ppermute(array, ALL, pairs)


def same_parity(k):
    return lambda y, x, z, c: (y, x, (z + k) % NZ, c)


def first_by(k):
    return lambda y, x, z, c: (y, (x + k) % NX, z, c) if c == 0 else ((y + k) % NY, x, z, c)


def second_by(k):
    return lambda y, x, z, c: ((y + k) % NY, x, z, c) if c == 0 else (y, (x + k) % NX, z, c)


def other_core(y, x, z, c):
    return (y, x, z, 1 - c)


def to_helper(y, x, z, c):
    return (y, x, (z - 1 if c == 0 else z + 1) % NZ, c)


def from_helper(y, x, z, c):
    return (y, x, (z + 1 if c == 0 else z - 1) % NZ, c)


def next_device(y, x, z, c):
    at = ((y * NX + x) * NZ + z) * NC + c + 1
    if at >= NY * NX * NZ * NC:
        return None
    return (at // (NX * NZ * NC), at // (NZ * NC) % NX, at // NC % NZ, at % NC)


def all_of_four(block, by):
    return block, moved(block, by(1)), moved(block, by(-1)), moved(block, by(2))


def ring_of_four(block, by):
    half = block.shape[0] // 2
    before = moved(block, by(1))
    after = moved(block, by(-1))
    top = moved(before[:half], by(1))
    bottom = moved(after[half:], by(-1))
    return block, before, after, top, bottom


VM = pl.BlockSpec(memory_space=pltpu.VMEM)
ANY = pl.BlockSpec(memory_space=pl.ANY)


def call(body, ins, outs, specs, *, flops=MB, nbytes=MB, scratch=(), limit=16):
    return pl.pallas_call(
        body,
        out_shape=outs,
        in_specs=specs,
        out_specs=[VM] * len(outs),
        scratch_shapes=list(scratch),
        compiler_params=pltpu.CompilerParams(vmem_limit_bytes=limit * MB),
        cost_estimate=pl.CostEstimate(flops=flops, bytes_accessed=nbytes, transcendentals=0),
    )(*ins)


def sds(shape, dtype=jnp.bfloat16):
    return jax.ShapeDtypeStruct(shape, dtype)


def here():
    y, x, c = lax.axis_index("y"), lax.axis_index("x"), lax.axis_index("c")
    mine, across = jnp.where(c == 0, x, y), jnp.where(c == 0, y, x)
    near = [(mine + k) & 3 for k in (0, 3, 1, 2)]
    far = [(across + k) & 3 for k in (0, 3, 1, 2)]
    place_near, place_far = jnp.where(c == 0, 64, 256), jnp.where(c == 0, 256, 64)
    blocks = [f * place_far + n * place_near for f in far for n in range(4)]
    members = [2 + c, c, 3 - c, 1 - c]
    spots = blocks + [m * BLOCK for m in members] + [n * 64 for n in near] + [c]
    return spots + [f * 256 for f in far] + [c * 256, (1 - c) * 256]


def placed(body, *fixed):
    return lambda *refs: body(*fixed, here(), *refs)


def normed_rows(wide, scale):
    power = jnp.mean(wide * wide, axis=-1, keepdims=True)
    return wide * lax.rsqrt(power + EPS) * scale


def turned(wide):
    blocks = [wide[:, (y * NX + x) * 64 : (y * NX + x + 1) * 64] for x in range(NX) for y in range(NY)]
    return jnp.concatenate(blocks, axis=1)


def norm_body(spots, tokens, scale, out, last):
    rows = normed_rows(tokens[...].astype(jnp.float32), scale[...])
    last[...] = rows[256 - HALO :].astype(jnp.bfloat16)

    @pl.when(spots[24] == 0)
    def _():
        out[...] = rows.astype(jnp.bfloat16)

    @pl.when(spots[24] == 1)
    def _():
        out[...] = turned(rows).astype(jnp.bfloat16)


def join_body(spots, own, halo, out):
    out[HALO:BLOCK, :] = own[...]

    @pl.when(spots[24] == 0)
    def _():
        out[0:HALO, :] = halo[...]

    @pl.when(spots[24] == 1)
    def _():
        out[0:HALO, :] = turned(halo[...].astype(jnp.float32)).astype(jnp.bfloat16)


def stack_body(own, chip, out):
    out[0:BLOCK, :] = turned(own[...].astype(jnp.float32)).astype(jnp.bfloat16)
    out[BLOCK : 2 * BLOCK, :] = turned(chip[...].astype(jnp.float32)).astype(jnp.bfloat16)


def rows_body(spots, own, chip, core, out):
    for k, ref, row in ((0, own, 0), (1, chip, 0), (2, core, 0), (3, core, BLOCK)):
        where = pl.multiple_of(spots[16 + k], 16)
        out[pl.ds(where, BLOCK), :] = ref[row : row + BLOCK, :]


def final_body(own, near, far, scale, out):
    total = own[...] + near[...].astype(jnp.float32) + far[...].astype(jnp.float32)
    out[...] = normed_rows(total, scale[...]).astype(jnp.bfloat16)


PACK = 304


def three_parts(values):
    high = values.astype(jnp.bfloat16).astype(jnp.float32)
    rest = values - high
    middle = rest.astype(jnp.bfloat16).astype(jnp.float32)
    return [high, middle, rest - middle]


def pack_body(joint, out):
    f32, bf16 = jnp.float32, jnp.bfloat16
    taps = joint[192:198, :]
    rows = jnp.concatenate(three_parts(taps[0:3, :]) + three_parts(taps[3:6, :]), axis=0)
    out[0:192, :] = joint[0:192, 0:128].astype(bf16)
    value, gate, down = (joint[k : k + 64, 128:176] for k in (0, 64, 128))
    out[192:256, :] = jnp.concatenate([value, gate, down[:, 0:32]], axis=1).astype(bf16)
    folded = [down[k : k + 16, 32:48] for k in (0, 16, 32, 48)]
    left = jnp.concatenate(folded + [rows[0:16, 128:176], jnp.zeros((16, 16), f32)], axis=1)
    out[256:272, :] = left.astype(bf16)
    ends = jnp.concatenate([rows[16:18, 128:176], jnp.zeros((2, 80), f32)], axis=1)
    gap = jnp.zeros((6, 128), f32)
    out[272:304, :] = jnp.concatenate([rows[:, 0:128], gap, ends, gap], axis=0).astype(bf16)


def arranged(v, g):
    return jnp.concatenate(
        [v[:, 0:256], g[:, 0:256], v[:, 256:512], g[:, 256:512], v[:, 512:640], g[:, 512:640], v[:, 640:704], g[:, 640:704]],
        axis=1,
    )


def assemble_body(p0, p1, p2, p3, both, taps):
    f32 = jnp.float32
    values, gates, downs, parts = [], [], [], []
    for p in (p0, p1, p2, p3):
        other = p[192:256, :].astype(f32)
        left = p[256:272, :].astype(f32)
        rows = p[272:304, :].astype(f32)
        folded = jnp.concatenate([left[:, k : k + 16] for k in (0, 16, 32, 48)], axis=0)
        values += [p[0:64, :].astype(f32), other[:, 0:48]]
        gates += [p[64:128, :].astype(f32), other[:, 48:96]]
        downs += [p[128:192, :].astype(f32), other[:, 96:128], folded]
        parts += [rows[0:18], jnp.concatenate([left[:, 64:112], rows[24:26, 0:48]], axis=0)]
    both[:, 0:1408] = arranged(jnp.concatenate(values, axis=1), jnp.concatenate(gates, axis=1)).astype(jnp.bfloat16)
    both[:, 1408:2176] = jnp.concatenate(downs + [jnp.zeros((64, 64), f32)], axis=1).astype(jnp.bfloat16)
    parts = jnp.concatenate(parts, axis=1)
    whole = [(parts[k : k + 3] + parts[k + 3 : k + 6]) + parts[k + 6 : k + 9] for k in (0, 9)]
    taps[...] = jnp.concatenate([arranged(*whole), jnp.zeros((5, 1408), f32)], axis=0)


def line_body(spots, b0, b1, b2, b3, up, down):
    for k, piece in enumerate((b0, b1, b2, b3)):
        where = pl.multiple_of(spots[20 + k], 64)
        up[pl.ds(where, 64), :] = piece[:, 0:1408]
        down[pl.ds(where, 64), :] = piece[:, 1408:2176]


def gelu(v):
    inner = v * (0.7978845608028654 + 0.035677408136300125 * (v * v))
    return 0.5 * v * (1.0 + jnp.tanh(inner))


GROUPS = ((0, 512), (512, 512), (1024, 384))


def own_body(spots, x_rows, w0, acc):
    x_some = x_rows[:, pl.ds(pl.multiple_of(spots[25], 256), 256)]
    for start, width in GROUPS:
        columns = slice(start, start + width)
        acc[:, columns] = jnp.dot(x_some, w0[:, columns], preferred_element_type=jnp.float32)


def more_body(spots, x_rows, before, w1, w2, acc, x_some, w_some):
    for k, piece in enumerate((w1, w2)):
        where = pl.multiple_of(spots[26 + k], 256)
        x_some[:, k * 256 : k * 256 + 256] = x_rows[:, pl.ds(where, 256)]
        w_some[k * 256 : k * 256 + 256, :] = piece[...]
    for start, width in GROUPS:
        columns = slice(start, start + width)
        acc[:, columns] = before[:, columns] + jnp.dot(
            x_some[...], w_some[:, columns], preferred_element_type=jnp.float32
        )


def down_body(spots, d0, d1, d2, d3, d4, gate, out):
    at = 0
    for piece in (d0, d1, d2, d3, d4):
        for row in range(0, piece.shape[0], 64):
            where = pl.multiple_of(spots[at], 64)
            out[pl.ds(where, 64), :] = piece[row : row + 64, :]
            at += 1


CHUNKS = (((0, 2, 0), (1, 3, 128)), ((4, 6, 256), (5, 7, 384)), ((8, 9, 512), (10, None, 640)))


def hidden_body(half, spots, x_rows, acc, w3, w4, taps, gate, hidden, w_some, full):
    w_some[0:128, :] = w3[...]
    w_some[128:256, :] = w4[...]
    r0 = half * 2 * BLOCK
    where = pl.multiple_of(spots[28], 256)
    x_some = x_rows[r0 : r0 + 2 * BLOCK, pl.ds(where, 256)]

    def conv(row, part):
        at = part * 2 * BLOCK + row + HALO * (row // 256) + HALO
        scale = taps[:, part * 128 : part * 128 + 128]
        made = full[at - 2 : at + 62, :] * scale[0:1]
        made = made + full[at - 1 : at + 63, :] * scale[1:2]
        return made + full[at : at + 64, :] * scale[2:3]

    for (start, width), chunks in zip(GROUPS, CHUNKS):
        columns = slice(start, start + width)
        whole = acc[r0 : r0 + 2 * BLOCK, columns] + jnp.dot(
            x_some, w_some[:, columns], preferred_element_type=jnp.float32
        )
        for k in range(width // 128):
            first = (start // 128 + k) * 2 * BLOCK
            full[first : first + 2 * BLOCK, :] = whole[:, k * 128 : k * 128 + 128]
        for value, gated, at in chunks:
            for row in range(0, 512, 64):
                made = conv(row, value)
                if gated is None:
                    made = gelu(pltpu.roll(made, 64, 1)) * made
                    lane = lax.broadcasted_iota(jnp.int32, made.shape, 1)
                    made = jnp.where(lane < 64, made, 0.0)
                else:
                    made = gelu(conv(row, gated)) * made
                hidden[row : row + 64, at : at + 128] = made.astype(jnp.bfloat16)


def product_body(spot, spots, hidden, d_all, gate, out):
    r0 = pl.multiple_of(spots[spot], 256)
    product = lax.dot_general(
        hidden[pl.ds(r0, 256), :], d_all[...], (((1,), (1,)), ((), ())), preferred_element_type=jnp.float32
    )
    out[...] = product.astype(out.dtype)


def shards(tokens, norm_in, value_weight, gate_weight, value_taps, gate_taps, down_weight, norm_out):
    f32 = jnp.float32
    (pack,) = call(
        pack_body,
        (
            jnp.concatenate(
                [a.astype(f32) for a in (value_weight, gate_weight, down_weight.T, value_taps, gate_taps)], axis=0
            ),
        ),
        [sds((PACK, 128))],
        [VM],
    )
    packs = [pack] + [moved(pack, same_parity(k)) for k in (4, 2, -2)]
    both, tap_rows = call(assemble_body, packs, [sds((64, 2176)), sds((8, 1408), f32)], [VM] * 4)
    up_line, down_line = call(
        placed(line_body), all_of_four(both, first_by), [sds((256, 1408)), sds((256, 768))], [VM] * 4
    )
    ups = ring_of_four(up_line, second_by)
    downs = ring_of_four(down_line, second_by)

    normed, last = call(
        placed(norm_body),
        (tokens, norm_in.reshape(1, -1)),
        [sds(tokens.shape), sds((HALO, 1024))],
        [VM] * 2,
    )
    halo = moved(last, next_device)
    (joined,) = call(placed(join_body), (normed, halo), [sds((BLOCK, 1024))], [VM] * 2)
    chip = moved(joined, to_helper)
    (stacked,) = call(stack_body, (joined, chip), [sds((2 * BLOCK, 1024))], [VM, VM])
    core = moved(stacked, other_core)
    (x_rows,) = call(placed(rows_body), (joined, chip, core), [sds((4 * BLOCK, 1024))], [VM] * 3)

    sums = [sds((4 * BLOCK, 1408), f32)]
    (acc_own,) = call(placed(own_body), (x_rows, ups[0]), sums, [VM] * 2, flops=2 * 1040 * 256 * 1408, nbytes=8 * MB)
    (acc,) = call(
        placed(more_body),
        (x_rows, acc_own, *ups[1:3]),
        sums,
        [VM] * 4,
        flops=2 * 1088 * 512 * 1408,
        nbytes=8 * MB,
        limit=16,
        scratch=(pltpu.VMEM((4 * BLOCK, 512), jnp.bfloat16), pltpu.VMEM((512, 1408), jnp.bfloat16)),
    )

    def hidden_of(half, gate):
        (out,) = call(
            placed(hidden_body, half),
            (x_rows, acc, ups[3], ups[4], tap_rows, gate),
            [sds((512, 768))],
            [VM] * 5 + [ANY],
            flops=2 * 544 * 256 * 1408 * 3,
            nbytes=4 * MB,
            limit=16,
            scratch=(pltpu.VMEM((256, 1408), jnp.bfloat16), pltpu.VMEM((11 * 2 * BLOCK, 128), f32)),
        )
        return out

    def product_of(spot, hidden, dtype, gate):
        (out,) = call(
            placed(product_body, spot),
            (hidden, d_all, gate),
            [sds((256, 1024), dtype)],
            [VM] * 2 + [ANY],
            flops=2 * 256 * 768 * 1024,
            nbytes=2 * MB,
        )
        return out

    hidden_far = hidden_of(0, acc)
    (d_all,) = call(
        placed(down_body),
        (*downs, hidden_far),
        [sds((1024, 768))],
        [VM] * 5 + [ANY],
    )
    first = product_of(30, hidden_far, jnp.bfloat16, d_all)
    got_far = moved(first, other_core)
    second = product_of(29, hidden_far, f32, first)
    sent = (second + got_far.astype(f32)).astype(jnp.bfloat16)
    back = moved(sent, from_helper)
    hidden_near = hidden_of(1, sent)
    third = product_of(30, hidden_near, jnp.bfloat16, sent)
    got_near = moved(third, other_core)
    fourth = product_of(29, hidden_near, f32, third)
    (out,) = call(final_body, (fourth, got_near, back, norm_out.reshape(1, -1)), [sds((256, 1024))], [VM] * 4)
    return out


def solution(mesh):
    split = Mesh(mesh.devices.reshape(NY, NX, NZ, NC), ALL)
    return jax.shard_map(
        shards,
        mesh=split,
        in_specs=(P(ALL, None), P(), P(FS, TP), P(FS, TP), P(None, TP), P(None, TP), P(TP, FS), P()),
        out_specs=P(ALL, None),
        check_vma=False,
    )
```

```python
import jax
import jax.numpy as jnp
from jax import lax
from jax.experimental import pallas as pl
from jax.experimental.pallas import tpu as pltpu
from jax.sharding import Mesh
from jax.sharding import PartitionSpec as P


FS = ("y", "x")
TP = ("z", "c")
ALL = ("y", "x", "z", "c")
NY, NX, NZ, NC = 4, 4, 8, 2
EPS = 1e-06
HALO = 16
BLOCK = 256 + HALO
MB = 1024 * 1024


def moved(array, target):
    pairs = []
    for y in range(NY):
        for x in range(NX):
            for z in range(NZ):
                for c in range(NC):
                    to = target(y, x, z, c)
                    if to is None:
                        continue
                    source = ((y * NX + x) * NZ + z) * NC + c
                    ty, tx, tz, tc = to
                    pairs.append((source, ((ty * NX + tx) * NZ + tz) * NC + tc))
    return lax.ppermute(array, ALL, pairs)


def same_parity(k):
    return lambda y, x, z, c: (y, x, (z + k) % NZ, c)


def first_by(k):
    return lambda y, x, z, c: (y, (x + k) % NX, z, c) if c == 0 else ((y + k) % NY, x, z, c)


def second_by(k):
    return lambda y, x, z, c: ((y + k) % NY, x, z, c) if c == 0 else (y, (x + k) % NX, z, c)


def other_core(y, x, z, c):
    return (y, x, z, 1 - c)


def to_helper(y, x, z, c):
    return (y, x, (z - 1 if c == 0 else z + 1) % NZ, c)


def from_helper(y, x, z, c):
    return (y, x, (z + 1 if c == 0 else z - 1) % NZ, c)


def next_device(y, x, z, c):
    at = ((y * NX + x) * NZ + z) * NC + c + 1
    if at >= NY * NX * NZ * NC:
        return None
    return (at // (NX * NZ * NC), at // (NZ * NC) % NX, at // NC % NZ, at % NC)


def all_of_four(block, by):
    return block, moved(block, by(1)), moved(block, by(-1)), moved(block, by(2))


VM = pl.BlockSpec(memory_space=pltpu.VMEM)
ANY = pl.BlockSpec(memory_space=pl.ANY)


def call(body, ins, outs, specs, *, flops=MB, nbytes=MB, scratch=(), limit=16, kept=VM):
    return pl.pallas_call(
        body,
        out_shape=outs,
        in_specs=specs,
        out_specs=[kept] * len(outs),
        scratch_shapes=list(scratch),
        compiler_params=pltpu.CompilerParams(vmem_limit_bytes=limit * MB),
        cost_estimate=pl.CostEstimate(flops=flops, bytes_accessed=nbytes, transcendentals=0),
    )(*ins)


def sds(shape, dtype=jnp.bfloat16):
    return jax.ShapeDtypeStruct(shape, dtype)


def here():
    y, x, c = lax.axis_index("y"), lax.axis_index("x"), lax.axis_index("c")
    mine, across = jnp.where(c == 0, x, y), jnp.where(c == 0, y, x)
    near = [(mine + k) & 3 for k in (0, 3, 1, 2)]
    far = [(across + k) & 3 for k in (0, 3, 1, 2)]
    place_near, place_far = jnp.where(c == 0, 64, 256), jnp.where(c == 0, 256, 64)
    blocks = [f * place_far + n * place_near for f in far for n in near]
    members = [2 + c, c, 3 - c, 1 - c]
    spots = blocks + [m * BLOCK for m in members] + [n * 64 for n in near] + [c]
    return spots + [f * 256 for f in far] + [c * 256, (1 - c) * 256]


def placed(body, *fixed):
    return lambda *refs: body(*fixed, here(), *refs)


def normed_rows(wide, scale):
    power = jnp.mean(wide * wide, axis=-1, keepdims=True)
    return wide * lax.rsqrt(power + EPS) * scale


def turned(wide):
    blocks = [wide[:, (y * NX + x) * 64 : (y * NX + x + 1) * 64] for x in range(NX) for y in range(NY)]
    return jnp.concatenate(blocks, axis=1)


def norm_body(spots, tokens, scale, out, last):
    rows = normed_rows(tokens[...].astype(jnp.float32), scale[...])
    last[...] = rows[256 - HALO :].astype(jnp.bfloat16)

    @pl.when(spots[24] == 0)
    def _():
        out[...] = rows.astype(jnp.bfloat16)

    @pl.when(spots[24] == 1)
    def _():
        out[...] = turned(rows).astype(jnp.bfloat16)


def join_body(spots, own, halo, out):
    out[HALO:BLOCK, :] = own[...]

    @pl.when(spots[24] == 0)
    def _():
        out[0:HALO, :] = halo[...]

    @pl.when(spots[24] == 1)
    def _():
        out[0:HALO, :] = turned(halo[...].astype(jnp.float32)).astype(jnp.bfloat16)


def stack_body(own, chip, out):
    out[0:BLOCK, :] = turned(own[...].astype(jnp.float32)).astype(jnp.bfloat16)
    out[BLOCK : 2 * BLOCK, :] = turned(chip[...].astype(jnp.float32)).astype(jnp.bfloat16)


def rows_body(spots, own, chip, core, out):
    for k, ref, row in ((0, own, 0), (1, chip, 0), (2, core, 0), (3, core, BLOCK)):
        where = pl.multiple_of(spots[16 + k], 16)
        out[pl.ds(where, BLOCK), :] = ref[row : row + BLOCK, :]


def final_body(own, near, far, scale, out, made, sems):
    copies = []
    for k in range(4):
        some = slice(64 * k, 64 * k + 64)
        total = own[some, :] + near[some, :].astype(jnp.float32) + far[some, :].astype(jnp.float32)
        made[some, :] = normed_rows(total, scale[...]).astype(jnp.bfloat16)
        copies.append(pltpu.make_async_copy(made.at[some, :], out.at[some, :], sems.at[k]))
        copies[-1].start()
    for copy in copies:
        copy.wait()


PACK = 304


def three_parts(values):
    high = values.astype(jnp.bfloat16).astype(jnp.float32)
    rest = values - high
    middle = rest.astype(jnp.bfloat16).astype(jnp.float32)
    return [high, middle, rest - middle]


def pack_body(joint, taps, out):
    f32, bf16 = jnp.float32, jnp.bfloat16
    rows = jnp.concatenate(three_parts(taps[0:3, :]) + three_parts(taps[3:6, :]), axis=0)
    out[0:192, :] = joint[:, 0:128]
    value, gate, down = (joint[k : k + 64, 128:176].astype(f32) for k in (0, 64, 128))
    out[192:256, :] = jnp.concatenate([value, gate, down[:, 0:32]], axis=1).astype(bf16)
    folded = [down[k : k + 16, 32:48] for k in (0, 16, 32, 48)]
    left = jnp.concatenate(folded + [rows[0:16, 128:176], jnp.zeros((16, 16), f32)], axis=1)
    out[256:272, :] = left.astype(bf16)
    ends = jnp.concatenate([rows[16:18, 128:176], jnp.zeros((2, 80), f32)], axis=1)
    gap = jnp.zeros((6, 128), f32)
    out[272:304, :] = jnp.concatenate([rows[:, 0:128], gap, ends, gap], axis=0).astype(bf16)


def arranged(v, g):
    return jnp.concatenate(
        [v[:, 0:256], g[:, 0:256], v[:, 256:512], g[:, 256:512], v[:, 512:640], g[:, 512:640], v[:, 640:704], g[:, 640:704]],
        axis=1,
    )


def assemble_body(p0, p1, p2, p3, both, taps):
    f32 = jnp.float32
    values, gates, downs, parts = [], [], [], []
    for p in (p0, p1, p2, p3):
        other = p[192:256, :].astype(f32)
        left = p[256:272, :].astype(f32)
        rows = p[272:304, :].astype(f32)
        folded = jnp.concatenate([left[:, k : k + 16] for k in (0, 16, 32, 48)], axis=0)
        values += [p[0:64, :].astype(f32), other[:, 0:48]]
        gates += [p[64:128, :].astype(f32), other[:, 48:96]]
        downs += [p[128:192, :].astype(f32), other[:, 96:128], folded]
        parts += [rows[0:18], jnp.concatenate([left[:, 64:112], rows[24:26, 0:48]], axis=0)]
    both[:, 0:1408] = arranged(jnp.concatenate(values, axis=1), jnp.concatenate(gates, axis=1)).astype(jnp.bfloat16)
    both[:, 1408:2176] = jnp.concatenate(downs + [jnp.zeros((64, 64), f32)], axis=1).astype(jnp.bfloat16)
    parts = jnp.concatenate(parts, axis=1)
    whole = [(parts[k : k + 3] + parts[k + 3 : k + 6]) + parts[k + 6 : k + 9] for k in (0, 9)]
    taps[...] = jnp.concatenate([arranged(*whole), jnp.zeros((5, 1408), f32)], axis=0)


def line_body(b1, b2, b3, up, down):
    for k, piece in enumerate((b1, b2, b3)):
        up[k * 64 : k * 64 + 64, :] = piece[:, 0:1408]
        down[k * 64 : k * 64 + 64, :] = piece[:, 1408:2176]


def gelu(v):
    inner = v * (0.7978845608028654 + 0.035677408136300125 * (v * v))
    return 0.5 * v * (1.0 + jnp.tanh(inner))


GROUPS = ((0, 512), (512, 512), (1024, 384))


def place_up(spots, target, first, pieces):
    at = 20
    for piece in pieces:
        for row in range(0, piece.shape[0], 64):
            where = pl.multiple_of(first + spots[at], 64)
            target[pl.ds(where, 64), :] = piece[row : row + 64, 0:1408]
            at += 1


def own_body(spots, x_rows, own, line, acc, w_some):
    x_some = x_rows[:, pl.ds(pl.multiple_of(spots[25], 256), 256)]
    place_up(spots, w_some, 0, (own, line))
    for start, width in GROUPS:
        columns = slice(start, start + width)
        acc[:, columns] = jnp.dot(x_some, w_some[:, columns], preferred_element_type=jnp.float32)


def more_body(spots, x_rows, before, own1, w1, own2, w2, acc, x_some, w_some):
    for k, pieces in enumerate(((own1, w1), (own2, w2))):
        where = pl.multiple_of(spots[26 + k], 256)
        x_some[:, k * 256 : k * 256 + 256] = x_rows[:, pl.ds(where, 256)]
        place_up(spots, w_some, k * 256, pieces)
    for start, width in GROUPS:
        columns = slice(start, start + width)
        acc[:, columns] = before[:, columns] + jnp.dot(
            x_some[...], w_some[:, columns], preferred_element_type=jnp.float32
        )


def down_body(spots, o0, d0, o1, d1, o2, d2, d3, d4, gate, out):
    at = 0
    for piece in (o0, d0, o1, d1, o2, d2, d3, d4):
        first = piece.shape[1] - 768
        for row in range(0, piece.shape[0], 64):
            where = pl.multiple_of(spots[at], 64)
            out[pl.ds(where, 64), :] = piece[row : row + 64, first : first + 768]
            at += 1


CHUNKS = (((0, 2, 0), (1, 3, 128)), ((4, 6, 256), (5, 7, 384)), ((8, 9, 512), (10, None, 640)))


def hidden_body(half, spots, x_rows, acc, w3, w4, taps, gate, hidden, w_some, full):
    place_up(spots, w_some, 0, (w3, w4))
    r0 = half * 2 * BLOCK
    where = pl.multiple_of(spots[28], 256)
    x_some = x_rows[r0 : r0 + 2 * BLOCK, pl.ds(where, 256)]

    def conv(row, part):
        at = part * 2 * BLOCK + row + HALO * (row // 256) + HALO
        scale = taps[:, part * 128 : part * 128 + 128]
        made = full[at - 2 : at + 62, :] * scale[0:1]
        made = made + full[at - 1 : at + 63, :] * scale[1:2]
        return made + full[at : at + 64, :] * scale[2:3]

    for (start, width), chunks in zip(GROUPS, CHUNKS):
        columns = slice(start, start + width)
        whole = acc[r0 : r0 + 2 * BLOCK, columns] + jnp.dot(
            x_some, w_some[:, columns], preferred_element_type=jnp.float32
        )
        for k in range(width // 128):
            first = (start // 128 + k) * 2 * BLOCK
            full[first : first + 2 * BLOCK, :] = whole[:, k * 128 : k * 128 + 128]
        for value, gated, at in chunks:
            for row in range(0, 512, 64):
                made = conv(row, value)
                if gated is None:
                    made = gelu(pltpu.roll(made, 64, 1)) * made
                    lane = lax.broadcasted_iota(jnp.int32, made.shape, 1)
                    made = jnp.where(lane < 64, made, 0.0)
                else:
                    made = gelu(conv(row, gated)) * made
                hidden[row : row + 64, at : at + 128] = made.astype(jnp.bfloat16)


def product_body(spot, spots, hidden, d_all, gate, out):
    r0 = pl.multiple_of(spots[spot], 256)
    product = lax.dot_general(
        hidden[pl.ds(r0, 256), :], d_all[...], (((1,), (1,)), ((), ())), preferred_element_type=jnp.float32
    )
    out[...] = product.astype(out.dtype)


def shards(tokens, norm_in, value_weight, gate_weight, value_taps, gate_taps, down_weight, norm_out):
    f32 = jnp.float32
    (pack,) = call(
        pack_body,
        (
            jnp.concatenate([value_weight, gate_weight, down_weight.T], axis=0),
            jnp.concatenate([value_taps, gate_taps], axis=0),
        ),
        [sds((PACK, 128))],
        [VM] * 2,
    )
    packs = [pack] + [moved(pack, same_parity(k)) for k in (4, 2, -2)]
    both, tap_rows = call(assemble_body, packs, [sds((64, 2176)), sds((8, 1408), f32)], [VM] * 4)
    near = all_of_four(both, first_by)
    own = (both, moved(both, second_by(1)), moved(both, second_by(-1)))
    lines = call(line_body, near[1:], [sds((192, 1408)), sds((192, 768))], [VM] * 3)

    def far_of(line, columns):
        before, after = moved(line, second_by(1)), moved(line, second_by(-1))
        top = moved(jnp.concatenate([own[1][:, columns], before[:64]], axis=0), second_by(1))
        bottom = moved(after[64:], second_by(-1))
        return line, before, after, top, bottom

    ups = far_of(lines[0], slice(0, 1408))
    downs = far_of(lines[1], slice(1408, 2176))

    normed, last = call(
        placed(norm_body),
        (tokens, norm_in.reshape(1, -1)),
        [sds(tokens.shape), sds((HALO, 1024))],
        [VM] * 2,
    )
    halo = moved(last, next_device)
    (joined,) = call(placed(join_body), (normed, halo), [sds((BLOCK, 1024))], [VM] * 2)
    chip = moved(joined, to_helper)
    (stacked,) = call(stack_body, (joined, chip), [sds((2 * BLOCK, 1024))], [VM, VM])
    core = moved(stacked, other_core)
    (x_rows,) = call(placed(rows_body), (joined, chip, core), [sds((4 * BLOCK, 1024))], [VM] * 3)

    sums = [sds((4 * BLOCK, 1408), f32)]
    (acc_own,) = call(
        placed(own_body),
        (x_rows, both, ups[0]),
        sums,
        [VM] * 3,
        flops=2 * 1088 * 256 * 1408,
        nbytes=8 * MB,
        scratch=(pltpu.VMEM((256, 1408), jnp.bfloat16),),
    )
    (acc,) = call(
        placed(more_body),
        (x_rows, acc_own, own[1], ups[1], own[2], ups[2]),
        sums,
        [VM] * 6,
        flops=2 * 1088 * 512 * 1408,
        nbytes=8 * MB,
        limit=16,
        scratch=(pltpu.VMEM((4 * BLOCK, 512), jnp.bfloat16), pltpu.VMEM((512, 1408), jnp.bfloat16)),
    )

    def hidden_of(half, gate):
        (out,) = call(
            placed(hidden_body, half),
            (x_rows, acc, ups[3], ups[4], tap_rows, gate),
            [sds((512, 768))],
            [VM] * 5 + [ANY],
            flops=2 * 544 * 256 * 1408 * 3,
            nbytes=4 * MB,
            limit=16,
            scratch=(pltpu.VMEM((256, 1408), jnp.bfloat16), pltpu.VMEM((11 * 2 * BLOCK, 128), f32)),
        )
        return out

    def product_of(spot, hidden, dtype, gate):
        (out,) = call(
            placed(product_body, spot),
            (hidden, d_all, gate),
            [sds((256, 1024), dtype)],
            [VM] * 2 + [ANY],
            flops=2 * 256 * 768 * 1024,
            nbytes=2 * MB,
        )
        return out

    hidden_far = hidden_of(0, acc)
    down_pieces = (both, downs[0], own[1], downs[1], own[2], downs[2], *downs[3:])
    (d_all,) = call(placed(down_body), (*down_pieces, hidden_far), [sds((1024, 768))], [VM] * 8 + [ANY])
    first = product_of(30, hidden_far, jnp.bfloat16, d_all)
    got_far = moved(first, other_core)
    second = product_of(29, hidden_far, f32, first)
    sent = (second + got_far.astype(f32)).astype(jnp.bfloat16)
    back = moved(sent, from_helper)
    hidden_near = hidden_of(1, sent)
    third = product_of(30, hidden_near, jnp.bfloat16, sent)
    got_near = moved(third, other_core)
    fourth = product_of(29, hidden_near, f32, third)
    (out,) = call(
        final_body,
        (fourth, got_near, back, norm_out.reshape(1, -1)),
        [sds((256, 1024))],
        [VM] * 4,
        scratch=(pltpu.VMEM((256, 1024), jnp.bfloat16), pltpu.SemaphoreType.DMA((4,))),
        kept=ANY,
    )
    return out


def solution(mesh):
    split = Mesh(mesh.devices.reshape(NY, NX, NZ, NC), ALL)
    return jax.shard_map(
        shards,
        mesh=split,
        in_specs=(P(ALL, None), P(), P(FS, TP), P(FS, TP), P(None, TP), P(None, TP), P(TP, FS), P()),
        out_specs=P(ALL, None),
        check_vma=False,
    )
```

```python
import jax
import jax.numpy as jnp
from jax import lax
from jax.experimental import pallas as pl
from jax.experimental.pallas import tpu as pltpu
from jax.sharding import Mesh
from jax.sharding import PartitionSpec as P


FS = ("y", "x")
TP = ("z", "c")
ALL = ("y", "x", "z", "c")
NY, NX, NZ, NC = 4, 4, 8, 2
EPS = 1e-06
HALO = 16
BLOCK = 256 + HALO
MB = 1024 * 1024


def moved(array, target):
    pairs = []
    for y in range(NY):
        for x in range(NX):
            for z in range(NZ):
                for c in range(NC):
                    to = target(y, x, z, c)
                    if to is None:
                        continue
                    source = ((y * NX + x) * NZ + z) * NC + c
                    ty, tx, tz, tc = to
                    pairs.append((source, ((ty * NX + tx) * NZ + tz) * NC + tc))
    return lax.ppermute(array, ALL, pairs)


def same_parity(k):
    return lambda y, x, z, c: (y, x, (z + k) % NZ, c)


def first_by(k):
    return lambda y, x, z, c: (y, (x + k) % NX, z, c) if c == 0 else ((y + k) % NY, x, z, c)


def second_by(k):
    return lambda y, x, z, c: ((y + k) % NY, x, z, c) if c == 0 else (y, (x + k) % NX, z, c)


def other_core(y, x, z, c):
    return (y, x, z, 1 - c)


def to_helper(y, x, z, c):
    return (y, x, (z - 1 if c == 0 else z + 1) % NZ, c)


def from_helper(y, x, z, c):
    return (y, x, (z + 1 if c == 0 else z - 1) % NZ, c)


def next_device(y, x, z, c):
    at = ((y * NX + x) * NZ + z) * NC + c + 1
    if at >= NY * NX * NZ * NC:
        return None
    return (at // (NX * NZ * NC), at // (NZ * NC) % NX, at // NC % NZ, at % NC)


def all_of_four(block, by):
    return block, moved(block, by(1)), moved(block, by(-1)), moved(block, by(2))


def ring_of_four(block, by):
    half = block.shape[0] // 2
    before = moved(block, by(1))
    after = moved(block, by(-1))
    top = moved(before[:half], by(1))
    bottom = moved(after[half:], by(-1))
    return block, before, after, top, bottom


VM = pl.BlockSpec(memory_space=pltpu.VMEM)
ANY = pl.BlockSpec(memory_space=pl.ANY)


def call(body, ins, outs, specs, *, flops=MB, nbytes=MB, scratch=(), limit=16, kept=VM):
    return pl.pallas_call(
        body,
        out_shape=outs,
        in_specs=specs,
        out_specs=[kept] * len(outs),
        scratch_shapes=list(scratch),
        compiler_params=pltpu.CompilerParams(vmem_limit_bytes=limit * MB),
        cost_estimate=pl.CostEstimate(flops=flops, bytes_accessed=nbytes, transcendentals=0),
    )(*ins)


def sds(shape, dtype=jnp.bfloat16):
    return jax.ShapeDtypeStruct(shape, dtype)


def here():
    y, x, c = lax.axis_index("y"), lax.axis_index("x"), lax.axis_index("c")
    mine, across = jnp.where(c == 0, x, y), jnp.where(c == 0, y, x)
    near = [(mine + k) & 3 for k in (0, 3, 1, 2)]
    far = [(across + k) & 3 for k in (0, 3, 1, 2)]
    place_near, place_far = jnp.where(c == 0, 64, 256), jnp.where(c == 0, 256, 64)
    blocks = [f * place_far + n * place_near for f in far for n in range(4)]
    members = [2 + c, c, 3 - c, 1 - c]
    spots = blocks + [m * BLOCK for m in members] + [n * 64 for n in near] + [c]
    return spots + [f * 256 for f in far] + [c * 256, (1 - c) * 256]


def placed(body, *fixed):
    return lambda *refs: body(*fixed, here(), *refs)


def normed_rows(wide, scale):
    power = jnp.mean(wide * wide, axis=-1, keepdims=True)
    return wide * lax.rsqrt(power + EPS) * scale


def turned(wide):
    blocks = [wide[:, (y * NX + x) * 64 : (y * NX + x + 1) * 64] for x in range(NX) for y in range(NY)]
    return jnp.concatenate(blocks, axis=1)


def norm_body(spots, tokens, scale, out, last):
    rows = normed_rows(tokens[...].astype(jnp.float32), scale[...])
    last[...] = rows[256 - HALO :].astype(jnp.bfloat16)

    @pl.when(spots[24] == 0)
    def _():
        out[...] = rows.astype(jnp.bfloat16)

    @pl.when(spots[24] == 1)
    def _():
        out[...] = turned(rows).astype(jnp.bfloat16)


def join_body(spots, own, halo, out):
    out[HALO:BLOCK, :] = own[...]

    @pl.when(spots[24] == 0)
    def _():
        out[0:HALO, :] = halo[...]

    @pl.when(spots[24] == 1)
    def _():
        out[0:HALO, :] = turned(halo[...].astype(jnp.float32)).astype(jnp.bfloat16)


def stack_body(own, chip, out):
    out[0:BLOCK, :] = turned(own[...].astype(jnp.float32)).astype(jnp.bfloat16)
    out[BLOCK : 2 * BLOCK, :] = turned(chip[...].astype(jnp.float32)).astype(jnp.bfloat16)


def rows_body(spots, own, chip, core, out):
    for k, ref, row in ((0, own, 0), (1, chip, 0), (2, core, 0), (3, core, BLOCK)):
        where = pl.multiple_of(spots[16 + k], 16)
        out[pl.ds(where, BLOCK), :] = ref[row : row + BLOCK, :]


def final_body(own, near, far, scale, out, made, sems):
    copies = []
    for k in range(4):
        some = slice(64 * k, 64 * k + 64)
        total = own[some, :] + near[some, :].astype(jnp.float32) + far[some, :].astype(jnp.float32)
        made[some, :] = normed_rows(total, scale[...]).astype(jnp.bfloat16)
        copies.append(pltpu.make_async_copy(made.at[some, :], out.at[some, :], sems.at[k]))
        copies[-1].start()
    for copy in copies:
        copy.wait()


PACK = 304


def three_parts(values):
    high = values.astype(jnp.bfloat16).astype(jnp.float32)
    rest = values - high
    middle = rest.astype(jnp.bfloat16).astype(jnp.float32)
    return [high, middle, rest - middle]


def pack_body(joint, taps, out):
    f32, bf16 = jnp.float32, jnp.bfloat16
    rows = jnp.concatenate(three_parts(taps[0:3, :]) + three_parts(taps[3:6, :]), axis=0)
    out[0:192, :] = joint[:, 0:128]
    value, gate, down = (joint[k : k + 64, 128:176].astype(f32) for k in (0, 64, 128))
    out[192:256, :] = jnp.concatenate([value, gate, down[:, 0:32]], axis=1).astype(bf16)
    folded = [down[k : k + 16, 32:48] for k in (0, 16, 32, 48)]
    left = jnp.concatenate(folded + [rows[0:16, 128:176], jnp.zeros((16, 16), f32)], axis=1)
    out[256:272, :] = left.astype(bf16)
    ends = jnp.concatenate([rows[16:18, 128:176], jnp.zeros((2, 80), f32)], axis=1)
    gap = jnp.zeros((6, 128), f32)
    out[272:304, :] = jnp.concatenate([rows[:, 0:128], gap, ends, gap], axis=0).astype(bf16)


def arranged(v, g):
    return jnp.concatenate(
        [v[:, 0:256], g[:, 0:256], v[:, 256:512], g[:, 256:512], v[:, 512:640], g[:, 512:640], v[:, 640:704], g[:, 640:704]],
        axis=1,
    )


def assemble_body(p0, p1, p2, p3, both, taps):
    f32 = jnp.float32
    values, gates, downs, parts = [], [], [], []
    for p in (p0, p1, p2, p3):
        other = p[192:256, :].astype(f32)
        left = p[256:272, :].astype(f32)
        rows = p[272:304, :].astype(f32)
        folded = jnp.concatenate([left[:, k : k + 16] for k in (0, 16, 32, 48)], axis=0)
        values += [p[0:64, :].astype(f32), other[:, 0:48]]
        gates += [p[64:128, :].astype(f32), other[:, 48:96]]
        downs += [p[128:192, :].astype(f32), other[:, 96:128], folded]
        parts += [rows[0:18], jnp.concatenate([left[:, 64:112], rows[24:26, 0:48]], axis=0)]
    both[:, 0:1408] = arranged(jnp.concatenate(values, axis=1), jnp.concatenate(gates, axis=1)).astype(jnp.bfloat16)
    both[:, 1408:2176] = jnp.concatenate(downs + [jnp.zeros((64, 64), f32)], axis=1).astype(jnp.bfloat16)
    parts = jnp.concatenate(parts, axis=1)
    whole = [(parts[k : k + 3] + parts[k + 3 : k + 6]) + parts[k + 6 : k + 9] for k in (0, 9)]
    taps[...] = jnp.concatenate([arranged(*whole), jnp.zeros((5, 1408), f32)], axis=0)


def line_body(spots, b0, b1, b2, b3, up, down):
    for k, piece in enumerate((b0, b1, b2, b3)):
        where = pl.multiple_of(spots[20 + k], 64)
        up[pl.ds(where, 64), :] = piece[:, 0:1408]
        down[pl.ds(where, 64), :] = piece[:, 1408:2176]


def gelu(v):
    inner = v * (0.7978845608028654 + 0.035677408136300125 * (v * v))
    return 0.5 * v * (1.0 + jnp.tanh(inner))


GROUPS = ((0, 512), (512, 512), (1024, 384))


def own_body(spots, x_rows, w0, acc):
    x_some = x_rows[:, pl.ds(pl.multiple_of(spots[25], 256), 256)]
    for start, width in GROUPS:
        columns = slice(start, start + width)
        acc[:, columns] = jnp.dot(x_some, w0[:, columns], preferred_element_type=jnp.float32)


def more_body(spots, x_rows, before, w1, w2, acc, x_some, w_some):
    for k, piece in enumerate((w1, w2)):
        where = pl.multiple_of(spots[26 + k], 256)
        x_some[:, k * 256 : k * 256 + 256] = x_rows[:, pl.ds(where, 256)]
        w_some[k * 256 : k * 256 + 256, :] = piece[...]
    for start, width in GROUPS:
        columns = slice(start, start + width)
        acc[:, columns] = before[:, columns] + jnp.dot(
            x_some[...], w_some[:, columns], preferred_element_type=jnp.float32
        )


def down_body(spots, d0, d1, d2, d3, d4, gate, out):
    at = 0
    for piece in (d0, d1, d2, d3, d4):
        for row in range(0, piece.shape[0], 64):
            where = pl.multiple_of(spots[at], 64)
            out[pl.ds(where, 64), :] = piece[row : row + 64, :]
            at += 1


CHUNKS = (((0, 2, 0), (1, 3, 128)), ((4, 6, 256), (5, 7, 384)), ((8, 9, 512), (10, None, 640)))


def hidden_body(half, spots, x_rows, acc, w3, w4, taps, gate, hidden, w_some, full):
    w_some[0:128, :] = w3[...]
    w_some[128:256, :] = w4[...]
    r0 = half * 2 * BLOCK
    where = pl.multiple_of(spots[28], 256)
    x_some = x_rows[r0 : r0 + 2 * BLOCK, pl.ds(where, 256)]

    def conv(row, part):
        at = part * 2 * BLOCK + row + HALO * (row // 256) + HALO
        scale = taps[:, part * 128 : part * 128 + 128]
        made = full[at - 2 : at + 62, :] * scale[0:1]
        made = made + full[at - 1 : at + 63, :] * scale[1:2]
        return made + full[at : at + 64, :] * scale[2:3]

    for (start, width), chunks in zip(GROUPS, CHUNKS):
        columns = slice(start, start + width)
        whole = acc[r0 : r0 + 2 * BLOCK, columns] + jnp.dot(
            x_some, w_some[:, columns], preferred_element_type=jnp.float32
        )
        for k in range(width // 128):
            first = (start // 128 + k) * 2 * BLOCK
            full[first : first + 2 * BLOCK, :] = whole[:, k * 128 : k * 128 + 128]
        for value, gated, at in chunks:
            for row in range(0, 512, 64):
                made = conv(row, value)
                if gated is None:
                    made = gelu(pltpu.roll(made, 64, 1)) * made
                    lane = lax.broadcasted_iota(jnp.int32, made.shape, 1)
                    made = jnp.where(lane < 64, made, 0.0)
                else:
                    made = gelu(conv(row, gated)) * made
                hidden[row : row + 64, at : at + 128] = made.astype(jnp.bfloat16)


def product_body(spot, spots, hidden, d_all, gate, out):
    r0 = pl.multiple_of(spots[spot], 256)
    product = lax.dot_general(
        hidden[pl.ds(r0, 256), :], d_all[...], (((1,), (1,)), ((), ())), preferred_element_type=jnp.float32
    )
    out[...] = product.astype(out.dtype)


def shards(tokens, norm_in, value_weight, gate_weight, value_taps, gate_taps, down_weight, norm_out):
    f32 = jnp.float32
    (pack,) = call(
        pack_body,
        (
            jnp.concatenate([value_weight, gate_weight, down_weight.T], axis=0),
            jnp.concatenate([value_taps, gate_taps], axis=0),
        ),
        [sds((PACK, 128))],
        [VM] * 2,
    )
    packs = [pack] + [moved(pack, same_parity(k)) for k in (4, -2, 2)]
    both, tap_rows = call(assemble_body, packs, [sds((64, 2176)), sds((8, 1408), f32)], [VM] * 4)
    up_line, down_line = call(
        placed(line_body), all_of_four(both, first_by), [sds((256, 1408)), sds((256, 768))], [VM] * 4
    )
    ups = ring_of_four(up_line, second_by)
    downs = ring_of_four(down_line, second_by)

    normed, last = call(
        placed(norm_body),
        (tokens, norm_in.reshape(1, -1)),
        [sds(tokens.shape), sds((HALO, 1024))],
        [VM] * 2,
    )
    halo = moved(last, next_device)
    (joined,) = call(placed(join_body), (normed, halo), [sds((BLOCK, 1024))], [VM] * 2)
    chip = moved(joined, to_helper)
    (stacked,) = call(stack_body, (joined, chip), [sds((2 * BLOCK, 1024))], [VM, VM])
    core = moved(stacked, other_core)
    (x_rows,) = call(placed(rows_body), (joined, chip, core), [sds((4 * BLOCK, 1024))], [VM] * 3)

    sums = [sds((4 * BLOCK, 1408), f32)]
    (acc_own,) = call(placed(own_body), (x_rows, ups[0]), sums, [VM] * 2, flops=2 * 1040 * 256 * 1408, nbytes=8 * MB)
    (acc,) = call(
        placed(more_body),
        (x_rows, acc_own, *ups[1:3]),
        sums,
        [VM] * 4,
        flops=2 * 1088 * 512 * 1408,
        nbytes=8 * MB,
        limit=16,
        scratch=(pltpu.VMEM((4 * BLOCK, 512), jnp.bfloat16), pltpu.VMEM((512, 1408), jnp.bfloat16)),
    )

    def hidden_of(half, gate):
        (out,) = call(
            placed(hidden_body, half),
            (x_rows, acc, ups[3], ups[4], tap_rows, gate),
            [sds((512, 768))],
            [VM] * 5 + [ANY],
            flops=2 * 544 * 256 * 1408 * 3,
            nbytes=4 * MB,
            limit=16,
            scratch=(pltpu.VMEM((256, 1408), jnp.bfloat16), pltpu.VMEM((11 * 2 * BLOCK, 128), f32)),
        )
        return out

    def product_of(spot, hidden, dtype, gate):
        (out,) = call(
            placed(product_body, spot),
            (hidden, d_all, gate),
            [sds((256, 1024), dtype)],
            [VM] * 2 + [ANY],
            flops=2 * 256 * 768 * 1024,
            nbytes=2 * MB,
        )
        return out

    hidden_far = hidden_of(0, acc)
    (d_all,) = call(
        placed(down_body),
        (*downs, hidden_far),
        [sds((1024, 768))],
        [VM] * 5 + [ANY],
    )
    first = product_of(30, hidden_far, jnp.bfloat16, d_all)
    got_far = moved(first, other_core)
    second = product_of(29, hidden_far, f32, first)
    sent = (second + got_far.astype(f32)).astype(jnp.bfloat16)
    back = moved(sent, from_helper)
    hidden_near = hidden_of(1, sent)
    third = product_of(30, hidden_near, jnp.bfloat16, sent)
    got_near = moved(third, other_core)
    fourth = product_of(29, hidden_near, f32, third)
    (out,) = call(
        final_body,
        (fourth, got_near, back, norm_out.reshape(1, -1)),
        [sds((256, 1024))],
        [VM] * 4,
        scratch=(pltpu.VMEM((256, 1024), jnp.bfloat16), pltpu.SemaphoreType.DMA((4,))),
        kept=ANY,
    )
    return out


def solution(mesh):
    split = Mesh(mesh.devices.reshape(NY, NX, NZ, NC), ALL)
    return jax.shard_map(
        shards,
        mesh=split,
        in_specs=(P(ALL, None), P(), P(FS, TP), P(FS, TP), P(None, TP), P(None, TP), P(TP, FS), P()),
        out_specs=P(ALL, None),
        check_vma=False,
    )
```

```python
import jax
import jax.numpy as jnp
from jax import lax
from jax.experimental import pallas as pl
from jax.experimental.pallas import tpu as pltpu
from jax.sharding import Mesh
from jax.sharding import PartitionSpec as P


FS = ("y", "x")
TP = ("z", "c")
ALL = ("y", "x", "z", "c")
NY, NX, NZ, NC = 4, 4, 8, 2
EPS = 1e-06
HALO = 16
BLOCK = 256 + HALO
MB = 1024 * 1024


def moved(array, target):
    pairs = []
    for y in range(NY):
        for x in range(NX):
            for z in range(NZ):
                for c in range(NC):
                    to = target(y, x, z, c)
                    if to is None:
                        continue
                    source = ((y * NX + x) * NZ + z) * NC + c
                    ty, tx, tz, tc = to
                    pairs.append((source, ((ty * NX + tx) * NZ + tz) * NC + tc))
    return lax.ppermute(array, ALL, pairs)


def same_parity(k):
    return lambda y, x, z, c: (y, x, (z + k) % NZ, c)


def first_by(k):
    return lambda y, x, z, c: (y, (x + k) % NX, z, c) if c == 0 else ((y + k) % NY, x, z, c)


def second_by(k):
    return lambda y, x, z, c: ((y + k) % NY, x, z, c) if c == 0 else (y, (x + k) % NX, z, c)


def other_core(y, x, z, c):
    return (y, x, z, 1 - c)


def to_helper(y, x, z, c):
    return (y, x, (z - 1 if c == 0 else z + 1) % NZ, c)


def from_helper(y, x, z, c):
    return (y, x, (z + 1 if c == 0 else z - 1) % NZ, c)


def next_device(y, x, z, c):
    at = ((y * NX + x) * NZ + z) * NC + c + 1
    if at >= NY * NX * NZ * NC:
        return None
    return (at // (NX * NZ * NC), at // (NZ * NC) % NX, at // NC % NZ, at % NC)


def all_of_four(block, by):
    return block, moved(block, by(1)), moved(block, by(-1)), moved(block, by(2))


def ring_of_four(block, by):
    half = block.shape[0] // 2
    before = moved(block, by(1))
    after = moved(block, by(-1))
    top = moved(before[:half], by(1))
    bottom = moved(after[half:], by(-1))
    return block, before, after, top, bottom


VM = pl.BlockSpec(memory_space=pltpu.VMEM)
ANY = pl.BlockSpec(memory_space=pl.ANY)


def call(body, ins, outs, specs, *, flops=MB, nbytes=MB, scratch=(), limit=16, kept=VM):
    return pl.pallas_call(
        body,
        out_shape=outs,
        in_specs=specs,
        out_specs=[kept] * len(outs),
        scratch_shapes=list(scratch),
        compiler_params=pltpu.CompilerParams(vmem_limit_bytes=limit * MB),
        cost_estimate=pl.CostEstimate(flops=flops, bytes_accessed=nbytes, transcendentals=0),
    )(*ins)


def sds(shape, dtype=jnp.bfloat16):
    return jax.ShapeDtypeStruct(shape, dtype)


def here():
    y, x, c = lax.axis_index("y"), lax.axis_index("x"), lax.axis_index("c")
    mine, across = jnp.where(c == 0, x, y), jnp.where(c == 0, y, x)
    near = [(mine + k) & 3 for k in (0, 3, 1, 2)]
    far = [(across + k) & 3 for k in (0, 3, 1, 2)]
    place_near, place_far = jnp.where(c == 0, 64, 256), jnp.where(c == 0, 256, 64)
    blocks = [f * place_far + n * place_near for f in far for n in range(4)]
    members = [2 + c, c, 3 - c, 1 - c]
    spots = blocks + [m * BLOCK for m in members] + [n * 64 for n in near] + [c]
    return spots + [f * 256 for f in far] + [c * 256, (1 - c) * 256]


def placed(body, *fixed):
    return lambda *refs: body(*fixed, here(), *refs)


def normed_rows(wide, scale):
    power = jnp.mean(wide * wide, axis=-1, keepdims=True)
    return wide * lax.rsqrt(power + EPS) * scale


def turned(wide):
    blocks = [wide[:, (y * NX + x) * 64 : (y * NX + x + 1) * 64] for x in range(NX) for y in range(NY)]
    return jnp.concatenate(blocks, axis=1)


def norm_body(spots, tokens, scale, out, last):
    rows = normed_rows(tokens[...].astype(jnp.float32), scale[...])
    last[...] = rows[256 - HALO :].astype(jnp.bfloat16)

    @pl.when(spots[24] == 0)
    def _():
        out[...] = rows.astype(jnp.bfloat16)

    @pl.when(spots[24] == 1)
    def _():
        out[...] = turned(rows).astype(jnp.bfloat16)


def join_body(spots, own, halo, out):
    out[HALO:BLOCK, :] = own[...]

    @pl.when(spots[24] == 0)
    def _():
        out[0:HALO, :] = halo[...]

    @pl.when(spots[24] == 1)
    def _():
        out[0:HALO, :] = turned(halo[...].astype(jnp.float32)).astype(jnp.bfloat16)


def stack_body(own, chip, out):
    out[0:BLOCK, :] = turned(own[...].astype(jnp.float32)).astype(jnp.bfloat16)
    out[BLOCK : 2 * BLOCK, :] = turned(chip[...].astype(jnp.float32)).astype(jnp.bfloat16)


def rows_body(spots, own, chip, core, out):
    for k, ref, row in ((0, own, 0), (1, chip, 0), (2, core, 0), (3, core, BLOCK)):
        where = pl.multiple_of(spots[16 + k], 16)
        out[pl.ds(where, BLOCK), :] = ref[row : row + BLOCK, :]


def final_body(own, near, far, scale, out, made, sems):
    copies = []
    for k in range(4):
        some = slice(64 * k, 64 * k + 64)
        total = own[some, :] + near[some, :].astype(jnp.float32) + far[some, :].astype(jnp.float32)
        made[some, :] = normed_rows(total, scale[...]).astype(jnp.bfloat16)
        copies.append(pltpu.make_async_copy(made.at[some, :], out.at[some, :], sems.at[k]))
        copies[-1].start()
    for copy in copies:
        copy.wait()


PACK = 304


def three_parts(values):
    high = values.astype(jnp.bfloat16).astype(jnp.float32)
    rest = values - high
    middle = rest.astype(jnp.bfloat16).astype(jnp.float32)
    return [high, middle, rest - middle]


def pack_body(joint, taps, out):
    f32, bf16 = jnp.float32, jnp.bfloat16
    rows = jnp.concatenate(three_parts(taps[0:3, :]) + three_parts(taps[3:6, :]), axis=0)
    out[0:192, :] = joint[:, 0:128]
    value, gate, down = (joint[k : k + 64, 128:176].astype(f32) for k in (0, 64, 128))
    out[192:256, :] = jnp.concatenate([value, gate, down[:, 0:32]], axis=1).astype(bf16)
    folded = [down[k : k + 16, 32:48] for k in (0, 16, 32, 48)]
    left = jnp.concatenate(folded + [rows[0:16, 128:176], jnp.zeros((16, 16), f32)], axis=1)
    out[256:272, :] = left.astype(bf16)
    ends = jnp.concatenate([rows[16:18, 128:176], jnp.zeros((2, 80), f32)], axis=1)
    gap = jnp.zeros((6, 128), f32)
    out[272:304, :] = jnp.concatenate([rows[:, 0:128], gap, ends, gap], axis=0).astype(bf16)


def arranged(v, g):
    return jnp.concatenate(
        [v[:, 0:256], g[:, 0:256], v[:, 256:512], g[:, 256:512], v[:, 512:640], g[:, 512:640], v[:, 640:704], g[:, 640:704]],
        axis=1,
    )


def assemble_body(p0, p1, p2, p3, both, taps):
    f32 = jnp.float32
    values, gates, downs, parts = [], [], [], []
    for p in (p0, p1, p2, p3):
        other = p[192:256, :].astype(f32)
        left = p[256:272, :].astype(f32)
        rows = p[272:304, :].astype(f32)
        folded = jnp.concatenate([left[:, k : k + 16] for k in (0, 16, 32, 48)], axis=0)
        values += [p[0:64, :].astype(f32), other[:, 0:48]]
        gates += [p[64:128, :].astype(f32), other[:, 48:96]]
        downs += [p[128:192, :].astype(f32), other[:, 96:128], folded]
        parts += [rows[0:18], jnp.concatenate([left[:, 64:112], rows[24:26, 0:48]], axis=0)]
    both[0:64, :] = arranged(jnp.concatenate(values, axis=1), jnp.concatenate(gates, axis=1)).astype(jnp.bfloat16)
    down = jnp.concatenate(downs, axis=1)
    both[64:96, :] = jnp.concatenate([down[0:32], down[32:64]], axis=1).astype(jnp.bfloat16)
    parts = jnp.concatenate(parts, axis=1)
    whole = [(parts[k : k + 3] + parts[k + 3 : k + 6]) + parts[k + 6 : k + 9] for k in (0, 9)]
    taps[...] = jnp.concatenate([arranged(*whole), jnp.zeros((5, 1408), f32)], axis=0)


def line_body(spots, b0, b1, b2, b3, up, down):
    for k, piece in enumerate((b0, b1, b2, b3)):
        where = spots[20 + k]
        up[pl.ds(pl.multiple_of(where, 64), 64), :] = piece[0:64, :]
        down[pl.ds(pl.multiple_of(where >> 1, 32), 32), :] = piece[64:96, :]


def gelu(v):
    inner = v * (0.7978845608028654 + 0.035677408136300125 * (v * v))
    return 0.5 * v * (1.0 + jnp.tanh(inner))


GROUPS = ((0, 512), (512, 512), (1024, 384))


def own_body(spots, x_rows, w0, acc):
    x_some = x_rows[:, pl.ds(pl.multiple_of(spots[25], 256), 256)]
    for start, width in GROUPS:
        columns = slice(start, start + width)
        acc[:, columns] = jnp.dot(x_some, w0[:, columns], preferred_element_type=jnp.float32)


def more_body(spots, x_rows, before, w1, w2, acc, x_some, w_some):
    for k, piece in enumerate((w1, w2)):
        where = pl.multiple_of(spots[26 + k], 256)
        x_some[:, k * 256 : k * 256 + 256] = x_rows[:, pl.ds(where, 256)]
        w_some[k * 256 : k * 256 + 256, :] = piece[...]
    for start, width in GROUPS:
        columns = slice(start, start + width)
        acc[:, columns] = before[:, columns] + jnp.dot(
            x_some[...], w_some[:, columns], preferred_element_type=jnp.float32
        )


def unfold(spots, at, pieces, out):
    for piece in pieces:
        for row in range(0, piece.shape[0], 32):
            where = pl.multiple_of(spots[at], 64)
            rows = piece[row : row + 32, :].astype(jnp.float32)
            gap = jnp.zeros((32, 64), jnp.float32)
            out[pl.ds(where, 32), :] = jnp.concatenate([rows[:, 0:704], gap], axis=1).astype(jnp.bfloat16)
            out[pl.ds(where + 32, 32), :] = jnp.concatenate([rows[:, 704:1408], gap], axis=1).astype(jnp.bfloat16)
            at += 1


def down_body(spots, d0, d1, d2, gate, out):
    unfold(spots, 0, (d0, d1, d2), out)


def rest_body(spots, early, d3, d4, gate, out):
    out[...] = early[...]
    unfold(spots, 12, (d3, d4), out)


CHUNKS = (((0, 2, 0), (1, 3, 128)), ((4, 6, 256), (5, 7, 384)), ((8, 9, 512), (10, None, 640)))


def hidden_body(half, spots, x_rows, acc, w3, w4, taps, gate, hidden, w_some, full):
    w_some[0:128, :] = w3[...]
    w_some[128:256, :] = w4[...]
    r0 = half * 2 * BLOCK
    where = pl.multiple_of(spots[28], 256)
    x_some = x_rows[r0 : r0 + 2 * BLOCK, pl.ds(where, 256)]

    def conv(row, part):
        at = part * 2 * BLOCK + row + HALO * (row // 256) + HALO
        scale = taps[:, part * 128 : part * 128 + 128]
        made = full[at - 2 : at + 62, :] * scale[0:1]
        made = made + full[at - 1 : at + 63, :] * scale[1:2]
        return made + full[at : at + 64, :] * scale[2:3]

    for (start, width), chunks in zip(GROUPS, CHUNKS):
        columns = slice(start, start + width)
        whole = acc[r0 : r0 + 2 * BLOCK, columns] + jnp.dot(
            x_some, w_some[:, columns], preferred_element_type=jnp.float32
        )
        for k in range(width // 128):
            first = (start // 128 + k) * 2 * BLOCK
            full[first : first + 2 * BLOCK, :] = whole[:, k * 128 : k * 128 + 128]
        for value, gated, at in chunks:
            for row in range(0, 512, 64):
                made = conv(row, value)
                if gated is None:
                    made = gelu(pltpu.roll(made, 64, 1)) * made
                    lane = lax.broadcasted_iota(jnp.int32, made.shape, 1)
                    made = jnp.where(lane < 64, made, 0.0)
                else:
                    made = gelu(conv(row, gated)) * made
                hidden[row : row + 64, at : at + 128] = made.astype(jnp.bfloat16)


def product_body(spot, spots, hidden, d_all, gate, out):
    r0 = pl.multiple_of(spots[spot], 256)
    product = lax.dot_general(
        hidden[pl.ds(r0, 256), :], d_all[...], (((1,), (1,)), ((), ())), preferred_element_type=jnp.float32
    )
    out[...] = product.astype(out.dtype)


def shards(tokens, norm_in, value_weight, gate_weight, value_taps, gate_taps, down_weight, norm_out):
    f32 = jnp.float32
    (pack,) = call(
        pack_body,
        (
            jnp.concatenate([value_weight, gate_weight, down_weight.T], axis=0),
            jnp.concatenate([value_taps, gate_taps], axis=0),
        ),
        [sds((PACK, 128))],
        [VM] * 2,
    )
    packs = [pack] + [moved(pack, same_parity(k)) for k in (4, -2, 2)]
    both, tap_rows = call(assemble_body, packs, [sds((96, 1408)), sds((8, 1408), f32)], [VM] * 4)
    up_line, down_line = call(
        placed(line_body), all_of_four(both, first_by), [sds((256, 1408)), sds((128, 1408))], [VM] * 4
    )
    ups = ring_of_four(up_line, second_by)
    downs = ring_of_four(down_line, second_by)

    normed, last = call(
        placed(norm_body),
        (tokens, norm_in.reshape(1, -1)),
        [sds(tokens.shape), sds((HALO, 1024))],
        [VM] * 2,
    )
    halo = moved(last, next_device)
    (joined,) = call(placed(join_body), (normed, halo), [sds((BLOCK, 1024))], [VM] * 2)
    chip = moved(joined, to_helper)
    (stacked,) = call(stack_body, (joined, chip), [sds((2 * BLOCK, 1024))], [VM, VM])
    core = moved(stacked, other_core)
    (x_rows,) = call(placed(rows_body), (joined, chip, core), [sds((4 * BLOCK, 1024))], [VM] * 3)

    sums = [sds((4 * BLOCK, 1408), f32)]
    (acc_own,) = call(placed(own_body), (x_rows, ups[0]), sums, [VM] * 2, flops=2 * 1040 * 256 * 1408, nbytes=8 * MB)
    (acc,) = call(
        placed(more_body),
        (x_rows, acc_own, *ups[1:3]),
        sums,
        [VM] * 4,
        flops=2 * 1088 * 512 * 1408,
        nbytes=8 * MB,
        limit=16,
        scratch=(pltpu.VMEM((4 * BLOCK, 512), jnp.bfloat16), pltpu.VMEM((512, 1408), jnp.bfloat16)),
    )

    def hidden_of(half, gate):
        (out,) = call(
            placed(hidden_body, half),
            (x_rows, acc, ups[3], ups[4], tap_rows, gate),
            [sds((512, 768))],
            [VM] * 5 + [ANY],
            flops=2 * 544 * 256 * 1408 * 3,
            nbytes=4 * MB,
            limit=16,
            scratch=(pltpu.VMEM((256, 1408), jnp.bfloat16), pltpu.VMEM((11 * 2 * BLOCK, 128), f32)),
        )
        return out

    def product_of(spot, hidden, dtype, gate):
        (out,) = call(
            placed(product_body, spot),
            (hidden, d_all, gate),
            [sds((256, 1024), dtype)],
            [VM] * 2 + [ANY],
            flops=2 * 256 * 768 * 1024,
            nbytes=2 * MB,
        )
        return out

    d_rows = sds((1024, 768))
    (d_early,) = call(placed(down_body), (*downs[:3], acc), [d_rows], [VM] * 3 + [ANY])
    hidden_far = hidden_of(0, d_early)
    (d_all,) = call(placed(rest_body), (d_early, *downs[3:], hidden_far), [d_rows], [VM] * 3 + [ANY])
    first = product_of(30, hidden_far, jnp.bfloat16, d_all)
    got_far = moved(first, other_core)
    second = product_of(29, hidden_far, f32, first)
    sent = (second + got_far.astype(f32)).astype(jnp.bfloat16)
    back = moved(sent, from_helper)
    hidden_near = hidden_of(1, sent)
    third = product_of(30, hidden_near, jnp.bfloat16, sent)
    got_near = moved(third, other_core)
    fourth = product_of(29, hidden_near, f32, third)
    (out,) = call(
        final_body,
        (fourth, got_near, back, norm_out.reshape(1, -1)),
        [sds((256, 1024))],
        [VM] * 4,
        scratch=(pltpu.VMEM((256, 1024), jnp.bfloat16), pltpu.SemaphoreType.DMA((4,))),
        kept=ANY,
    )
    return out


def solution(mesh):
    split = Mesh(mesh.devices.reshape(NY, NX, NZ, NC), ALL)
    return jax.shard_map(
        shards,
        mesh=split,
        in_specs=(P(ALL, None), P(), P(FS, TP), P(FS, TP), P(None, TP), P(None, TP), P(TP, FS), P()),
        out_specs=P(ALL, None),
        check_vma=False,
    )
```

```python
import jax
import jax.numpy as jnp
from jax import lax
from jax.experimental import pallas as pl
from jax.experimental.pallas import tpu as pltpu
from jax.sharding import Mesh
from jax.sharding import PartitionSpec as P


FS = ("y", "x")
TP = ("z", "c")
ALL = ("y", "x", "z", "c")
NY, NX, NZ, NC = 4, 4, 8, 2
EPS = 1e-06
HALO = 16
BLOCK = 256 + HALO
MB = 1024 * 1024


def moved(array, target):
    pairs = []
    for y in range(NY):
        for x in range(NX):
            for z in range(NZ):
                for c in range(NC):
                    to = target(y, x, z, c)
                    if to is None:
                        continue
                    source = ((y * NX + x) * NZ + z) * NC + c
                    ty, tx, tz, tc = to
                    pairs.append((source, ((ty * NX + tx) * NZ + tz) * NC + tc))
    return lax.ppermute(array, ALL, pairs)


def same_parity(k):
    return lambda y, x, z, c: (y, x, (z + k) % NZ, c)


def first_by(k):
    return lambda y, x, z, c: (y, (x + k) % NX, z, c) if c == 0 else ((y + k) % NY, x, z, c)


def second_by(k):
    return lambda y, x, z, c: ((y + k) % NY, x, z, c) if c == 0 else (y, (x + k) % NX, z, c)


def other_core(y, x, z, c):
    return (y, x, z, 1 - c)


def to_helper(y, x, z, c):
    return (y, x, (z - 1 if c == 0 else z + 1) % NZ, c)


def from_helper(y, x, z, c):
    return (y, x, (z + 1 if c == 0 else z - 1) % NZ, c)


def next_device(y, x, z, c):
    at = ((y * NX + x) * NZ + z) * NC + c + 1
    if at >= NY * NX * NZ * NC:
        return None
    return (at // (NX * NZ * NC), at // (NZ * NC) % NX, at // NC % NZ, at % NC)


def all_of_four(block, by):
    return block, moved(block, by(1)), moved(block, by(-1)), moved(block, by(2))


def ring_of_four(block, by):
    half = block.shape[0] // 2
    before = moved(block, by(1))
    after = moved(block, by(-1))
    top = moved(before[:half], by(1))
    bottom = moved(after[half:], by(-1))
    return block, before, after, top, bottom


VM = pl.BlockSpec(memory_space=pltpu.VMEM)
ANY = pl.BlockSpec(memory_space=pl.ANY)


def call(body, ins, outs, specs, *, flops=MB, nbytes=MB, scratch=(), limit=16, kept=VM):
    return pl.pallas_call(
        body,
        out_shape=outs,
        in_specs=specs,
        out_specs=[kept] * len(outs),
        scratch_shapes=list(scratch),
        compiler_params=pltpu.CompilerParams(vmem_limit_bytes=limit * MB),
        cost_estimate=pl.CostEstimate(flops=flops, bytes_accessed=nbytes, transcendentals=0),
    )(*ins)


def sds(shape, dtype=jnp.bfloat16):
    return jax.ShapeDtypeStruct(shape, dtype)


def here():
    y, x, c = lax.axis_index("y"), lax.axis_index("x"), lax.axis_index("c")
    mine, across = jnp.where(c == 0, x, y), jnp.where(c == 0, y, x)
    near = [(mine + k) & 3 for k in (0, 3, 1, 2)]
    far = [(across + k) & 3 for k in (0, 3, 1, 2)]
    place_near, place_far = jnp.where(c == 0, 64, 256), jnp.where(c == 0, 256, 64)
    blocks = [f * place_far + n * place_near for f in far for n in range(4)]
    members = [2 + c, c, 3 - c, 1 - c]
    spots = blocks + [m * BLOCK for m in members] + [n * 64 for n in near] + [c]
    return spots + [f * 256 for f in far] + [c * 256, (1 - c) * 256]


def placed(body, *fixed):
    return lambda *refs: body(*fixed, here(), *refs)


def normed_rows(wide, scale):
    power = jnp.mean(wide * wide, axis=-1, keepdims=True)
    return wide * lax.rsqrt(power + EPS) * scale


def turned(wide):
    blocks = [wide[:, (y * NX + x) * 64 : (y * NX + x + 1) * 64] for x in range(NX) for y in range(NY)]
    return jnp.concatenate(blocks, axis=1)


def norm_body(spots, tokens, scale, out, last):
    rows = normed_rows(tokens[...].astype(jnp.float32), scale[...])
    last[...] = rows[256 - HALO :].astype(jnp.bfloat16)

    @pl.when(spots[24] == 0)
    def _():
        out[...] = rows.astype(jnp.bfloat16)

    @pl.when(spots[24] == 1)
    def _():
        out[...] = turned(rows).astype(jnp.bfloat16)


def join_body(spots, own, halo, out):
    out[HALO:BLOCK, :] = own[...]

    @pl.when(spots[24] == 0)
    def _():
        out[0:HALO, :] = halo[...]

    @pl.when(spots[24] == 1)
    def _():
        out[0:HALO, :] = turned(halo[...].astype(jnp.float32)).astype(jnp.bfloat16)


def stack_body(own, chip, out):
    out[0:BLOCK, :] = turned(own[...].astype(jnp.float32)).astype(jnp.bfloat16)
    out[BLOCK : 2 * BLOCK, :] = turned(chip[...].astype(jnp.float32)).astype(jnp.bfloat16)


def rows_body(spots, own, chip, core, out):
    for k, ref, row in ((0, own, 0), (1, chip, 0), (2, core, 0), (3, core, BLOCK)):
        where = pl.multiple_of(spots[16 + k], 16)
        out[pl.ds(where, BLOCK), :] = ref[row : row + BLOCK, :]


def final_body(own, near, far, scale, out, made, sems):
    copies = []
    for k in range(4):
        some = slice(64 * k, 64 * k + 64)
        total = own[some, :] + near[some, :].astype(jnp.float32) + far[some, :].astype(jnp.float32)
        made[some, :] = normed_rows(total, scale[...]).astype(jnp.bfloat16)
        copies.append(pltpu.make_async_copy(made.at[some, :], out.at[some, :], sems.at[k]))
        copies[-1].start()
    for copy in copies:
        copy.wait()


PACK = 304


def three_parts(values):
    high = values.astype(jnp.bfloat16).astype(jnp.float32)
    rest = values - high
    middle = rest.astype(jnp.bfloat16).astype(jnp.float32)
    return [high, middle, rest - middle]


def pack_body(joint, taps, out):
    f32, bf16 = jnp.float32, jnp.bfloat16
    rows = jnp.concatenate(three_parts(taps[0:3, :]) + three_parts(taps[3:6, :]), axis=0)
    out[0:192, :] = joint[:, 0:128]
    value, gate, down = (joint[k : k + 64, 128:176].astype(f32) for k in (0, 64, 128))
    out[192:256, :] = jnp.concatenate([value, gate, down[:, 0:32]], axis=1).astype(bf16)
    folded = [down[k : k + 16, 32:48] for k in (0, 16, 32, 48)]
    left = jnp.concatenate(folded + [rows[0:16, 128:176], jnp.zeros((16, 16), f32)], axis=1)
    out[256:272, :] = left.astype(bf16)
    ends = jnp.concatenate([rows[16:18, 128:176], jnp.zeros((2, 80), f32)], axis=1)
    gap = jnp.zeros((6, 128), f32)
    out[272:304, :] = jnp.concatenate([rows[:, 0:128], gap, ends, gap], axis=0).astype(bf16)


def arranged(v, g):
    return jnp.concatenate(
        [v[:, 0:256], g[:, 0:256], v[:, 256:512], g[:, 256:512], v[:, 512:640], g[:, 512:640], v[:, 640:704], g[:, 640:704]],
        axis=1,
    )


def assemble_body(p0, p1, p2, p3, both, taps):
    f32 = jnp.float32
    values, gates, downs, parts = [], [], [], []
    for p in (p0, p1, p2, p3):
        other = p[192:256, :].astype(f32)
        left = p[256:272, :].astype(f32)
        rows = p[272:304, :].astype(f32)
        folded = jnp.concatenate([left[:, k : k + 16] for k in (0, 16, 32, 48)], axis=0)
        values += [p[0:64, :].astype(f32), other[:, 0:48]]
        gates += [p[64:128, :].astype(f32), other[:, 48:96]]
        downs += [p[128:192, :].astype(f32), other[:, 96:128], folded]
        parts += [rows[0:18], jnp.concatenate([left[:, 64:112], rows[24:26, 0:48]], axis=0)]
    both[0:64, :] = arranged(jnp.concatenate(values, axis=1), jnp.concatenate(gates, axis=1)).astype(jnp.bfloat16)
    down = jnp.concatenate(downs, axis=1)
    both[64:96, :] = jnp.concatenate([down[0:32], down[32:64]], axis=1).astype(jnp.bfloat16)
    parts = jnp.concatenate(parts, axis=1)
    whole = [(parts[k : k + 3] + parts[k + 3 : k + 6]) + parts[k + 6 : k + 9] for k in (0, 9)]
    taps[...] = jnp.concatenate([arranged(*whole), jnp.zeros((5, 1408), f32)], axis=0)


def line_body(spots, b0, b1, b2, b3, up, down):
    for k, piece in enumerate((b0, b1, b2, b3)):
        where = spots[20 + k]
        up[pl.ds(pl.multiple_of(where, 64), 64), :] = piece[0:64, :]
        down[pl.ds(pl.multiple_of(where >> 1, 32), 32), :] = piece[64:96, :]


def gelu(v):
    inner = v * (0.7978845608028654 + 0.035677408136300125 * (v * v))
    return 0.5 * v * (1.0 + jnp.tanh(inner))


GROUPS = ((0, 512), (512, 512), (1024, 384))


def own_body(spots, x_rows, w0, acc):
    x_some = x_rows[:, pl.ds(pl.multiple_of(spots[25], 256), 256)]
    for start, width in GROUPS:
        columns = slice(start, start + width)
        acc[:, columns] = jnp.dot(x_some, w0[:, columns], preferred_element_type=jnp.float32)


def more_body(spots, x_rows, before, w1, w2, d0, d1, d2, acc, down, x_some, w_some):
    unfold(spots, 0, (d0, d1, d2), down)
    for k, piece in enumerate((w1, w2)):
        where = pl.multiple_of(spots[26 + k], 256)
        x_some[:, k * 256 : k * 256 + 256] = x_rows[:, pl.ds(where, 256)]
        w_some[k * 256 : k * 256 + 256, :] = piece[...]
    for start, width in GROUPS:
        columns = slice(start, start + width)
        acc[:, columns] = before[:, columns] + jnp.dot(
            x_some[...], w_some[:, columns], preferred_element_type=jnp.float32
        )


def unfold(spots, at, pieces, out):
    for piece in pieces:
        for row in range(0, piece.shape[0], 32):
            where = pl.multiple_of(spots[at], 64)
            rows = piece[row : row + 32, :].astype(jnp.float32)
            gap = jnp.zeros((32, 64), jnp.float32)
            out[pl.ds(where, 32), :] = jnp.concatenate([rows[:, 0:704], gap], axis=1).astype(jnp.bfloat16)
            out[pl.ds(where + 32, 32), :] = jnp.concatenate([rows[:, 704:1408], gap], axis=1).astype(jnp.bfloat16)
            at += 1


def first_body(spot, spots, hidden, early, d3, d4, out, d_all):
    d_all[...] = early[...]
    unfold(spots, 12, (d3, d4), d_all)
    r0 = pl.multiple_of(spots[spot], 256)
    product = lax.dot_general(
        hidden[pl.ds(r0, 256), :], d_all[...], (((1,), (1,)), ((), ())), preferred_element_type=jnp.float32
    )
    out[...] = product.astype(out.dtype)


CHUNKS = (((0, 2, 0), (1, 3, 128)), ((4, 6, 256), (5, 7, 384)), ((8, 9, 512), (10, None, 640)))


def hidden_body(half, spots, x_rows, acc, w3, w4, taps, gate, hidden, w_some, full):
    w_some[0:128, :] = w3[...]
    w_some[128:256, :] = w4[...]
    r0 = half * 2 * BLOCK
    where = pl.multiple_of(spots[28], 256)
    x_some = x_rows[r0 : r0 + 2 * BLOCK, pl.ds(where, 256)]

    def conv(row, part):
        at = part * 2 * BLOCK + row + HALO * (row // 256) + HALO
        scale = taps[:, part * 128 : part * 128 + 128]
        made = full[at - 2 : at + 62, :] * scale[0:1]
        made = made + full[at - 1 : at + 63, :] * scale[1:2]
        return made + full[at : at + 64, :] * scale[2:3]

    for (start, width), chunks in zip(GROUPS, CHUNKS):
        columns = slice(start, start + width)
        whole = acc[r0 : r0 + 2 * BLOCK, columns] + jnp.dot(
            x_some, w_some[:, columns], preferred_element_type=jnp.float32
        )
        for k in range(width // 128):
            first = (start // 128 + k) * 2 * BLOCK
            full[first : first + 2 * BLOCK, :] = whole[:, k * 128 : k * 128 + 128]
        for value, gated, at in chunks:
            for row in range(0, 512, 64):
                made = conv(row, value)
                if gated is None:
                    made = gelu(pltpu.roll(made, 64, 1)) * made
                    lane = lax.broadcasted_iota(jnp.int32, made.shape, 1)
                    made = jnp.where(lane < 64, made, 0.0)
                else:
                    made = gelu(conv(row, gated)) * made
                hidden[row : row + 64, at : at + 128] = made.astype(jnp.bfloat16)


def product_body(spot, spots, hidden, d_all, gate, out):
    r0 = pl.multiple_of(spots[spot], 256)
    product = lax.dot_general(
        hidden[pl.ds(r0, 256), :], d_all[...], (((1,), (1,)), ((), ())), preferred_element_type=jnp.float32
    )
    out[...] = product.astype(out.dtype)


def shards(tokens, norm_in, value_weight, gate_weight, value_taps, gate_taps, down_weight, norm_out):
    f32 = jnp.float32
    (pack,) = call(
        pack_body,
        (
            jnp.concatenate([value_weight, gate_weight, down_weight.T], axis=0),
            jnp.concatenate([value_taps, gate_taps], axis=0),
        ),
        [sds((PACK, 128))],
        [VM] * 2,
    )
    packs = [pack] + [moved(pack, same_parity(k)) for k in (4, -2, 2)]
    both, tap_rows = call(assemble_body, packs, [sds((96, 1408)), sds((8, 1408), f32)], [VM] * 4)
    up_line, down_line = call(
        placed(line_body), all_of_four(both, first_by), [sds((256, 1408)), sds((128, 1408))], [VM] * 4
    )
    ups = ring_of_four(up_line, second_by)
    downs = ring_of_four(down_line, second_by)

    normed, last = call(
        placed(norm_body),
        (tokens, norm_in.reshape(1, -1)),
        [sds(tokens.shape), sds((HALO, 1024))],
        [VM] * 2,
    )
    halo = moved(last, next_device)
    (joined,) = call(placed(join_body), (normed, halo), [sds((BLOCK, 1024))], [VM] * 2)
    chip = moved(joined, to_helper)
    (stacked,) = call(stack_body, (joined, chip), [sds((2 * BLOCK, 1024))], [VM, VM])
    core = moved(stacked, other_core)
    (x_rows,) = call(placed(rows_body), (joined, chip, core), [sds((4 * BLOCK, 1024))], [VM] * 3)

    sums, d_rows = [sds((4 * BLOCK, 1408), f32)], sds((1024, 768))
    (acc_own,) = call(placed(own_body), (x_rows, ups[0]), sums, [VM] * 2, flops=2 * 1040 * 256 * 1408, nbytes=8 * MB)
    acc, d_early = call(
        placed(more_body),
        (x_rows, acc_own, *ups[1:3], *downs[:3]),
        sums + [d_rows],
        [VM] * 7,
        flops=2 * 1088 * 512 * 1408,
        nbytes=8 * MB,
        limit=16,
        scratch=(pltpu.VMEM((4 * BLOCK, 512), jnp.bfloat16), pltpu.VMEM((512, 1408), jnp.bfloat16)),
    )

    def hidden_of(half, gate):
        (out,) = call(
            placed(hidden_body, half),
            (x_rows, acc, ups[3], ups[4], tap_rows, gate),
            [sds((512, 768))],
            [VM] * 5 + [ANY],
            flops=2 * 544 * 256 * 1408 * 3,
            nbytes=4 * MB,
            limit=16,
            scratch=(pltpu.VMEM((256, 1408), jnp.bfloat16), pltpu.VMEM((11 * 2 * BLOCK, 128), f32)),
        )
        return out

    def product_of(spot, hidden, dtype, gate):
        (out,) = call(
            placed(product_body, spot),
            (hidden, d_all, gate),
            [sds((256, 1024), dtype)],
            [VM] * 2 + [ANY],
            flops=2 * 256 * 768 * 1024,
            nbytes=2 * MB,
        )
        return out

    hidden_far = hidden_of(0, acc)
    first, d_all = call(
        placed(first_body, 30),
        (hidden_far, d_early, *downs[3:]),
        [sds((256, 1024)), d_rows],
        [VM] * 4,
        flops=2 * 256 * 768 * 1024,
        nbytes=4 * MB,
    )
    got_far = moved(first, other_core)
    second = product_of(29, hidden_far, f32, first)
    sent = (second + got_far.astype(f32)).astype(jnp.bfloat16)
    back = moved(sent, from_helper)
    hidden_near = hidden_of(1, sent)
    third = product_of(30, hidden_near, jnp.bfloat16, sent)
    got_near = moved(third, other_core)
    fourth = product_of(29, hidden_near, f32, third)
    (out,) = call(
        final_body,
        (fourth, got_near, back, norm_out.reshape(1, -1)),
        [sds((256, 1024))],
        [VM] * 4,
        scratch=(pltpu.VMEM((256, 1024), jnp.bfloat16), pltpu.SemaphoreType.DMA((4,))),
        kept=ANY,
    )
    return out


def solution(mesh):
    split = Mesh(mesh.devices.reshape(NY, NX, NZ, NC), ALL)
    return jax.shard_map(
        shards,
        mesh=split,
        in_specs=(P(ALL, None), P(), P(FS, TP), P(FS, TP), P(None, TP), P(None, TP), P(TP, FS), P()),
        out_specs=P(ALL, None),
        check_vma=False,
    )
```

```python
import jax
import jax.numpy as jnp
from jax import lax
from jax.experimental import pallas as pl
from jax.experimental.pallas import tpu as pltpu
from jax.sharding import Mesh
from jax.sharding import PartitionSpec as P


FS = ("y", "x")
TP = ("z", "c")
ALL = ("y", "x", "z", "c")
NY, NX, NZ, NC = 4, 4, 8, 2
EPS = 1e-06
HALO = 16
BLOCK = 256 + HALO
MB = 1024 * 1024


def moved(array, target):
    pairs = []
    for y in range(NY):
        for x in range(NX):
            for z in range(NZ):
                for c in range(NC):
                    to = target(y, x, z, c)
                    if to is None:
                        continue
                    source = ((y * NX + x) * NZ + z) * NC + c
                    ty, tx, tz, tc = to
                    pairs.append((source, ((ty * NX + tx) * NZ + tz) * NC + tc))
    return lax.ppermute(array, ALL, pairs)


def same_parity(k):
    return lambda y, x, z, c: (y, x, (z + k) % NZ, c)


def first_by(k):
    return lambda y, x, z, c: (y, (x + k) % NX, z, c) if c == 0 else ((y + k) % NY, x, z, c)


def second_by(k):
    return lambda y, x, z, c: ((y + k) % NY, x, z, c) if c == 0 else (y, (x + k) % NX, z, c)


def other_core(y, x, z, c):
    return (y, x, z, 1 - c)


def to_helper(y, x, z, c):
    return (y, x, (z - 1 if c == 0 else z + 1) % NZ, c)


def from_helper(y, x, z, c):
    return (y, x, (z + 1 if c == 0 else z - 1) % NZ, c)


def next_device(y, x, z, c):
    at = ((y * NX + x) * NZ + z) * NC + c + 1
    if at >= NY * NX * NZ * NC:
        return None
    return (at // (NX * NZ * NC), at // (NZ * NC) % NX, at // NC % NZ, at % NC)


def all_of_four(block, by):
    return block, moved(block, by(1)), moved(block, by(-1)), moved(block, by(2))


def ring_of_four(block, by):
    half = block.shape[0] // 2
    before = moved(block, by(1))
    after = moved(block, by(-1))
    top = moved(before[:half], by(1))
    bottom = moved(after[half:], by(-1))
    return block, before, after, top, bottom


VM = pl.BlockSpec(memory_space=pltpu.VMEM)
ANY = pl.BlockSpec(memory_space=pl.ANY)


def call(body, ins, outs, specs, *, flops=MB, nbytes=MB, scratch=(), limit=16, kept=VM):
    return pl.pallas_call(
        body,
        out_shape=outs,
        in_specs=specs,
        out_specs=[kept] * len(outs),
        scratch_shapes=list(scratch),
        compiler_params=pltpu.CompilerParams(vmem_limit_bytes=limit * MB),
        cost_estimate=pl.CostEstimate(flops=flops, bytes_accessed=nbytes, transcendentals=0),
    )(*ins)


def sds(shape, dtype=jnp.bfloat16):
    return jax.ShapeDtypeStruct(shape, dtype)


def here():
    y, x, c = lax.axis_index("y"), lax.axis_index("x"), lax.axis_index("c")
    mine, across = jnp.where(c == 0, x, y), jnp.where(c == 0, y, x)
    near = [(mine + k) & 3 for k in (0, 3, 1, 2)]
    far = [(across + k) & 3 for k in (0, 3, 1, 2)]
    place_near, place_far = jnp.where(c == 0, 64, 256), jnp.where(c == 0, 256, 64)
    blocks = [f * place_far + n * place_near for f in far for n in range(4)]
    members = [2 + c, c, 3 - c, 1 - c]
    spots = blocks + [m * BLOCK for m in members] + [n * 64 for n in near] + [c]
    return spots + [f * 256 for f in far] + [c * 256, (1 - c) * 256]


def placed(body, *fixed):
    return lambda *refs: body(*fixed, here(), *refs)


def normed_rows(wide, scale):
    power = jnp.mean(wide * wide, axis=-1, keepdims=True)
    return wide * lax.rsqrt(power + EPS) * scale


def turned(wide):
    blocks = [wide[:, (y * NX + x) * 64 : (y * NX + x + 1) * 64] for x in range(NX) for y in range(NY)]
    return jnp.concatenate(blocks, axis=1)


def norm_body(spots, tokens, scale, out, last):
    rows = normed_rows(tokens[...].astype(jnp.float32), scale[...])
    last[...] = rows[256 - HALO :].astype(jnp.bfloat16)

    @pl.when(spots[24] == 0)
    def _():
        out[...] = rows.astype(jnp.bfloat16)

    @pl.when(spots[24] == 1)
    def _():
        out[...] = turned(rows).astype(jnp.bfloat16)


def join_body(spots, own, halo, out):
    out[HALO:BLOCK, :] = own[...]

    @pl.when(spots[24] == 0)
    def _():
        out[0:HALO, :] = halo[...]

    @pl.when(spots[24] == 1)
    def _():
        out[0:HALO, :] = turned(halo[...].astype(jnp.float32)).astype(jnp.bfloat16)


def stack_body(own, chip, out):
    out[0:BLOCK, :] = turned(own[...].astype(jnp.float32)).astype(jnp.bfloat16)
    out[BLOCK : 2 * BLOCK, :] = turned(chip[...].astype(jnp.float32)).astype(jnp.bfloat16)


def rows_body(spots, own, chip, core, out):
    for k, ref, row in ((0, own, 0), (1, chip, 0), (2, core, 0), (3, core, BLOCK)):
        where = pl.multiple_of(spots[16 + k], 16)
        out[pl.ds(where, BLOCK), :] = ref[row : row + BLOCK, :]


def final_body(own, near, far, scale, out, made, sems):
    copies = []
    for k in range(4):
        some = slice(64 * k, 64 * k + 64)
        total = own[some, :] + near[some, :].astype(jnp.float32) + far[some, :].astype(jnp.float32)
        made[some, :] = normed_rows(total, scale[...]).astype(jnp.bfloat16)
        copies.append(pltpu.make_async_copy(made.at[some, :], out.at[some, :], sems.at[k]))
        copies[-1].start()
    for copy in copies:
        copy.wait()


PACK = 304


def three_parts(values):
    high = values.astype(jnp.bfloat16).astype(jnp.float32)
    rest = values - high
    middle = rest.astype(jnp.bfloat16).astype(jnp.float32)
    return [high, middle, rest - middle]


def pack_body(joint, taps, out):
    f32, bf16 = jnp.float32, jnp.bfloat16
    rows = jnp.concatenate(three_parts(taps[0:3, :]) + three_parts(taps[3:6, :]), axis=0)
    out[0:192, :] = joint[:, 0:128]
    value, gate, down = (joint[k : k + 64, 128:176].astype(f32) for k in (0, 64, 128))
    out[192:256, :] = jnp.concatenate([value, gate, down[:, 0:32]], axis=1).astype(bf16)
    folded = [down[k : k + 16, 32:48] for k in (0, 16, 32, 48)]
    left = jnp.concatenate(folded + [rows[0:16, 128:176], jnp.zeros((16, 16), f32)], axis=1)
    out[256:272, :] = left.astype(bf16)
    ends = jnp.concatenate([rows[16:18, 128:176], jnp.zeros((2, 80), f32)], axis=1)
    gap = jnp.zeros((6, 128), f32)
    out[272:304, :] = jnp.concatenate([rows[:, 0:128], gap, ends, gap], axis=0).astype(bf16)


def arranged(v, g):
    return jnp.concatenate(
        [v[:, 0:256], g[:, 0:256], v[:, 256:512], g[:, 256:512], v[:, 512:640], g[:, 512:640], v[:, 640:704], g[:, 640:704]],
        axis=1,
    )


def assemble_body(p0, p1, p2, p3, both, taps):
    f32 = jnp.float32
    values, gates, downs, parts = [], [], [], []
    for p in (p0, p1, p2, p3):
        other = p[192:256, :].astype(f32)
        left = p[256:272, :].astype(f32)
        rows = p[272:304, :].astype(f32)
        folded = jnp.concatenate([left[:, k : k + 16] for k in (0, 16, 32, 48)], axis=0)
        values += [p[0:64, :].astype(f32), other[:, 0:48]]
        gates += [p[64:128, :].astype(f32), other[:, 48:96]]
        downs += [p[128:192, :].astype(f32), other[:, 96:128], folded]
        parts += [rows[0:18], jnp.concatenate([left[:, 64:112], rows[24:26, 0:48]], axis=0)]
    both[0:64, :] = arranged(jnp.concatenate(values, axis=1), jnp.concatenate(gates, axis=1)).astype(jnp.bfloat16)
    down = jnp.concatenate(downs, axis=1)
    both[64:96, :] = jnp.concatenate([down[0:32], down[32:64]], axis=1).astype(jnp.bfloat16)
    parts = jnp.concatenate(parts, axis=1)
    whole = [(parts[k : k + 3] + parts[k + 3 : k + 6]) + parts[k + 6 : k + 9] for k in (0, 9)]
    taps[...] = jnp.concatenate([arranged(*whole), jnp.zeros((5, 1408), f32)], axis=0)


def line_body(spots, b0, b1, b2, b3, up, down):
    for k, piece in enumerate((b0, b1, b2, b3)):
        where = spots[20 + k]
        up[pl.ds(pl.multiple_of(where, 64), 64), :] = piece[0:64, :]
        down[pl.ds(pl.multiple_of(where >> 1, 32), 32), :] = piece[64:96, :]


def gelu(v):
    inner = v * (0.7978845608028654 + 0.035677408136300125 * (v * v))
    return 0.5 * v * (1.0 + jnp.tanh(inner))


GROUPS = ((0, 512), (512, 512), (1024, 384))


def own_body(spots, x_rows, w0, acc):
    x_some = x_rows[:, pl.ds(pl.multiple_of(spots[25], 256), 256)]
    for start, width in GROUPS:
        columns = slice(start, start + width)
        acc[:, columns] = jnp.dot(x_some, w0[:, columns], preferred_element_type=jnp.float32)


def more_body(spots, x_rows, before, w1, w2, acc, x_some, w_some):
    for k, piece in enumerate((w1, w2)):
        where = pl.multiple_of(spots[26 + k], 256)
        x_some[:, k * 256 : k * 256 + 256] = x_rows[:, pl.ds(where, 256)]
        w_some[k * 256 : k * 256 + 256, :] = piece[...]
    for start, width in GROUPS:
        columns = slice(start, start + width)
        acc[:, columns] = before[:, columns] + jnp.dot(
            x_some[...], w_some[:, columns], preferred_element_type=jnp.float32
        )


def unfold(spots, at, pieces, out):
    for piece in pieces:
        for row in range(0, piece.shape[0], 32):
            where = pl.multiple_of(spots[at], 64)
            rows = piece[row : row + 32, :].astype(jnp.float32)
            gap = jnp.zeros((32, 64), jnp.float32)
            out[pl.ds(where, 32), :] = jnp.concatenate([rows[:, 0:704], gap], axis=1).astype(jnp.bfloat16)
            out[pl.ds(where + 32, 32), :] = jnp.concatenate([rows[:, 704:1408], gap], axis=1).astype(jnp.bfloat16)
            at += 1


def down_body(spots, d0, d1, d2, gate, out):
    unfold(spots, 0, (d0, d1, d2), out)


def first_body(spot, spots, hidden, early, d3, d4, out, d_all):
    d_all[...] = early[...]
    unfold(spots, 12, (d3, d4), d_all)
    r0 = pl.multiple_of(spots[spot], 256)
    product = lax.dot_general(
        hidden[pl.ds(r0, 256), :], d_all[...], (((1,), (1,)), ((), ())), preferred_element_type=jnp.float32
    )
    out[...] = product.astype(out.dtype)


CHUNKS = (((0, 2, 0), (1, 3, 128)), ((4, 6, 256), (5, 7, 384)), ((8, 9, 512), (10, None, 640)))


def hidden_body(half, spots, x_rows, acc, w3, w4, taps, gate, hidden, w_some, full):
    w_some[0:128, :] = w3[...]
    w_some[128:256, :] = w4[...]
    r0 = half * 2 * BLOCK
    where = pl.multiple_of(spots[28], 256)
    x_some = x_rows[r0 : r0 + 2 * BLOCK, pl.ds(where, 256)]

    def conv(row, part):
        at = part * 2 * BLOCK + row + HALO * (row // 256) + HALO
        scale = taps[:, part * 128 : part * 128 + 128]
        made = full[at - 2 : at + 62, :] * scale[0:1]
        made = made + full[at - 1 : at + 63, :] * scale[1:2]
        return made + full[at : at + 64, :] * scale[2:3]

    for (start, width), chunks in zip(GROUPS, CHUNKS):
        columns = slice(start, start + width)
        whole = acc[r0 : r0 + 2 * BLOCK, columns] + jnp.dot(
            x_some, w_some[:, columns], preferred_element_type=jnp.float32
        )
        for k in range(width // 128):
            first = (start // 128 + k) * 2 * BLOCK
            full[first : first + 2 * BLOCK, :] = whole[:, k * 128 : k * 128 + 128]
        for value, gated, at in chunks:
            for row in range(0, 512, 64):
                made = conv(row, value)
                if gated is None:
                    made = gelu(pltpu.roll(made, 64, 1)) * made
                    lane = lax.broadcasted_iota(jnp.int32, made.shape, 1)
                    made = jnp.where(lane < 64, made, 0.0)
                else:
                    made = gelu(conv(row, gated)) * made
                hidden[row : row + 64, at : at + 128] = made.astype(jnp.bfloat16)


def product_body(spot, spots, hidden, d_all, gate, out):
    r0 = pl.multiple_of(spots[spot], 256)
    product = lax.dot_general(
        hidden[pl.ds(r0, 256), :], d_all[...], (((1,), (1,)), ((), ())), preferred_element_type=jnp.float32
    )
    out[...] = product.astype(out.dtype)


def shards(tokens, norm_in, value_weight, gate_weight, value_taps, gate_taps, down_weight, norm_out):
    f32 = jnp.float32
    (pack,) = call(
        pack_body,
        (
            jnp.concatenate([value_weight, gate_weight, down_weight.T], axis=0),
            jnp.concatenate([value_taps, gate_taps], axis=0),
        ),
        [sds((PACK, 128))],
        [VM] * 2,
    )
    packs = [pack] + [moved(pack, same_parity(k)) for k in (4, -2, 2)]
    both, tap_rows = call(assemble_body, packs, [sds((96, 1408)), sds((8, 1408), f32)], [VM] * 4)
    up_line, down_line = call(
        placed(line_body), all_of_four(both, first_by), [sds((256, 1408)), sds((128, 1408))], [VM] * 4
    )
    ups = ring_of_four(up_line, second_by)
    downs = ring_of_four(down_line, second_by)

    normed, last = call(
        placed(norm_body),
        (tokens, norm_in.reshape(1, -1)),
        [sds(tokens.shape), sds((HALO, 1024))],
        [VM] * 2,
    )
    halo = moved(last, next_device)
    (joined,) = call(placed(join_body), (normed, halo), [sds((BLOCK, 1024))], [VM] * 2)
    chip = moved(joined, to_helper)
    (stacked,) = call(stack_body, (joined, chip), [sds((2 * BLOCK, 1024))], [VM, VM])
    core = moved(stacked, other_core)
    (x_rows,) = call(placed(rows_body), (joined, chip, core), [sds((4 * BLOCK, 1024))], [VM] * 3)

    sums = [sds((4 * BLOCK, 1408), f32)]
    (acc_own,) = call(placed(own_body), (x_rows, ups[0]), sums, [VM] * 2, flops=2 * 1040 * 256 * 1408, nbytes=8 * MB)
    (acc,) = call(
        placed(more_body),
        (x_rows, acc_own, *ups[1:3]),
        sums,
        [VM] * 4,
        flops=2 * 1088 * 512 * 1408,
        nbytes=8 * MB,
        limit=16,
        scratch=(pltpu.VMEM((4 * BLOCK, 512), jnp.bfloat16), pltpu.VMEM((512, 1408), jnp.bfloat16)),
    )

    def hidden_of(half, gate):
        (out,) = call(
            placed(hidden_body, half),
            (x_rows, acc, ups[3], ups[4], tap_rows, gate),
            [sds((512, 768))],
            [VM] * 5 + [ANY],
            flops=2 * 544 * 256 * 1408 * 3,
            nbytes=4 * MB,
            limit=16,
            scratch=(pltpu.VMEM((256, 1408), jnp.bfloat16), pltpu.VMEM((11 * 2 * BLOCK, 128), f32)),
        )
        return out

    def product_of(spot, hidden, dtype, gate):
        (out,) = call(
            placed(product_body, spot),
            (hidden, d_all, gate),
            [sds((256, 1024), dtype)],
            [VM] * 2 + [ANY],
            flops=2 * 256 * 768 * 1024,
            nbytes=2 * MB,
        )
        return out

    d_rows = sds((1024, 768))
    (d_early,) = call(placed(down_body), (*downs[:3], acc), [d_rows], [VM] * 3 + [ANY])
    hidden_far = hidden_of(0, d_early)
    first, d_all = call(
        placed(first_body, 30),
        (hidden_far, d_early, *downs[3:]),
        [sds((256, 1024)), d_rows],
        [VM] * 4,
        flops=2 * 256 * 768 * 1024,
        nbytes=4 * MB,
    )
    got_far = moved(first, other_core)
    second = product_of(29, hidden_far, f32, first)
    sent = (second + got_far.astype(f32)).astype(jnp.bfloat16)
    back = moved(sent, from_helper)
    hidden_near = hidden_of(1, sent)
    third = product_of(30, hidden_near, jnp.bfloat16, sent)
    got_near = moved(third, other_core)
    fourth = product_of(29, hidden_near, f32, third)
    (out,) = call(
        final_body,
        (fourth, got_near, back, norm_out.reshape(1, -1)),
        [sds((256, 1024))],
        [VM] * 4,
        scratch=(pltpu.VMEM((256, 1024), jnp.bfloat16), pltpu.SemaphoreType.DMA((4,))),
        kept=ANY,
    )
    return out


def solution(mesh):
    split = Mesh(mesh.devices.reshape(NY, NX, NZ, NC), ALL)
    return jax.shard_map(
        shards,
        mesh=split,
        in_specs=(P(ALL, None), P(), P(FS, TP), P(FS, TP), P(None, TP), P(None, TP), P(TP, FS), P()),
        out_specs=P(ALL, None),
        check_vma=False,
    )
```
